32 devices in a mesh: sp: 8 (over z, y), tp: 4 (over x, core).
Axes of the slice: x: 2, y: 2, z: 4, core: 2. Of those that a mesh axis runs over, the one named last changes fastest.
Arguments:
- activations: bfloat16 [3584, 2048], P(('sp', 'tp')), may hold values from -27.5 to 27.5
- query_weight: bfloat16 [2048, 2048], P(None, 'tp'), may hold values from -0.088388348 to 0.088388348
- key_weight: bfloat16 [2048, 2048], P(None, 'tp'), may hold values from -0.088388348 to 0.088388348
- value_weight: bfloat16 [2048, 2048], P(None, 'tp'), may hold values from -0.125 to 0.125
- out_weight: bfloat16 [2048, 2048], P('tp'), may hold values from -0.125 to 0.125
- lambdas: float32 [8], P('tp'), may hold values from 0.3 to 0.8
- head_gain: float32 [256], replicated, may hold values from 0.1 to 1.9
Outputs:
- mixed: bfloat16 [3584, 2048], P(('sp', 'tp'))
The draws below stay inside these ranges and needn't reach their ends.
All inputs are finite; a program needn't handle non-finite values.
Results may differ from the reference program's by a relative error of at most 0.014.
Values may be sent and summed in bfloat16 or wider, within the bound.
A program may use at most 128 MiB of HBM per device.

```python
import jax
import jax.numpy as jnp
from jax import lax

D = 2048
HEADS = 8
HEAD = 128
VALUE = 256
TOK_DEV = 448
SEQ = 3584
N_TP = 4


def draw_activations(key, part):
    noise_base = jnp.clip(jax.random.normal(jax.random.fold_in(key, 1), (SEQ, D), jnp.float32), -4.0, 4.0)
    block_means = jax.random.uniform(jax.random.fold_in(key, 2), (SEQ // TOK_DEV, D), jnp.float32, -1.5, 1.5)
    result = noise_base + jnp.repeat(block_means, TOK_DEV, axis=0)
    return result.astype(jnp.bfloat16)


def paired_weights(key):
    bound_value = 4.0 * D ** (-0.5)
    first_draw = jax.random.normal(jax.random.fold_in(key, 11), (D, HEADS * 2 * HEAD), jnp.float32) * D ** (-0.5)
    second = jax.random.normal(jax.random.fold_in(key, 12), (D, HEADS * 2 * HEAD), jnp.float32) * D ** (-0.5)
    return (first_draw, second, bound_value)


def draw_query_weight(key, part):
    first_draw, second, bound_value = paired_weights(key)
    return jnp.clip(first_draw, -bound_value, bound_value).astype(jnp.bfloat16)


def draw_key_weight(key, part):
    first_draw, second, bound_value = paired_weights(key)
    mixed_draw = second
    return jnp.clip(mixed_draw, -bound_value, bound_value).astype(jnp.bfloat16)


def level_of(key, shape, shards, least, largest):
    gain = 1.0
    for dim, blocks in shards:
        draws = jax.random.uniform(jax.random.fold_in(jax.random.fold_in(key, 6), dim), (blocks,), jnp.float32, least / len(shards), largest / len(shards))
        gain = gain * jnp.repeat(jnp.exp(draws), shape[dim] // blocks).reshape((-1,) + (1,) * (len(shape) - 1 - dim))
    return gain


def bell_draw(stream_key, dims, deviation, reach, split=(), kind=jnp.bfloat16):
    values = jax.random.normal(stream_key, dims, jnp.float32) * deviation
    if len(split) > 0:
        values = level_of(stream_key, dims, split, -0.22, 0.18) * values
    return jnp.clip(values, min=-reach, max=reach).astype(kind)


def setup_inputs(seed: int = 0) -> dict:
    key_of = jax.random.split(jax.random.key(seed), 8)
    activations = draw_activations(jax.random.fold_in(key_of[7], 71), 0)
    query_weight = draw_query_weight(jax.random.fold_in(key_of[7], 71), 0)
    key_weight = draw_key_weight(jax.random.fold_in(key_of[7], 71), 0)
    value_weight = bell_draw(key_of[3], (D, HEADS * VALUE), D ** -0.5, 0.125, ((1, 4),))
    out_weight = bell_draw(key_of[4], (HEADS * VALUE, D), (HEADS * VALUE) ** -0.5, 0.125, ((0, 4),))
    lambdas = jnp.clip(0.3 + 0.5 * jax.random.uniform(key_of[5], (HEADS,), jnp.float32) ** level_of(key_of[5], (HEADS,), ((0, 4),), -0.2, 0.2), 0.3, 0.8)
    head_gain = jnp.clip(1.0 + 0.18 * jax.random.normal(key_of[6], (VALUE,), jnp.float32), 0.1, 1.9)
    return dict(activations=activations, query_weight=query_weight, key_weight=key_weight, value_weight=value_weight, out_weight=out_weight, lambdas=lambdas, head_gain=head_gain)


norm_floor = 0.02

def reference(activations, query_weight, key_weight, value_weight, out_weight, lambdas, head_gain):
    queries = jnp.dot(activations, query_weight, preferred_element_type=jnp.float32).astype(jnp.bfloat16)
    key_rows = jnp.dot(activations, key_weight, preferred_element_type=jnp.float32).astype(jnp.bfloat16)
    value_rows = jnp.dot(activations, value_weight, preferred_element_type=jnp.float32).astype(jnp.bfloat16)
    queries = queries.reshape(SEQ, HEADS, 2, HEAD).transpose(1, 0, 2, 3)
    key_rows = key_rows.reshape(SEQ, HEADS, 2, HEAD).transpose(1, 0, 2, 3)
    value_rows = value_rows.reshape(SEQ, HEADS, VALUE).transpose(1, 0, 2)
    blocks = SEQ // TOK_DEV
    score_scale = HEAD ** (-0.5)
    key_pos = jnp.arange(SEQ, dtype=jnp.int32)

    def one_block(index):
        head_index = index // blocks
        block_index = index % blocks
        first_row = (block_index * TOK_DEV).astype(jnp.int32)
        query_rows = lax.dynamic_slice_in_dim(queries[head_index], first_row, TOK_DEV, 0).astype(jnp.float32)
        key_all = key_rows[head_index].astype(jnp.float32)
        value_all = value_rows[head_index].astype(jnp.float32)
        scores = jnp.einsum('qme,kme->mqk', query_rows, key_all) * score_scale
        query_pos = first_row + jnp.arange(TOK_DEV, dtype=jnp.int32)
        allowed = key_pos[None, :] <= query_pos[:, None]
        masked = jnp.where(allowed[None], scores, -jnp.inf)
        row_top = lax.optimization_barrier(jnp.max(masked, axis=-1, keepdims=True))
        exp_weights = jnp.where(allowed[None], jnp.exp(masked - row_top), 0.0)
        denominators = lax.optimization_barrier(jnp.sum(exp_weights, axis=-1))
        rounded = lax.optimization_barrier(exp_weights.astype(jnp.bfloat16)).astype(jnp.float32)
        weighted = jnp.einsum('mqk,kv->mqv', rounded, value_all)
        lambda_head = lambdas[head_index]
        combined = weighted[0] / denominators[0][:, None] - lambda_head * weighted[1] / denominators[1][:, None]
        inverse_rms = lax.rsqrt(lax.optimization_barrier(jnp.mean(combined * combined, axis=-1, keepdims=True)) + norm_floor)
        return (combined * inverse_rms * head_gain).astype(jnp.bfloat16)
    heads_out = lax.map(one_block, jnp.arange(HEADS * blocks, dtype=jnp.int32))
    heads_out = heads_out.reshape(HEADS, SEQ, VALUE).transpose(1, 0, 2).reshape(SEQ, HEADS * VALUE)
    group_width = HEADS // N_TP * VALUE
    totals = jnp.zeros((SEQ, D), jnp.float32)
    for group_index in range(N_TP):
        columns = heads_out[:, group_index * group_width:(group_index + 1) * group_width]
        weight_rows = out_weight[group_index * group_width:(group_index + 1) * group_width]
        partial_value = jnp.dot(columns, weight_rows, preferred_element_type=jnp.float32).astype(jnp.bfloat16)
        totals = totals + partial_value.astype(jnp.float32)
    return totals.astype(jnp.bfloat16)
```

```python
import functools
import math

import jax
import jax.numpy as jnp
from jax import lax
from jax.experimental import pallas as pl
from jax.experimental.pallas import tpu as pltpu
from jax.sharding import PartitionSpec as P

HEAD = 128
VALUE = 256


norm_floor = 0.02
very_low = -1e30
MESH = pl.DeviceIdType.MESH


def layer_kernel(
    S, T, L, R,
    act, qw, kw, vw, ow, lam_in, gain,
    out,
    A, WP, W, PR, PC, KV, HO, HI, LS, LB, ACC, MX, DN, TOT,
    w_sem, own_sem, a_send, a_recv, lam_send, lam_recv,
    ox_send, ox_recv, oy_send, oy_recv, m_send, m_recv,
    p_send, p_recv, f_send, f_recv, h_send, h_recv,
):
    X, Y = 2, 2
    Z = S // Y
    H = Z // 2
    s = lax.axis_index("sp")
    t = lax.axis_index("tp")
    x = t // 2
    c = t % 2
    y = s % Y
    z = s // Y
    half = z // H
    low = z % H
    mate = x * 2 + (1 - c)
    across = (1 - x) * 2 + c
    diagonal = (1 - x) * 2 + (1 - c)
    beside = z * Y + (1 - y)
    pair = (half * H + 1 - low) * Y + y
    side = (low + y) % 2
    near = half * H + 1 - low
    outer = (1 - half) * (Z - 1)
    inner = (1 - half) * H + half * (H - 1)
    head = x * 2 * L + z
    span = T * R
    scale = HEAD ** (-0.5) * math.log2(math.e)

    def remote(src, dst, ss, rs, sp, tp):
        return pltpu.make_async_remote_copy(
            src_ref=src, dst_ref=dst, send_sem=ss, recv_sem=rs,
            device_id=(sp, tp), device_id_type=MESH,
        )

    first_head = jnp.where(c == half, 1 - low, c)

    def head_at(i):
        return first_head if i == 0 else 1 - first_head

    def weight_copy(i, part):
        l = head_at(i)
        return pltpu.make_async_copy(
            (qw, kw, vw)[part].at[:, pl.ds(pl.multiple_of(l * 256, 256), 256)],
            WP.at[l, :, part * 256:(part + 1) * 256], w_sem.at[i, part],
        )

    def own_act():
        return pltpu.make_async_copy(act, A.at[t], own_sem.at[0])

    def own_ow():
        return pltpu.make_async_copy(ow, W.at[pl.ds(t * L, L)], own_sem.at[1])

    def act_across():
        return remote(A.at[t], A.at[t], a_send.at[0], a_recv.at[t], s, across)

    def act_mate():
        return remote(A.at[t], A.at[t], a_send.at[1], a_recv.at[t], s, mate)

    def act_pass():
        return remote(A.at[across], A.at[across], a_send.at[2], a_recv.at[across], s, mate)

    def wait_act(i):
        remote(A.at[i], A.at[i], a_send.at[0], a_recv.at[i], s, mate).wait_recv()

    cut = VALUE // 4
    order = (0, 2, 3, 1)

    def slab(owner, l, k):
        return W.at[owner * L + l, pl.ds(k * cut, cut)]

    def ow_across(k):
        l, q = (side, order[k]) if k < 4 else (1 - side, 1)
        return remote(
            ow.at[l, pl.ds(q * cut, cut)], slab(t, l, q), ox_send.at[k], ox_recv.at[k], s, across
        )

    def ow_side(k, l):
        part = slab(across, l, order[k])
        target = beside if k == 0 else pair
        return remote(part, part, oy_send.at[k], oy_recv.at[k], target, t)

    def ow_pass(k):
        l, q = (side, order[k]) if k < 4 else (1 - side, (1, 0, 2, 3)[k - 4])
        part = slab(across, l, q)
        return remote(part, part, m_send.at[k], m_recv.at[k], s, mate)

    def ow_mate():
        return remote(ow, W.at[pl.ds(t * L, L)], m_send.at[8], m_recv.at[8], s, mate)

    def lam_out():
        return remote(LS, LB, lam_send.at[0], lam_recv.at[0], s, mate)

    barrier = pltpu.get_barrier_semaphore()
    own_act().start()
    for i in range(L):
        for part in range(3):
            weight_copy(i, part).start()
    greeted = [(beside, t)]
    for i in range(Z):
        row = ((z + i) % Z) * Y + y
        greeted += [(row, mate), (row, across)] + ([(row, t)] if i > 0 else [])
    for sp, tp in greeted:
        pl.semaphore_signal(barrier, inc=1, device_id=(sp, tp), device_id_type=MESH)
    own_ow().start()
    for l in range(L):
        LS[l] = jnp.full((8, 128), lam_in[l], jnp.float32)
    MX[...] = jnp.full(MX.shape, very_low, jnp.float32)
    DN[...] = jnp.zeros(DN.shape, jnp.float32)
    ACC[...] = jnp.zeros(ACC.shape, jnp.float32)
    own_act().wait()
    pl.semaphore_wait(barrier, len(greeted))

    act_across().start()
    act_mate().start()
    for k in range(5):
        ow_across(k).start()

    def piece_sp(l):
        return (c * L + l) * Y + y

    def piece(l, xx, d):
        return remote(
            PR.at[l, xx, d], PC.at[z, xx], p_send.at[l, xx, d], p_recv.at[z, xx],
            piece_sp(l), x * 2 + d,
        )

    def stays(l, d):
        return (piece_sp(l) == s) & (c == d)

    def send_piece(l, xx, d):
        @pl.when(stays(l, d))
        def _():
            pltpu.make_async_copy(PR.at[l, xx, d], PC.at[z, xx], p_recv.at[z, xx]).start()

        @pl.when(jnp.logical_not(stays(l, d)))
        def _():
            piece(l, xx, d).start()

    def project(xx, i):
        l = head_at(i)
        rows = A[pl.ds(xx * 2, 2)].reshape(2 * R, A.shape[2])
        got = jnp.dot(rows, WP[l], preferred_element_type=jnp.float32)
        PR[l, xx, :, :, :256] = (got[:, :256] * scale).astype(jnp.bfloat16).reshape(2, R, 256)
        PR[l, xx, :, :, 256:] = got[:, 256:].astype(jnp.bfloat16).reshape(2, R, 512)
        for d in range(2):
            send_piece(l, xx, d)

    def kv_rows(row, zs, xx, core):
        return pl.ds(((zs * Y + row) * T + xx * 2 + core) * R, R)

    def kv_part(zs, xx):
        return PC.at[zs, xx, :, 256:768]

    def to_beside(zs, xx):
        return remote(
            kv_part(zs, xx), KV.at[kv_rows(y, zs, xx, c)],
            f_send.at[0, zs, xx], f_recv.at[0, zs, xx], beside, t,
        )

    def to_mate(zs, xx):
        return remote(
            kv_part(zs, xx), KV.at[kv_rows(y, zs, xx, c)],
            f_send.at[1, zs, xx], f_recv.at[1, zs, xx], s, mate,
        )

    def to_mate_again(zs, xx):
        part = KV.at[kv_rows(1 - y, zs, xx, c)]
        return remote(part, part, f_send.at[2, zs, xx], f_recv.at[2, zs, xx], s, mate)

    def to_self(zs, xx):
        return pltpu.make_async_copy(
            kv_part(zs, xx), KV.at[kv_rows(y, zs, xx, c)], f_recv.at[3, zs, xx]
        )

    def forward(zs, xx):
        remote(PR.at[0, 0, 0], PC.at[zs, xx], p_send.at[0, 0, 0], p_recv.at[zs, xx], s, mate).wait_recv()
        to_beside(zs, xx).start()
        to_mate(zs, xx).start()
        to_self(zs, xx).start()

    def relay(zs, xx):
        to_beside(zs, xx).wait_recv()
        to_mate_again(zs, xx).start()

    def wait_plane(zs):
        for xx in range(X):
            to_self(zs, xx).wait()
            to_mate(zs, xx).wait_recv()
            to_mate_again(zs, xx).wait_recv()

    q_rows = X * R
    k_rows = Y * span

    def chunk(i, j):
        row = lax.broadcasted_iota(jnp.int32, (q_rows, 1), 0)
        col = lax.broadcasted_iota(jnp.int32, (q_rows, k_rows), 1)
        pos = row + jnp.where(row >= R, R, 0) + (y * span + c * R + (i - j) * k_rows)
        seen = col <= pos
        values = KV[pl.ds(j * k_rows, k_rows), 256:512]
        for m in range(2):
            q = PC[i, :, :, m * 128:(m + 1) * 128].reshape(q_rows, 128)
            keys = KV[pl.ds(j * k_rows, k_rows), m * 128:(m + 1) * 128]
            sc = lax.dot_general(
                q, keys, (((1,), (1,)), ((), ())), preferred_element_type=jnp.float32
            )
            sc = jnp.where(seen, sc, very_low)
            old = MX[i, m, :, :1]
            new = jnp.maximum(old, jnp.max(sc, axis=1, keepdims=True))
            p = jnp.exp2(sc - new)
            factor = jnp.exp2(old - new)
            total = DN[i, m, :, :1] * factor + jnp.sum(p, axis=1, keepdims=True)
            got = jnp.dot(p.astype(jnp.bfloat16), values, preferred_element_type=jnp.float32)
            ACC[i, m] = ACC[i, m] * factor + got
            MX[i, m] = jnp.broadcast_to(new, MX.shape[2:])
            DN[i, m] = jnp.broadcast_to(total, DN.shape[2:])

    def home(zs, xx):
        return remote(
            HO.at[zs, xx], HI.at[head], h_send.at[zs, xx], h_recv.at[head],
            zs * Y + y, xx * 2 + c,
        )

    def ends_here(zs, xx):
        return (zs == z) & (xx == x)

    def finish(i):
        mine = jnp.where(z // L == c, LS[z % L], LB[z % L])[:1, :1]
        comb = ACC[i, 0] / DN[i, 0, :, :1] - mine * (ACC[i, 1] / DN[i, 1, :, :1])
        inv = lax.rsqrt(jnp.mean(comb * comb, axis=1, keepdims=True) + norm_floor)
        HO[i] = (comb * inv * gain[...]).astype(jnp.bfloat16).reshape(X, R, VALUE)
        for k in range(X):
            xx = (x + 1 + k) % X

            @pl.when(ends_here(i, xx))
            def _():
                pltpu.make_async_copy(HO.at[i, xx], HI.at[head], h_recv.at[head]).start()

            @pl.when(jnp.logical_not(ends_here(i, xx)))
            def _():
                home(i, xx).start()

    for part in range(3):
        weight_copy(0, part).wait()
    wait_act(mate)
    project(x, 0)
    for part in range(3):
        weight_copy(1, part).wait()
    project(x, 1)
    lam_out().start()
    ow_mate().start()
    forward(z, x)
    relay(z, x)
    wait_act(across)
    act_pass().start()
    wait_act(diagonal)
    project(1 - x, 0)
    forward(near, x)
    project(1 - x, 1)
    forward(z, 1 - x)
    forward(outer, x)
    relay(near, x)
    relay(z, 1 - x)
    ow_across(0).wait_recv()
    ow_side(0, side).start()
    ow_pass(0).start()
    forward(near, 1 - x)
    relay(outer, x)
    forward(inner, x)
    relay(near, 1 - x)
    ow_across(1).wait_recv()
    ow_side(1, side).start()
    ow_pass(1).start()
    lam_out().wait_recv()
    wait_plane(z)
    wait_plane(near)

    def near_step(k, carry):
        @pl.when(k == 1)
        def _():
            relay(inner, x)
            ow_side(0, 1 - side).wait_recv()
            ow_pass(5).start()

        i = half * H + jnp.where(k == 0, 0, 1)
        chunk(i, half * H + k // 2)

        @pl.when((half == 0) & (k != 1))
        def _():
            finish(i)

        return carry

    lax.fori_loop(0, 3, near_step, 0)
    forward(outer, 1 - x)
    ow_across(2).wait_recv()
    ow_side(2, side).start()
    ow_pass(2).start()
    relay(outer, 1 - x)
    wait_plane(outer)

    def outer_step(k, carry):
        @pl.when(k == 2)
        def _():
            forward(inner, 1 - x)

        i = jnp.where(half == 0, Z - 1, jnp.where(k == 0, 0, k + 1))
        j = jnp.where(half == 0, jnp.where(k == 0, Z - 1, k - 1), 0)
        chunk(i, j)

        @pl.when((half == 1) & (k == 0))
        def _():
            finish(i)

        return carry

    lax.fori_loop(0, 3, outer_step, 0)
    ow_across(3).wait_recv()
    ow_pass(3).start()
    relay(inner, 1 - x)
    ow_side(1, 1 - side).wait_recv()
    ow_pass(6).start()
    wait_plane(inner)

    def inner_step(k, carry):
        @pl.when(k == 3)
        def _():
            ow_across(4).wait_recv()
            ow_pass(4).start()

        i = jnp.where(k < 2, inner, jnp.where((half == 0) & (k == 2), inner, k))
        j = jnp.where(k == 0, inner, jnp.where(k == 1, 0, jnp.where((half == 0) & (k == 3), inner, 1)))
        chunk(i, j)

        @pl.when((half == 1) & (k > 0) | (k > 1))
        def _():
            finish(i)

        return carry

    lax.fori_loop(0, 4, inner_step, 0)

    own_ow().wait()
    ow_mate().wait_recv()
    ow_side(2, 1 - side).wait_recv()
    ow_pass(7).start()
    TOT[...] = jnp.zeros(TOT.shape, jnp.float32)

    def add_head(i, carry):
        @pl.when(i == 2)
        def _():
            for k in range(8):
                ow_pass(k).wait_recv()

        plane = (half * H + i // 4 * H + i % 2) % Z
        h = ((x + i // 2) % 2) * 2 * L + plane
        remote(HO.at[0, 0], HI.at[h], h_send.at[0, 0], h_recv.at[h], s, mate).wait_recv()
        TOT[...] += jnp.dot(HI[h], W[h], preferred_element_type=jnp.float32)
        return carry

    lax.fori_loop(0, T * L, add_head, 0)
    out[...] = TOT[...].astype(jnp.bfloat16)

    act_across().wait_send()
    act_mate().wait_send()
    act_pass().wait_send()
    ow_mate().wait_send()
    for k in range(5):
        ow_across(k).wait_send()
    for k in range(3):
        ow_side(k, side).wait_send()
    for k in range(8):
        ow_pass(k).wait_send()
    lam_out().wait_send()
    for l in range(L):
        for xx in range(X):
            for d in range(2):
                @pl.when(jnp.logical_not(stays(l, d)))
                def _():
                    piece(l, xx, d).wait_send()

    def drain(zs, carry):
        for xx in range(X):
            to_beside(zs, xx).wait_send()
            to_mate(zs, xx).wait_send()
            to_mate_again(zs, xx).wait_send()

            @pl.when(jnp.logical_not(ends_here(zs, xx)))
            def _():
                home(zs, xx).wait_send()

        return carry

    lax.fori_loop(0, Z, drain, 0)


def fused(S, T, L, activations, query_weight, key_weight, value_weight, out_weight, lambdas, head_gain):
    R, D = activations.shape
    X, Y = 2, 2
    Z = S // Y
    bf, f32 = jnp.bfloat16, jnp.float32
    vmem = pl.BlockSpec(memory_space=pltpu.VMEM)
    hbm = pl.BlockSpec(memory_space=pl.ANY)
    smem = pl.BlockSpec(memory_space=pltpu.SMEM)
    dma = pltpu.SemaphoreType.DMA
    width = query_weight.shape[1]
    return pl.pallas_call(
        functools.partial(layer_kernel, S, T, L, R),
        out_shape=jax.ShapeDtypeStruct((R, D), bf),
        in_specs=[hbm, hbm, hbm, hbm, hbm, smem, vmem],
        out_specs=vmem,
        scratch_shapes=[
            pltpu.VMEM((T, R, D), bf),
            pltpu.VMEM((L, D, 3 * width // L), bf),
            pltpu.VMEM((T * L, VALUE, D), bf),
            pltpu.VMEM((L, X, 2, R, 768), bf),
            pltpu.VMEM((Z, X, R, 768), bf),
            pltpu.VMEM((S * T * R, 512), bf),
            pltpu.VMEM((Z, X, R, VALUE), bf),
            pltpu.VMEM((T * L, R, VALUE), bf),
            pltpu.VMEM((L, 8, 128), f32),
            pltpu.VMEM((L, 8, 128), f32),
            pltpu.VMEM((Z, 2, X * R, VALUE), f32),
            pltpu.VMEM((Z, 2, X * R, 128), f32),
            pltpu.VMEM((Z, 2, X * R, 128), f32),
            pltpu.VMEM((R, D), f32),
            dma((L, 3)), dma((2,)),
            dma((3,)), dma((T,)),
            dma((1,)), dma((1,)),
            dma((5,)), dma((5,)), dma((3,)), dma((3,)), dma((9,)), dma((9,)),
            dma((L, X, 2)), dma((Z, X)),
            dma((3, Z, X)), dma((4, Z, X)),
            dma((Z, X)), dma((T * L,)),
        ],
        compiler_params=pltpu.CompilerParams(
            has_side_effects=True, collective_id=0, vmem_limit_bytes=60 * 1024 * 1024
        ),
    )(
        activations, query_weight, key_weight, value_weight,
        out_weight.reshape(L, VALUE, D), lambdas, head_gain.reshape(1, VALUE),
    )


def empty_state(count, local_heads):
    return (
        jnp.full((local_heads, 2, count), very_low, jnp.float32),
        jnp.zeros((local_heads, 2, count), jnp.float32),
        jnp.zeros((local_heads, 2, count, VALUE), jnp.float32),
    )


def absorb(state, query_set, query_pos, key_block, value_block, key_first):
    running, denoms, accums = state
    local_heads = running.shape[0]
    span = key_block.shape[0]
    key_grid = key_block.reshape(span, local_heads, 2, HEAD)
    scores = jnp.einsum(
        "qhme,khme->hmqk", query_set, key_grid, preferred_element_type=jnp.float32
    ) * HEAD ** (-0.5)
    key_pos = key_first + jnp.arange(span, dtype=jnp.int32)
    allowed = key_pos[None, :] <= query_pos[:, None]
    masked = jnp.where(allowed, scores, very_low)
    updated = jnp.maximum(running, jnp.max(masked, axis=-1))
    exp_weights = jnp.where(allowed, jnp.exp(masked - updated[..., None]), 0.0)
    factor = jnp.exp(running - updated)
    denoms = denoms * factor + jnp.sum(exp_weights, axis=-1)
    value_grid = value_block.reshape(span, local_heads, VALUE)
    product = jnp.einsum(
        "hmqk,khv->hmqv",
        exp_weights.astype(jnp.bfloat16),
        value_grid,
        preferred_element_type=jnp.float32,
    )
    accums = accums * factor[..., None] + product
    return (updated, denoms, accums)


def make_folder(query_sets, carry, pieces):
    key_piece, value_piece = pieces
    length = key_piece.shape[0]
    span = math.gcd(length, 512)

    def one_span(span_index, states):
        offset = span_index * span
        key_block = lax.dynamic_slice_in_dim(key_piece, offset, span, 0)
        value_block = lax.dynamic_slice_in_dim(value_piece, offset, span, 0)
        fresh = []
        for state, query_entry in zip(states, query_sets):
            query_set, query_pos = query_entry

            def take(current):
                return absorb(current, query_set, query_pos, key_block, value_block, offset)

            def leave(current):
                return current

            fresh.append(lax.cond(offset <= query_pos[-1], take, leave, state))
        return tuple(fresh)

    return lax.fori_loop(0, length // span, one_span, carry)


def shards(activations, query_weight, key_weight, value_weight, out_weight, lambdas, head_gain):
    local_heads = lambdas.shape[0]
    query_width = query_weight.shape[1]
    joined_weight = jnp.concatenate([query_weight, key_weight, value_weight], axis=1)
    projected = jnp.dot(
        lax.all_gather(activations, "tp", axis=0, tiled=True),
        joined_weight,
        preferred_element_type=jnp.float32,
    ).astype(jnp.bfloat16)
    row_count = projected.shape[0]
    queries = projected[:, :query_width].reshape(row_count, local_heads, 2, HEAD)
    key_rows = projected[:, query_width : 2 * query_width]
    value_rows = projected[:, 2 * query_width :]
    position = lax.axis_index("sp") * row_count + jnp.arange(row_count, dtype=jnp.int32)
    query_sets = [(queries, position)]
    start_states = tuple((empty_state(entry[0].shape[0], local_heads) for entry in query_sets))
    finals = make_folder(
        query_sets,
        start_states,
        (
            lax.all_gather(key_rows, "sp", axis=0, tiled=True),
            lax.all_gather(value_rows, "sp", axis=0, tiled=True),
        ),
    )
    outputs = []
    for state in finals:
        running, denoms, accums = state
        combined = (
            accums[:, 0] / denoms[:, 0, :, None]
            - lambdas[:, None, None] * accums[:, 1] / denoms[:, 1, :, None]
        )
        inverse_rms = lax.rsqrt(jnp.mean(combined * combined, axis=-1, keepdims=True) + norm_floor)
        normed = (combined * inverse_rms * head_gain).astype(jnp.bfloat16)
        outputs.append(
            jnp.transpose(normed, (1, 0, 2)).reshape(normed.shape[1], local_heads * VALUE)
        )
    heads_out = outputs[0]
    return lax.psum_scatter(
        jnp.dot(heads_out, out_weight, preferred_element_type=jnp.float32).astype(jnp.bfloat16),
        "tp",
        scatter_dimension=0,
        tiled=True,
    )


def solution(mesh):
    in_specs = (
        P(("sp", "tp"), None),
        P(None, "tp"),
        P(None, "tp"),
        P(None, "tp"),
        P("tp", None),
        P("tp"),
        P(),
    )
    out_specs = P(("sp", "tp"), None)
    S, T = mesh.shape["sp"], mesh.shape["tp"]

    def layer(*args):
        L = args[5].shape[0] // T
        rows = args[0].shape[0] // (S * T)
        fits = T == 4 and L == 2 and S == L * T and rows % 16 == 0
        local = functools.partial(fused, S, T, L) if fits else shards
        return jax.shard_map(
            local, mesh=mesh, in_specs=in_specs, out_specs=out_specs, check_vma=False
        )(*args)

    return layer
```

```python
import functools
import math

import jax
import jax.numpy as jnp
from jax import lax
from jax.experimental import pallas as pl
from jax.experimental.pallas import tpu as pltpu
from jax.sharding import PartitionSpec as P

HEAD = 128
VALUE = 256


norm_floor = 0.02
very_low = -1e30
MESH = pl.DeviceIdType.MESH


def layer_kernel(
    S, T, L, R,
    act, qw, kw, vw, ow, lam_in, gain,
    out,
    A, WP, W, PR, PC, KV, HO, HI, LS, LB, ACC, MX, DN, TOT,
    w_sem, own_sem, a_send, a_recv, lam_send, lam_recv,
    ox_send, ox_recv, oy_send, oy_recv, m_send, m_recv,
    p_send, p_recv, f_send, f_recv, h_send, h_recv,
):
    X, Y = 2, 2
    Z = S // Y
    H = Z // 2
    s = lax.axis_index("sp")
    t = lax.axis_index("tp")
    x = t // 2
    c = t % 2
    y = s % Y
    z = s // Y
    half = z // H
    low = z % H
    mate = x * 2 + (1 - c)
    across = (1 - x) * 2 + c
    diagonal = (1 - x) * 2 + (1 - c)
    beside = z * Y + (1 - y)
    pair = (half * H + 1 - low) * Y + y
    side = (low + y) % 2
    near = half * H + 1 - low
    third = (1 - half) * H
    last = third + 1
    edge = (z == 0) | (z == Z - 1)
    early = jnp.where(edge, third, near)
    later = jnp.where(edge, near, third)
    held = (z == Z - 1) & (c != half)
    head = x * 2 * L + z
    span = T * R
    scale = HEAD ** (-0.5) * math.log2(math.e)

    def remote(src, dst, ss, rs, sp, tp):
        return pltpu.make_async_remote_copy(
            src_ref=src, dst_ref=dst, send_sem=ss, recv_sem=rs,
            device_id=(sp, tp), device_id_type=MESH,
        )

    first_head = jnp.where(c == half, 1 - low, c)

    def head_at(i):
        return first_head if i == 0 else 1 - first_head

    def weight_copy(i, part):
        l = head_at(i)
        return pltpu.make_async_copy(
            (qw, kw, vw)[part].at[:, pl.ds(pl.multiple_of(l * 256, 256), 256)],
            WP.at[l, :, part * 256:(part + 1) * 256], w_sem.at[i, part],
        )

    def own_act():
        return pltpu.make_async_copy(act, A.at[t], own_sem.at[0])

    def own_ow():
        return pltpu.make_async_copy(ow, W.at[pl.ds(t * L, L)], own_sem.at[1])

    def act_across():
        return remote(A.at[t], A.at[t], a_send.at[0], a_recv.at[t], s, across)

    def act_mate():
        return remote(A.at[t], A.at[t], a_send.at[1], a_recv.at[t], s, mate)

    def act_pass():
        return remote(A.at[across], A.at[across], a_send.at[2], a_recv.at[across], s, mate)

    def wait_act(i):
        remote(A.at[i], A.at[i], a_send.at[0], a_recv.at[i], s, mate).wait_recv()

    cut = VALUE // 4
    order = (0, 2, 3, 1)

    def slab(owner, l, k):
        return W.at[owner * L + l, pl.ds(k * cut, cut)]

    def ow_across(k):
        l, q = (side, order[k]) if k < 4 else (1 - side, 1)
        return remote(
            ow.at[l, pl.ds(q * cut, cut)], slab(t, l, q), ox_send.at[k], ox_recv.at[k], s, across
        )

    def ow_side(k, l):
        part = slab(across, l, order[k])
        target = beside if k == 0 else pair
        return remote(part, part, oy_send.at[k], oy_recv.at[k], target, t)

    def ow_pass(k):
        l, q = (side, order[k]) if k < 4 else (1 - side, (1, 0, 2, 3)[k - 4])
        part = slab(across, l, q)
        return remote(part, part, m_send.at[k], m_recv.at[k], s, mate)

    def ow_mate():
        return remote(ow, W.at[pl.ds(t * L, L)], m_send.at[8], m_recv.at[8], s, mate)

    def lam_out():
        return remote(LS, LB, lam_send.at[0], lam_recv.at[0], s, mate)

    barrier = pltpu.get_barrier_semaphore()
    own_act().start()
    greeted = [(beside, t)]
    for i in range(Z):
        row = ((z + i) % Z) * Y + y
        greeted += [(row, mate), (row, across)] + ([(row, t)] if i > 0 else [])
    for sp, tp in greeted:
        pl.semaphore_signal(barrier, inc=1, device_id=(sp, tp), device_id_type=MESH)
    for l in range(L):
        LS[l] = jnp.full((8, 128), lam_in[l], jnp.float32)
    own_act().wait()
    for i in range(L):
        for part in range(3):
            weight_copy(i, part).start()
    own_ow().start()
    pl.semaphore_wait(barrier, len(greeted))

    act_across().start()
    act_mate().start()
    for k in range(5):
        ow_across(k).start()

    def piece_sp(l):
        return (c * L + l) * Y + y

    def piece(l, xx, d):
        return remote(
            PR.at[l, xx, d], PC.at[z, xx], p_send.at[l, xx, d], p_recv.at[z, xx],
            piece_sp(l), x * 2 + d,
        )

    def stays(l, d):
        return (piece_sp(l) == s) & (c == d)

    def send_piece(l, xx, d):
        @pl.when(stays(l, d))
        def _():
            pltpu.make_async_copy(PR.at[l, xx, d], PC.at[z, xx], p_recv.at[z, xx]).start()

        @pl.when(jnp.logical_not(stays(l, d)))
        def _():
            piece(l, xx, d).start()

    def project(xx, i):
        l = head_at(i)
        rows = A[pl.ds(xx * 2, 2)].reshape(2 * R, A.shape[2])
        got = jnp.dot(rows, WP[l], preferred_element_type=jnp.float32)
        PR[l, xx, :, :, :256] = (got[:, :256] * scale).astype(jnp.bfloat16).reshape(2, R, 256)
        PR[l, xx, :, :, 256:] = got[:, 256:].astype(jnp.bfloat16).reshape(2, R, 512)

        @pl.when(jnp.logical_not(held))
        def _():
            for d in range(2):
                send_piece(l, xx, d)

    def send_held(xx):
        @pl.when(held)
        def _():
            for i in range(L):
                for d in range(2):
                    piece(head_at(i), xx, d).start()

    def kv_rows(row, zs, xx, core):
        return pl.ds(((zs * Y + row) * T + xx * 2 + core) * R, R)

    def kv_part(zs, xx):
        return PC.at[zs, xx, :, 256:768]

    def to_beside(zs, xx):
        return remote(
            kv_part(zs, xx), KV.at[kv_rows(y, zs, xx, c)],
            f_send.at[0, zs, xx], f_recv.at[0, zs, xx], beside, t,
        )

    def to_mate(zs, xx):
        return remote(
            kv_part(zs, xx), KV.at[kv_rows(y, zs, xx, c)],
            f_send.at[1, zs, xx], f_recv.at[1, zs, xx], s, mate,
        )

    def to_mate_again(zs, xx):
        part = KV.at[kv_rows(1 - y, zs, xx, c)]
        return remote(part, part, f_send.at[2, zs, xx], f_recv.at[2, zs, xx], s, mate)

    def to_self(zs, xx):
        return pltpu.make_async_copy(
            kv_part(zs, xx), KV.at[kv_rows(y, zs, xx, c)], f_recv.at[3, zs, xx]
        )

    def forward(zs, xx):
        remote(PR.at[0, 0, 0], PC.at[zs, xx], p_send.at[0, 0, 0], p_recv.at[zs, xx], s, mate).wait_recv()
        to_beside(zs, xx).start()
        to_mate(zs, xx).start()
        to_self(zs, xx).start()

    def relay(zs, xx):
        to_beside(zs, xx).wait_recv()
        to_mate_again(zs, xx).start()

    def wait_plane(zs):
        for xx in range(X):
            to_self(zs, xx).wait()
            to_mate(zs, xx).wait_recv()
            to_mate_again(zs, xx).wait_recv()

    q_rows = X * R
    k_rows = Y * span

    def chunk(i, j):
        row = lax.broadcasted_iota(jnp.int32, (q_rows, 1), 0)
        col = lax.broadcasted_iota(jnp.int32, (q_rows, k_rows), 1)
        pos = row + jnp.where(row >= R, R, 0) + (y * span + c * R + (i - j) * k_rows)
        seen = col <= pos
        values = KV[pl.ds(j * k_rows, k_rows), 256:512]
        for m in range(2):
            q = PC[i, :, :, m * 128:(m + 1) * 128].reshape(q_rows, 128)
            keys = KV[pl.ds(j * k_rows, k_rows), m * 128:(m + 1) * 128]
            sc = lax.dot_general(
                q, keys, (((1,), (1,)), ((), ())), preferred_element_type=jnp.float32
            )
            sc = jnp.where(seen, sc, very_low)
            old = MX[i, m, :, :1]
            new = jnp.maximum(old, jnp.max(sc, axis=1, keepdims=True))
            p = jnp.exp2(sc - new)
            factor = jnp.exp2(old - new)
            total = DN[i, m, :, :1] * factor + jnp.sum(p, axis=1, keepdims=True)
            got = jnp.dot(p.astype(jnp.bfloat16), values, preferred_element_type=jnp.float32)
            ACC[i, m] = ACC[i, m] * factor + got
            MX[i, m] = jnp.broadcast_to(new, MX.shape[2:])
            DN[i, m] = jnp.broadcast_to(total, DN.shape[2:])

    def home(zs, xx):
        return remote(
            HO.at[zs, xx], HI.at[head], h_send.at[zs, xx], h_recv.at[head],
            zs * Y + y, xx * 2 + c,
        )

    def ends_here(zs, xx):
        return (zs == z) & (xx == x)

    def finish(i):
        mine = jnp.where(z // L == c, LS[z % L], LB[z % L])[:1, :1]
        comb = ACC[i, 0] / DN[i, 0, :, :1] - mine * (ACC[i, 1] / DN[i, 1, :, :1])
        inv = lax.rsqrt(jnp.mean(comb * comb, axis=1, keepdims=True) + norm_floor)
        HO[i] = (comb * inv * gain[...]).astype(jnp.bfloat16).reshape(X, R, VALUE)
        for k in range(X):
            xx = (x + 1 + k) % X

            @pl.when(ends_here(i, xx))
            def _():
                pltpu.make_async_copy(HO.at[i, xx], HI.at[head], h_recv.at[head]).start()

            @pl.when(jnp.logical_not(ends_here(i, xx)))
            def _():
                home(i, xx).start()

    for part in range(3):
        weight_copy(0, part).wait()
    wait_act(mate)
    project(x, 0)
    for part in range(3):
        weight_copy(1, part).wait()
    project(x, 1)
    forward(z, x)
    lam_out().start()
    ow_mate().start()
    MX[...] = jnp.full(MX.shape, very_low, jnp.float32)
    DN[...] = jnp.zeros(DN.shape, jnp.float32)
    ACC[...] = jnp.zeros(ACC.shape, jnp.float32)
    forward(early, x)
    send_held(x)
    relay(z, x)
    wait_act(across)
    act_pass().start()
    forward(later, x)
    wait_act(diagonal)
    project(1 - x, 0)
    project(1 - x, 1)
    forward(z, 1 - x)
    relay(early, x)
    relay(later, x)
    forward(last, x)
    forward(near, 1 - x)
    relay(z, 1 - x)
    send_held(1 - x)
    forward(third, 1 - x)
    ow_across(0).wait_recv()
    ow_side(0, side).start()
    ow_pass(0).start()
    ow_across(1).wait_recv()
    ow_side(1, side).start()
    ow_pass(1).start()
    relay(last, x)
    relay(near, 1 - x)
    lam_out().wait_recv()
    wait_plane(z)
    wait_plane(near)

    def near_step(k, carry):
        i = half * H + jnp.where(k == 0, 0, 1)
        chunk(i, half * H + k // 2)

        @pl.when((half == 0) & (k != 1))
        def _():
            finish(i)

        return carry

    lax.fori_loop(0, 3, near_step, 0)
    relay(third, 1 - x)
    ow_across(2).wait_recv()
    ow_side(2, side).start()
    ow_pass(2).start()
    wait_plane(third)

    def third_step(k, carry):
        i = jnp.where(half == 0, H, jnp.where(k == 0, 0, k + 1))
        chunk(i, jnp.where(half == 0, k, 0))

        @pl.when(k == 0)
        def _():
            forward(last, 1 - x)

        @pl.when(jnp.where(half == 0, k == 2, k == 0))
        def _():
            finish(i)

        return carry

    lax.fori_loop(0, 3, third_step, 0)

    def last_step(k, carry):
        @pl.when(k == 1)
        def _():
            relay(last, 1 - x)

        @pl.when(k == jnp.where(half == 0, 3, 1))
        def _():
            wait_plane(last)

        i = jnp.where(half == 0, last, jnp.where(k == 0, last, k))
        chunk(i, jnp.where(half == 0, k, jnp.where(k == 0, 0, last)))

        @pl.when(jnp.where(half == 0, k == 3, k > 0))
        def _():
            finish(i)

        return carry

    lax.fori_loop(0, 4, last_step, 0)
    ow_across(3).wait_recv()
    ow_pass(3).start()
    ow_side(0, 1 - side).wait_recv()
    ow_pass(5).start()
    ow_side(1, 1 - side).wait_recv()
    ow_pass(6).start()
    ow_across(4).wait_recv()
    ow_pass(4).start()
    ow_side(2, 1 - side).wait_recv()
    ow_pass(7).start()
    act_across().wait_send()
    act_mate().wait_send()
    act_pass().wait_send()
    ow_mate().wait_send()
    for k in range(5):
        ow_across(k).wait_send()
    for k in range(3):
        ow_side(k, side).wait_send()
    lam_out().wait_send()
    for l in range(L):
        for xx in range(X):
            for d in range(2):
                @pl.when(jnp.logical_not(stays(l, d)))
                def _():
                    piece(l, xx, d).wait_send()

    def settle(zs, carry):
        for xx in range(X):
            to_beside(zs, xx).wait_send()
            to_mate(zs, xx).wait_send()
            to_mate_again(zs, xx).wait_send()

        return carry

    lax.fori_loop(0, Z, settle, 0)
    own_ow().wait()
    ow_mate().wait_recv()
    TOT[...] = jnp.zeros(TOT.shape, jnp.float32)

    def add_head(i, carry):
        @pl.when(i == 2)
        def _():
            for k in range(8):
                ow_pass(k).wait_recv()

        plane = (half * H + i // 4 * H + i % 2) % Z
        h = ((x + i // 2) % 2) * 2 * L + plane
        remote(HO.at[0, 0], HI.at[h], h_send.at[0, 0], h_recv.at[h], s, mate).wait_recv()
        TOT[...] += jnp.dot(HI[h], W[h], preferred_element_type=jnp.float32)
        return carry

    lax.fori_loop(0, T * L, add_head, 0)
    for k in range(8):
        ow_pass(k).wait_send()
    out[...] = TOT[...].astype(jnp.bfloat16)


    def drain(zs, carry):
        for xx in range(X):
            @pl.when(jnp.logical_not(ends_here(zs, xx)))
            def _():
                home(zs, xx).wait_send()

        return carry

    lax.fori_loop(0, Z, drain, 0)


def fused(S, T, L, activations, query_weight, key_weight, value_weight, out_weight, lambdas, head_gain):
    R, D = activations.shape
    X, Y = 2, 2
    Z = S // Y
    bf, f32 = jnp.bfloat16, jnp.float32
    vmem = pl.BlockSpec(memory_space=pltpu.VMEM)
    hbm = pl.BlockSpec(memory_space=pl.ANY)
    smem = pl.BlockSpec(memory_space=pltpu.SMEM)
    dma = pltpu.SemaphoreType.DMA
    width = query_weight.shape[1]
    return pl.pallas_call(
        functools.partial(layer_kernel, S, T, L, R),
        out_shape=jax.ShapeDtypeStruct((R, D), bf),
        in_specs=[hbm, hbm, hbm, hbm, hbm, smem, vmem],
        out_specs=vmem,
        scratch_shapes=[
            pltpu.VMEM((T, R, D), bf),
            pltpu.VMEM((L, D, 3 * width // L), bf),
            pltpu.VMEM((T * L, VALUE, D), bf),
            pltpu.VMEM((L, X, 2, R, 768), bf),
            pltpu.VMEM((Z, X, R, 768), bf),
            pltpu.VMEM((S * T * R, 512), bf),
            pltpu.VMEM((Z, X, R, VALUE), bf),
            pltpu.VMEM((T * L, R, VALUE), bf),
            pltpu.VMEM((L, 8, 128), f32),
            pltpu.VMEM((L, 8, 128), f32),
            pltpu.VMEM((Z, 2, X * R, VALUE), f32),
            pltpu.VMEM((Z, 2, X * R, 128), f32),
            pltpu.VMEM((Z, 2, X * R, 128), f32),
            pltpu.VMEM((R, D), f32),
            dma((L, 3)), dma((2,)),
            dma((3,)), dma((T,)),
            dma((1,)), dma((1,)),
            dma((5,)), dma((5,)), dma((3,)), dma((3,)), dma((9,)), dma((9,)),
            dma((L, X, 2)), dma((Z, X)),
            dma((3, Z, X)), dma((4, Z, X)),
            dma((Z, X)), dma((T * L,)),
        ],
        compiler_params=pltpu.CompilerParams(
            has_side_effects=True, collective_id=0, vmem_limit_bytes=60 * 1024 * 1024
        ),
    )(
        activations, query_weight, key_weight, value_weight,
        out_weight.reshape(L, VALUE, D), lambdas, head_gain.reshape(1, VALUE),
    )


def empty_state(count, local_heads):
    return (
        jnp.full((local_heads, 2, count), very_low, jnp.float32),
        jnp.zeros((local_heads, 2, count), jnp.float32),
        jnp.zeros((local_heads, 2, count, VALUE), jnp.float32),
    )


def absorb(state, query_set, query_pos, key_block, value_block, key_first):
    running, denoms, accums = state
    local_heads = running.shape[0]
    span = key_block.shape[0]
    key_grid = key_block.reshape(span, local_heads, 2, HEAD)
    scores = jnp.einsum(
        "qhme,khme->hmqk", query_set, key_grid, preferred_element_type=jnp.float32
    ) * HEAD ** (-0.5)
    key_pos = key_first + jnp.arange(span, dtype=jnp.int32)
    allowed = key_pos[None, :] <= query_pos[:, None]
    masked = jnp.where(allowed, scores, very_low)
    updated = jnp.maximum(running, jnp.max(masked, axis=-1))
    exp_weights = jnp.where(allowed, jnp.exp(masked - updated[..., None]), 0.0)
    factor = jnp.exp(running - updated)
    denoms = denoms * factor + jnp.sum(exp_weights, axis=-1)
    value_grid = value_block.reshape(span, local_heads, VALUE)
    product = jnp.einsum(
        "hmqk,khv->hmqv",
        exp_weights.astype(jnp.bfloat16),
        value_grid,
        preferred_element_type=jnp.float32,
    )
    accums = accums * factor[..., None] + product
    return (updated, denoms, accums)


def make_folder(query_sets, carry, pieces):
    key_piece, value_piece = pieces
    length = key_piece.shape[0]
    span = math.gcd(length, 512)

    def one_span(span_index, states):
        offset = span_index * span
        key_block = lax.dynamic_slice_in_dim(key_piece, offset, span, 0)
        value_block = lax.dynamic_slice_in_dim(value_piece, offset, span, 0)
        fresh = []
        for state, query_entry in zip(states, query_sets):
            query_set, query_pos = query_entry

            def take(current):
                return absorb(current, query_set, query_pos, key_block, value_block, offset)

            def leave(current):
                return current

            fresh.append(lax.cond(offset <= query_pos[-1], take, leave, state))
        return tuple(fresh)

    return lax.fori_loop(0, length // span, one_span, carry)


def shards(activations, query_weight, key_weight, value_weight, out_weight, lambdas, head_gain):
    local_heads = lambdas.shape[0]
    query_width = query_weight.shape[1]
    joined_weight = jnp.concatenate([query_weight, key_weight, value_weight], axis=1)
    projected = jnp.dot(
        lax.all_gather(activations, "tp", axis=0, tiled=True),
        joined_weight,
        preferred_element_type=jnp.float32,
    ).astype(jnp.bfloat16)
    row_count = projected.shape[0]
    queries = projected[:, :query_width].reshape(row_count, local_heads, 2, HEAD)
    key_rows = projected[:, query_width : 2 * query_width]
    value_rows = projected[:, 2 * query_width :]
    position = lax.axis_index("sp") * row_count + jnp.arange(row_count, dtype=jnp.int32)
    query_sets = [(queries, position)]
    start_states = tuple((empty_state(entry[0].shape[0], local_heads) for entry in query_sets))
    finals = make_folder(
        query_sets,
        start_states,
        (
            lax.all_gather(key_rows, "sp", axis=0, tiled=True),
            lax.all_gather(value_rows, "sp", axis=0, tiled=True),
        ),
    )
    outputs = []
    for state in finals:
        running, denoms, accums = state
        combined = (
            accums[:, 0] / denoms[:, 0, :, None]
            - lambdas[:, None, None] * accums[:, 1] / denoms[:, 1, :, None]
        )
        inverse_rms = lax.rsqrt(jnp.mean(combined * combined, axis=-1, keepdims=True) + norm_floor)
        normed = (combined * inverse_rms * head_gain).astype(jnp.bfloat16)
        outputs.append(
            jnp.transpose(normed, (1, 0, 2)).reshape(normed.shape[1], local_heads * VALUE)
        )
    heads_out = outputs[0]
    return lax.psum_scatter(
        jnp.dot(heads_out, out_weight, preferred_element_type=jnp.float32).astype(jnp.bfloat16),
        "tp",
        scatter_dimension=0,
        tiled=True,
    )


def solution(mesh):
    in_specs = (
        P(("sp", "tp"), None),
        P(None, "tp"),
        P(None, "tp"),
        P(None, "tp"),
        P("tp", None),
        P("tp"),
        P(),
    )
    out_specs = P(("sp", "tp"), None)
    S, T = mesh.shape["sp"], mesh.shape["tp"]

    def layer(*args):
        L = args[5].shape[0] // T
        rows = args[0].shape[0] // (S * T)
        fits = T == 4 and L == 2 and S == L * T and rows % 16 == 0
        local = functools.partial(fused, S, T, L) if fits else shards
        return jax.shard_map(
            local, mesh=mesh, in_specs=in_specs, out_specs=out_specs, check_vma=False
        )(*args)

    return layer
```

```python
import functools
import math

import jax
import jax.numpy as jnp
from jax import lax
from jax.experimental import pallas as pl
from jax.experimental.pallas import tpu as pltpu
from jax.sharding import PartitionSpec as P

HEAD = 128
VALUE = 256


norm_floor = 0.02
very_low = -1e30
MESH = pl.DeviceIdType.MESH


def layer_kernel(
    S, T, L, R,
    act, qw, kw, vw, ow, lam_in, gain,
    out,
    A, WP, W, PR, PC, KV, HO, HI, LS, LB, ACC, MX, DN, TOT,
    w_sem, own_sem, a_send, a_recv, lam_send, lam_recv,
    ox_send, ox_recv, oy_send, oy_recv, m_send, m_recv,
    p_send, p_recv, f_send, f_recv, h_send, h_recv,
):
    X, Y = 2, 2
    Z = S // Y
    H = Z // 2
    s = lax.axis_index("sp")
    t = lax.axis_index("tp")
    x = t // 2
    c = t % 2
    y = s % Y
    z = s // Y
    half = z // H
    low = z % H
    mate = x * 2 + (1 - c)
    across = (1 - x) * 2 + c
    diagonal = (1 - x) * 2 + (1 - c)
    beside = z * Y + (1 - y)
    pair = (half * H + 1 - low) * Y + y
    side = (low + y) % 2
    near = half * H + 1 - low
    third = (1 - half) * H
    last = third + 1
    edge = (z == 0) | (z == Z - 1)
    ahead = (1 - half) * (Z - 1)
    behind = (1 - half) * H + half * (H - 1)
    early = jnp.where(edge, ahead, near)
    later = jnp.where(edge, near, ahead)
    held = (z == Z - 1) & (c != half)
    head = x * 2 * L + z
    span = T * R
    scale = HEAD ** (-0.5) * math.log2(math.e)

    def remote(src, dst, ss, rs, sp, tp):
        return pltpu.make_async_remote_copy(
            src_ref=src, dst_ref=dst, send_sem=ss, recv_sem=rs,
            device_id=(sp, tp), device_id_type=MESH,
        )

    first_head = jnp.where(c == half, 1 - low, c)

    def head_at(i):
        return first_head if i == 0 else 1 - first_head

    def weight_copy(i, part):
        l = head_at(i)
        return pltpu.make_async_copy(
            (qw, kw, vw)[part].at[:, pl.ds(pl.multiple_of(l * 256, 256), 256)],
            WP.at[l, :, part * 256:(part + 1) * 256], w_sem.at[i, part],
        )

    def own_act():
        return pltpu.make_async_copy(act, A.at[t], own_sem.at[0])

    def own_ow():
        return pltpu.make_async_copy(ow, W.at[pl.ds(t * L, L)], own_sem.at[1])

    def act_across():
        return remote(A.at[t], A.at[t], a_send.at[0], a_recv.at[t], s, across)

    def act_mate():
        return remote(A.at[t], A.at[t], a_send.at[1], a_recv.at[t], s, mate)

    def act_pass():
        return remote(A.at[across], A.at[across], a_send.at[2], a_recv.at[across], s, mate)

    def wait_act(i):
        remote(A.at[i], A.at[i], a_send.at[0], a_recv.at[i], s, mate).wait_recv()

    cut = VALUE // 4
    order = (0, 2, 3, 1)

    def slab(owner, l, k):
        return W.at[owner * L + l, pl.ds(k * cut, cut)]

    def ow_across(k):
        l, q = (side, order[k]) if k < 4 else (1 - side, 1)
        return remote(
            ow.at[l, pl.ds(q * cut, cut)], slab(t, l, q), ox_send.at[k], ox_recv.at[k], s, across
        )

    def ow_side(k, l):
        part = slab(across, l, order[k])
        target = beside if k == 2 else pair
        return remote(part, part, oy_send.at[k], oy_recv.at[k], target, t)

    def ow_pass(k):
        l, q = (side, order[k]) if k < 4 else (1 - side, (1, 0, 2, 3)[k - 4])
        part = slab(across, l, q)
        return remote(part, part, m_send.at[k], m_recv.at[k], s, mate)

    def ow_mate():
        return remote(ow, W.at[pl.ds(t * L, L)], m_send.at[8], m_recv.at[8], s, mate)

    def lam_out():
        return remote(LS, LB, lam_send.at[0], lam_recv.at[0], s, mate)

    barrier = pltpu.get_barrier_semaphore()
    own_act().start()
    for part in range(3):
        weight_copy(0, part).start()
    greeted = [(beside, t)]
    for i in range(Z):
        row = ((z + i) % Z) * Y + y
        greeted += [(row, mate), (row, across)] + ([(row, t)] if i > 0 else [])
    for sp, tp in greeted:
        pl.semaphore_signal(barrier, inc=1, device_id=(sp, tp), device_id_type=MESH)
    for l in range(L):
        LS[l] = jnp.full((8, 128), lam_in[l], jnp.float32)
    own_act().wait()
    for part in range(3):
        weight_copy(1, part).start()
    own_ow().start()
    pl.semaphore_wait(barrier, len(greeted))

    act_across().start()
    act_mate().start()
    for k in range(5):
        ow_across(k).start()

    def piece_sp(l):
        return (c * L + l) * Y + y

    def piece(l, xx, d):
        return remote(
            PR.at[l, xx, d], PC.at[z, xx], p_send.at[l, xx, d], p_recv.at[z, xx],
            piece_sp(l), x * 2 + d,
        )

    def stays(l, d):
        return (piece_sp(l) == s) & (c == d)

    def send_piece(l, xx, d):
        @pl.when(stays(l, d))
        def _():
            pltpu.make_async_copy(PR.at[l, xx, d], PC.at[z, xx], p_recv.at[z, xx]).start()

        @pl.when(jnp.logical_not(stays(l, d)))
        def _():
            piece(l, xx, d).start()

    def project(xx, i):
        l = head_at(i)
        rows = A[pl.ds(xx * 2, 2)].reshape(2 * R, A.shape[2])
        got = jnp.dot(rows, WP[l], preferred_element_type=jnp.float32)
        PR[l, xx, :, :, :256] = (got[:, :256] * scale).astype(jnp.bfloat16).reshape(2, R, 256)
        PR[l, xx, :, :, 256:] = got[:, 256:].astype(jnp.bfloat16).reshape(2, R, 512)

    def send(xx, i):
        for d in range(2):
            send_piece(head_at(i), xx, d)

    def kv_rows(row, zs, xx, core):
        return pl.ds(((zs * Y + row) * T + xx * 2 + core) * R, R)

    def kv_part(zs, xx):
        return PC.at[zs, xx, :, 256:768]

    def to_beside(zs, xx):
        return remote(
            kv_part(zs, xx), KV.at[kv_rows(y, zs, xx, c)],
            f_send.at[0, zs, xx], f_recv.at[0, zs, xx], beside, t,
        )

    def to_mate(zs, xx):
        return remote(
            kv_part(zs, xx), KV.at[kv_rows(y, zs, xx, c)],
            f_send.at[1, zs, xx], f_recv.at[1, zs, xx], s, mate,
        )

    def to_mate_again(zs, xx):
        part = KV.at[kv_rows(1 - y, zs, xx, c)]
        return remote(part, part, f_send.at[2, zs, xx], f_recv.at[2, zs, xx], s, mate)

    def to_self(zs, xx):
        return pltpu.make_async_copy(
            kv_part(zs, xx), KV.at[kv_rows(y, zs, xx, c)], f_recv.at[3, zs, xx]
        )

    def forward(zs, xx):
        remote(PR.at[0, 0, 0], PC.at[zs, xx], p_send.at[0, 0, 0], p_recv.at[zs, xx], s, mate).wait_recv()
        to_beside(zs, xx).start()
        to_mate(zs, xx).start()
        to_self(zs, xx).start()

    def relay(zs, xx):
        to_beside(zs, xx).wait_recv()
        to_mate_again(zs, xx).start()

    def wait_plane(zs):
        for xx in range(X):
            to_self(zs, xx).wait()
            to_mate(zs, xx).wait_recv()
            to_mate_again(zs, xx).wait_recv()

    q_rows = X * R
    k_rows = Y * span

    def chunk(i, j):
        row = lax.broadcasted_iota(jnp.int32, (q_rows, 128), 0)
        lane = lax.broadcasted_iota(jnp.int32, (q_rows, 128), 1)
        ahead_by = row + jnp.where(row >= R, R, 0) - lane + (y * span + c * R + (i - j) * k_rows)
        cols = range(0, k_rows, 128)
        for m in range(2):
            q = PC[i, :, :, m * 128:(m + 1) * 128].reshape(q_rows, 128)
            keys = KV[pl.ds(j * k_rows, k_rows), m * 128:(m + 1) * 128]
            sc = lax.dot_general(
                q, keys, (((1,), (1,)), ((), ())), preferred_element_type=jnp.float32
            )
            parts = [jnp.where(ahead_by >= b, sc[:, b:b + 128], very_low) for b in cols]
            top_part = functools.reduce(jnp.maximum, parts)
            old = MX[i, m]
            new = jnp.maximum(old, jnp.max(top_part, axis=1, keepdims=True))
            parts = [jnp.exp2(part - new) for part in parts]
            factor = jnp.exp2(old - new)
            DN[i, m] = DN[i, m] * factor + functools.reduce(jnp.add, parts)
            MX[i, m] = new
            p = jnp.concatenate([part.astype(jnp.bfloat16) for part in parts], axis=1)
            values = KV[pl.ds(j * k_rows, k_rows), 256:512]
            got = jnp.dot(p, values, preferred_element_type=jnp.float32)
            for b in range(0, VALUE, 128):
                ACC[i, m, :, b:b + 128] = ACC[i, m, :, b:b + 128] * factor + got[:, b:b + 128]

    def home(zs, xx):
        return remote(
            HO.at[zs, xx], HI.at[head], h_send.at[zs, xx], h_recv.at[head],
            zs * Y + y, xx * 2 + c,
        )

    def ends_here(zs, xx):
        return (zs == z) & (xx == x)

    def finish(i):
        mine = jnp.where(z // L == c, LS[z % L], LB[z % L])[:1, :1]
        dens = [jnp.sum(DN[i, m], axis=1, keepdims=True) for m in range(2)]
        comb = ACC[i, 0] * (1.0 / dens[0]) - ACC[i, 1] * (mine / dens[1])
        inv = lax.rsqrt(jnp.mean(comb * comb, axis=1, keepdims=True) + norm_floor)
        HO[i] = (comb * inv * gain[...]).astype(jnp.bfloat16).reshape(X, R, VALUE)
        for k in range(X):
            xx = (x + 1 + k) % X

            @pl.when(ends_here(i, xx))
            def _():
                pltpu.make_async_copy(HO.at[i, xx], HI.at[head], h_recv.at[head]).start()

            @pl.when(jnp.logical_not(ends_here(i, xx)))
            def _():
                home(i, xx).start()

    for part in range(3):
        weight_copy(0, part).wait()
    wait_act(mate)
    project(x, 0)
    send(x, 0)
    for part in range(3):
        weight_copy(1, part).wait()
    project(x, 1)
    send(x, 1)
    forward(z, x)
    lam_out().start()
    ow_mate().start()
    MX[...] = jnp.full(MX.shape, very_low, jnp.float32)
    DN[...] = jnp.zeros(DN.shape, jnp.float32)
    ACC[...] = jnp.zeros(ACC.shape, jnp.float32)
    forward(early, x)
    relay(z, x)
    wait_act(across)
    act_pass().start()
    forward(later, x)
    wait_act(diagonal)
    for i in range(L):
        project(1 - x, i)

        @pl.when(jnp.logical_not(held))
        def _():
            send(1 - x, i)

    forward(z, 1 - x)
    relay(early, x)
    relay(later, x)
    forward(behind, x)
    top = z == Z - 1
    sooner = jnp.where(top, third, near)
    after = jnp.where(top, near, third)
    forward(sooner, 1 - x)

    @pl.when(held)
    def _():
        for i in range(L):
            send(1 - x, i)

    relay(z, 1 - x)
    forward(after, 1 - x)
    relay(behind, x)
    relay(sooner, 1 - x)
    ow_across(0).wait_recv()
    ow_side(0, side).start()
    ow_pass(0).start()
    ow_across(1).wait_recv()
    ow_side(1, side).start()
    ow_pass(1).start()
    lam_out().wait_recv()
    wait_plane(z)
    wait_plane(sooner)

    def body_step(k, carry):
        upper = half == 1

        @pl.when(k == 4 - half)
        def _():
            forward(last, 1 - x)

        @pl.when(k == 3)
        def _():
            relay(after, 1 - x)
            ow_across(2).wait_recv()
            ow_pass(2).start()
            wait_plane(after)

        @pl.when(k == 5 - half)
        def _():
            ow_side(2, side).start()

        n = k % 3
        local = (k < 3) != top
        i_near = half * H + jnp.where(n == 0, 0, 1)
        i_third = jnp.where(upper, jnp.where(n == 0, 0, n + 1), H)
        i = jnp.where(local, i_near, i_third)
        j = jnp.where(local, half * H + n // 2, jnp.where(upper, 0, n))
        chunk(i, j)

        @pl.when(jnp.where(upper, jnp.logical_not(local) & (n == 0), jnp.where(local, n != 1, n == 2)))
        def _():
            finish(i)

        return carry

    lax.fori_loop(0, 6, body_step, 0)

    def last_step(k, carry):
        @pl.when(k == 1 - half)
        def _():
            relay(last, 1 - x)

        @pl.when(k == 3 * (1 - half))
        def _():
            wait_plane(last)

        i = jnp.where((half == 0) | (k == 1) | (k == 2), last, jnp.where(k == 0, near, z))
        chunk(i, jnp.where(half == 0, k, jnp.where(k == 1, 0, last)))

        @pl.when(jnp.where(half == 0, k == 3, k != 1))
        def _():
            finish(i)

        return carry

    lax.fori_loop(0, 4, last_step, 0)
    ow_across(3).wait_recv()
    ow_pass(3).start()
    ow_side(0, 1 - side).wait_recv()
    ow_pass(5).start()
    act_across().wait_send()
    act_mate().wait_send()
    act_pass().wait_send()
    ow_mate().wait_send()
    lam_out().wait_send()
    for l in range(L):
        for xx in range(X):
            for d in range(2):
                @pl.when(jnp.logical_not(stays(l, d)))
                def _():
                    piece(l, xx, d).wait_send()

    def settle(zs, carry):
        for xx in range(X):
            to_beside(zs, xx).wait_send()
            to_mate(zs, xx).wait_send()
            to_mate_again(zs, xx).wait_send()

        return carry

    lax.fori_loop(0, Z, settle, 0)
    own_ow().wait()
    ow_mate().wait_recv()
    TOT[...] = jnp.zeros(TOT.shape, jnp.float32)

    def add_head(i, carry):
        @pl.when(i == 2)
        def _():
            ow_side(1, 1 - side).wait_recv()
            ow_pass(6).start()
            ow_across(4).wait_recv()
            ow_pass(4).start()
            ow_side(2, 1 - side).wait_recv()
            ow_pass(7).start()
            for k in range(8):
                ow_pass(k).wait_recv()

        tail = i // 4
        plane = (1 - tail) * (i % 2) + tail * (Z - 1 - (i - 4) // 2)
        h = ((x + (1 - tail) * (i // 2) + tail * i) % 2) * 2 * L + plane
        remote(HO.at[0, 0], HI.at[h], h_send.at[0, 0], h_recv.at[h], s, mate).wait_recv()
        TOT[...] += jnp.dot(HI[h], W[h], preferred_element_type=jnp.float32)
        return carry

    lax.fori_loop(0, T * L, add_head, 0)
    for k in range(5):
        ow_across(k).wait_send()
    for k in range(3):
        ow_side(k, side).wait_send()
    for k in range(8):
        ow_pass(k).wait_send()
    out[...] = TOT[...].astype(jnp.bfloat16)


    def drain(zs, carry):
        for xx in range(X):
            @pl.when(jnp.logical_not(ends_here(zs, xx)))
            def _():
                home(zs, xx).wait_send()

        return carry

    lax.fori_loop(0, Z, drain, 0)


def fused(S, T, L, activations, query_weight, key_weight, value_weight, out_weight, lambdas, head_gain):
    R, D = activations.shape
    X, Y = 2, 2
    Z = S // Y
    bf, f32 = jnp.bfloat16, jnp.float32
    vmem = pl.BlockSpec(memory_space=pltpu.VMEM)
    hbm = pl.BlockSpec(memory_space=pl.ANY)
    smem = pl.BlockSpec(memory_space=pltpu.SMEM)
    dma = pltpu.SemaphoreType.DMA
    width = query_weight.shape[1]
    return pl.pallas_call(
        functools.partial(layer_kernel, S, T, L, R),
        out_shape=pltpu.VMEM((R, D), bf),
        in_specs=[hbm, hbm, hbm, hbm, hbm, smem, vmem],
        out_specs=vmem,
        scratch_shapes=[
            pltpu.VMEM((T, R, D), bf),
            pltpu.VMEM((L, D, 3 * width // L), bf),
            pltpu.VMEM((T * L, VALUE, D), bf),
            pltpu.VMEM((L, X, 2, R, 768), bf),
            pltpu.VMEM((Z, X, R, 768), bf),
            pltpu.VMEM((S * T * R, 512), bf),
            pltpu.VMEM((Z, X, R, VALUE), bf),
            pltpu.VMEM((T * L, R, VALUE), bf),
            pltpu.VMEM((L, 8, 128), f32),
            pltpu.VMEM((L, 8, 128), f32),
            pltpu.VMEM((Z, 2, X * R, VALUE), f32),
            pltpu.VMEM((Z, 2, X * R, 128), f32),
            pltpu.VMEM((Z, 2, X * R, 128), f32),
            pltpu.VMEM((R, D), f32),
            dma((L, 3)), dma((2,)),
            dma((3,)), dma((T,)),
            dma((1,)), dma((1,)),
            dma((5,)), dma((5,)), dma((3,)), dma((3,)), dma((9,)), dma((9,)),
            dma((L, X, 2)), dma((Z, X)),
            dma((3, Z, X)), dma((4, Z, X)),
            dma((Z, X)), dma((T * L,)),
        ],
        compiler_params=pltpu.CompilerParams(
            has_side_effects=True, collective_id=0, vmem_limit_bytes=60 * 1024 * 1024
        ),
    )(
        activations, query_weight, key_weight, value_weight,
        out_weight.reshape(L, VALUE, D), lambdas, head_gain.reshape(1, VALUE),
    )


def empty_state(count, local_heads):
    return (
        jnp.full((local_heads, 2, count), very_low, jnp.float32),
        jnp.zeros((local_heads, 2, count), jnp.float32),
        jnp.zeros((local_heads, 2, count, VALUE), jnp.float32),
    )


def absorb(state, query_set, query_pos, key_block, value_block, key_first):
    running, denoms, accums = state
    local_heads = running.shape[0]
    span = key_block.shape[0]
    key_grid = key_block.reshape(span, local_heads, 2, HEAD)
    scores = jnp.einsum(
        "qhme,khme->hmqk", query_set, key_grid, preferred_element_type=jnp.float32
    ) * HEAD ** (-0.5)
    key_pos = key_first + jnp.arange(span, dtype=jnp.int32)
    allowed = key_pos[None, :] <= query_pos[:, None]
    masked = jnp.where(allowed, scores, very_low)
    updated = jnp.maximum(running, jnp.max(masked, axis=-1))
    exp_weights = jnp.where(allowed, jnp.exp(masked - updated[..., None]), 0.0)
    factor = jnp.exp(running - updated)
    denoms = denoms * factor + jnp.sum(exp_weights, axis=-1)
    value_grid = value_block.reshape(span, local_heads, VALUE)
    product = jnp.einsum(
        "hmqk,khv->hmqv",
        exp_weights.astype(jnp.bfloat16),
        value_grid,
        preferred_element_type=jnp.float32,
    )
    accums = accums * factor[..., None] + product
    return (updated, denoms, accums)


def make_folder(query_sets, carry, pieces):
    key_piece, value_piece = pieces
    length = key_piece.shape[0]
    span = math.gcd(length, 512)

    def one_span(span_index, states):
        offset = span_index * span
        key_block = lax.dynamic_slice_in_dim(key_piece, offset, span, 0)
        value_block = lax.dynamic_slice_in_dim(value_piece, offset, span, 0)
        fresh = []
        for state, query_entry in zip(states, query_sets):
            query_set, query_pos = query_entry

            def take(current):
                return absorb(current, query_set, query_pos, key_block, value_block, offset)

            def leave(current):
                return current

            fresh.append(lax.cond(offset <= query_pos[-1], take, leave, state))
        return tuple(fresh)

    return lax.fori_loop(0, length // span, one_span, carry)


def shards(activations, query_weight, key_weight, value_weight, out_weight, lambdas, head_gain):
    local_heads = lambdas.shape[0]
    query_width = query_weight.shape[1]
    joined_weight = jnp.concatenate([query_weight, key_weight, value_weight], axis=1)
    projected = jnp.dot(
        lax.all_gather(activations, "tp", axis=0, tiled=True),
        joined_weight,
        preferred_element_type=jnp.float32,
    ).astype(jnp.bfloat16)
    row_count = projected.shape[0]
    queries = projected[:, :query_width].reshape(row_count, local_heads, 2, HEAD)
    key_rows = projected[:, query_width : 2 * query_width]
    value_rows = projected[:, 2 * query_width :]
    position = lax.axis_index("sp") * row_count + jnp.arange(row_count, dtype=jnp.int32)
    query_sets = [(queries, position)]
    start_states = tuple((empty_state(entry[0].shape[0], local_heads) for entry in query_sets))
    finals = make_folder(
        query_sets,
        start_states,
        (
            lax.all_gather(key_rows, "sp", axis=0, tiled=True),
            lax.all_gather(value_rows, "sp", axis=0, tiled=True),
        ),
    )
    outputs = []
    for state in finals:
        running, denoms, accums = state
        combined = (
            accums[:, 0] / denoms[:, 0, :, None]
            - lambdas[:, None, None] * accums[:, 1] / denoms[:, 1, :, None]
        )
        inverse_rms = lax.rsqrt(jnp.mean(combined * combined, axis=-1, keepdims=True) + norm_floor)
        normed = (combined * inverse_rms * head_gain).astype(jnp.bfloat16)
        outputs.append(
            jnp.transpose(normed, (1, 0, 2)).reshape(normed.shape[1], local_heads * VALUE)
        )
    heads_out = outputs[0]
    return lax.psum_scatter(
        jnp.dot(heads_out, out_weight, preferred_element_type=jnp.float32).astype(jnp.bfloat16),
        "tp",
        scatter_dimension=0,
        tiled=True,
    )


def solution(mesh):
    in_specs = (
        P(("sp", "tp"), None),
        P(None, "tp"),
        P(None, "tp"),
        P(None, "tp"),
        P("tp", None),
        P("tp"),
        P(),
    )
    out_specs = P(("sp", "tp"), None)
    S, T = mesh.shape["sp"], mesh.shape["tp"]

    def layer(*args):
        L = args[5].shape[0] // T
        rows = args[0].shape[0] // (S * T)
        fits = T == 4 and L == 2 and S == L * T and rows % 16 == 0 and rows * 8 % 128 == 0
        local = functools.partial(fused, S, T, L) if fits else shards
        return jax.shard_map(
            local, mesh=mesh, in_specs=in_specs, out_specs=out_specs, check_vma=False
        )(*args)

    return layer
```

```python
import functools
import math

import jax
import jax.numpy as jnp
from jax import lax
from jax.experimental import pallas as pl
from jax.experimental.pallas import tpu as pltpu
from jax.sharding import PartitionSpec as P

HEAD = 128
VALUE = 256


norm_floor = 0.02
very_low = -1e30
MESH = pl.DeviceIdType.MESH


def layer_kernel(
    S, T, L, R,
    act, qw, kw, vw, ow, lam_in, gain,
    out,
    A, WP, W, PQ, PK, QC, KV, HO, HI, LS, LB, ACC, MX, DN, TOT,
    w_sem, own_sem, a_send, a_recv, lam_send, lam_recv,
    ox_send, ox_recv, oy_send, oy_recv, m_send, m_recv,
    p_send, p_recv, f_send, f_recv, h_send, h_recv,
):
    X, Y = 2, 2
    Z = S // Y
    H = Z // 2
    s = lax.axis_index("sp")
    t = lax.axis_index("tp")
    x = t // 2
    c = t % 2
    y = s % Y
    z = s // Y
    half = z // H
    low = z % H
    mate = x * 2 + (1 - c)
    across = (1 - x) * 2 + c
    diagonal = (1 - x) * 2 + (1 - c)
    beside = z * Y + (1 - y)
    pair = (half * H + 1 - low) * Y + y
    side = (low + y) % 2
    near = half * H + 1 - low
    third = (1 - half) * H
    last = third + 1
    edge = (z == 0) | (z == Z - 1)
    ahead = (1 - half) * (Z - 1)
    behind = (1 - half) * H + half * (H - 1)
    early = jnp.where(edge, ahead, near)
    later = jnp.where(edge, near, ahead)
    held = (z == Z - 1) & (c != half)
    head = x * 2 * L + z
    span = T * R
    scale = HEAD ** (-0.5) * math.log2(math.e)

    def remote(src, dst, ss, rs, sp, tp):
        return pltpu.make_async_remote_copy(
            src_ref=src, dst_ref=dst, send_sem=ss, recv_sem=rs,
            device_id=(sp, tp), device_id_type=MESH,
        )

    first_head = jnp.where(c == half, 1 - low, c)

    def head_at(i):
        return first_head if i == 0 else 1 - first_head

    def weight_copy(i, part):
        l = head_at(i)
        return pltpu.make_async_copy(
            (qw, kw, vw)[part].at[:, pl.ds(pl.multiple_of(l * 256, 256), 256)],
            WP.at[l, :, part * 256:(part + 1) * 256], w_sem.at[i, part],
        )

    def own_act():
        return pltpu.make_async_copy(act, A.at[t], own_sem.at[0])

    def own_ow():
        return pltpu.make_async_copy(ow, W.at[pl.ds(t * L, L)], own_sem.at[1])

    def act_across():
        return remote(A.at[t], A.at[t], a_send.at[0], a_recv.at[t], s, across)

    def act_mate():
        return remote(A.at[t], A.at[t], a_send.at[1], a_recv.at[t], s, mate)

    def act_pass():
        return remote(A.at[across], A.at[across], a_send.at[2], a_recv.at[across], s, mate)

    def wait_act(i):
        remote(A.at[i], A.at[i], a_send.at[0], a_recv.at[i], s, mate).wait_recv()

    cut = VALUE // 4
    order = (0, 2, 3, 1)

    def slab(owner, l, k):
        return W.at[owner * L + l, pl.ds(k * cut, cut)]

    def ow_across(k):
        l, q = (side, order[k]) if k < 4 else (1 - side, order[3])
        return remote(
            ow.at[l, pl.ds(q * cut, cut)], slab(t, l, q), ox_send.at[k], ox_recv.at[k], s, across
        )

    def ow_side(k, l):
        if k < 2:
            part = slab(across, l, order[k])
        else:
            part = W.at[across * L + l, pl.ds(order[2] * cut + (k - 2) * (cut // 2), cut // 2)]
        target = (beside, pair)[k % 2]
        return remote(part, part, oy_send.at[k], oy_recv.at[k], target, t)

    def ow_pass(k):
        l, q = (side, order[k]) if k < 4 else (1 - side, (1, 0, 2, 3)[k - 4])
        part = slab(across, l, q)
        return remote(part, part, m_send.at[k], m_recv.at[k], s, mate)

    def ow_mate():
        return remote(ow, W.at[pl.ds(t * L, L)], m_send.at[8], m_recv.at[8], s, mate)

    def lam_out():
        return remote(LS, LB, lam_send.at[0], lam_recv.at[0], s, mate)

    barrier = pltpu.get_barrier_semaphore()
    own_act().start()
    for part in range(3):
        weight_copy(0, part).start()
    greeted = [(beside, t)]
    for i in range(Z):
        row = ((z + i) % Z) * Y + y
        greeted += [(row, mate), (row, across)] + ([(row, t)] if i > 0 else [])
    for sp, tp in greeted:
        pl.semaphore_signal(barrier, inc=1, device_id=(sp, tp), device_id_type=MESH)
    for l in range(L):
        LS[l] = jnp.full((8, 128), lam_in[l], jnp.float32)
    own_act().wait()
    for part in range(3):
        weight_copy(1, part).start()
    own_ow().start()
    pl.semaphore_wait(barrier, len(greeted))

    act_across().start()
    act_mate().start()
    for k in range(5):
        ow_across(k).start()

    def piece_sp(l):
        return (c * L + l) * Y + y

    def kv_rows(row, zs, xx, core):
        return pl.ds(((zs * Y + row) * T + xx * 2 + core) * R, R)

    def ends(kind, l, xx, d):
        if kind == 0:
            return PK.at[l, xx, d], KV.at[kv_rows(y, z, xx, d)]
        return PQ.at[l, xx, d], QC.at[z, xx]

    def piece(kind, l, xx, d):
        return remote(
            *ends(kind, l, xx, d), p_send.at[kind, l, xx, d], p_recv.at[kind, z, xx],
            piece_sp(l), x * 2 + d,
        )

    def stays(l, d):
        return (piece_sp(l) == s) & (c == d)

    def send(kind, xx, i):
        l = head_at(i)
        for d in range(2):
            @pl.when(stays(l, d))
            def _():
                pltpu.make_async_copy(*ends(kind, l, xx, d), p_recv.at[kind, z, xx]).start()

            @pl.when(jnp.logical_not(stays(l, d)))
            def _():
                piece(kind, l, xx, d).start()

    def project(xx, i):
        l = head_at(i)
        rows = A[pl.ds(xx * 2, 2)].reshape(2 * R, A.shape[2])
        got = jnp.dot(rows, WP[l], preferred_element_type=jnp.float32)
        PQ[l, xx] = (got[:, :256] * scale).astype(jnp.bfloat16).reshape(2, R, 256)
        PK[l, xx] = got[:, 256:].astype(jnp.bfloat16).reshape(2, R, 512)

    def to_beside(zs, xx):
        part = KV.at[kv_rows(y, zs, xx, c)]
        return remote(part, part, f_send.at[0, zs, xx], f_recv.at[0, zs, xx], beside, t)

    def to_mate(zs, xx):
        part = KV.at[kv_rows(y, zs, xx, c)]
        return remote(part, part, f_send.at[1, zs, xx], f_recv.at[1, zs, xx], s, mate)

    def to_mate_again(zs, xx):
        part = KV.at[kv_rows(1 - y, zs, xx, c)]
        return remote(part, part, f_send.at[2, zs, xx], f_recv.at[2, zs, xx], s, mate)

    def forward(zs, xx):
        part = KV.at[kv_rows(y, zs, xx, c)]
        remote(part, part, p_send.at[0, 0, 0, 0], p_recv.at[0, zs, xx], s, mate).wait_recv()
        to_beside(zs, xx).start()
        to_mate(zs, xx).start()

    def wait_q(zs):
        for xx in range(X):
            part = QC.at[zs, xx]
            remote(part, part, p_send.at[1, 0, 0, 0], p_recv.at[1, zs, xx], s, mate).wait_recv()

    def relay(zs, xx):
        to_beside(zs, xx).wait_recv()
        to_mate_again(zs, xx).start()

    def wait_plane(zs):
        for xx in range(X):
            to_mate(zs, xx).wait_recv()
            to_mate_again(zs, xx).wait_recv()

    q_rows = X * R
    k_rows = Y * span

    def chunk(i, j):
        row = lax.broadcasted_iota(jnp.int32, (q_rows, 128), 0)
        lane = lax.broadcasted_iota(jnp.int32, (q_rows, 128), 1)
        ahead_by = row + jnp.where(row >= R, R, 0) - lane + (y * span + c * R + (i - j) * k_rows)
        cols = range(0, k_rows, 128)
        for m in range(2):
            q = QC[i, :, :, m * 128:(m + 1) * 128].reshape(q_rows, 128)
            keys = KV[pl.ds(j * k_rows, k_rows), m * 128:(m + 1) * 128]
            sc = lax.dot_general(
                q, keys, (((1,), (1,)), ((), ())), preferred_element_type=jnp.float32
            )
            parts = [jnp.where(ahead_by >= b, sc[:, b:b + 128], very_low) for b in cols]
            top_part = functools.reduce(jnp.maximum, parts)
            old = MX[i, m]
            new = jnp.maximum(old, jnp.max(top_part, axis=1, keepdims=True))
            parts = [jnp.exp2(part - new) for part in parts]
            factor = jnp.exp2(old - new)
            DN[i, m] = DN[i, m] * factor + functools.reduce(jnp.add, parts)
            MX[i, m] = new
            p = jnp.concatenate([part.astype(jnp.bfloat16) for part in parts], axis=1)
            values = KV[pl.ds(j * k_rows, k_rows), 256:512]
            got = jnp.dot(p, values, preferred_element_type=jnp.float32)
            for b in range(0, VALUE, 128):
                ACC[i, m, :, b:b + 128] = ACC[i, m, :, b:b + 128] * factor + got[:, b:b + 128]

    def home(zs, xx):
        return remote(
            HO.at[zs, xx], HI.at[head], h_send.at[zs, xx], h_recv.at[head],
            zs * Y + y, xx * 2 + c,
        )

    def ends_here(zs, xx):
        return (zs == z) & (xx == x)

    def finish(i):
        mine = jnp.where(z // L == c, LS[z % L], LB[z % L])[:1, :1]
        dens = [jnp.sum(DN[i, m], axis=1, keepdims=True) for m in range(2)]
        comb = ACC[i, 0] * (1.0 / dens[0]) - ACC[i, 1] * (mine / dens[1])
        inv = lax.rsqrt(jnp.mean(comb * comb, axis=1, keepdims=True) + norm_floor)
        HO[i] = (comb * inv * gain[...]).astype(jnp.bfloat16).reshape(X, R, VALUE)
        for k in range(X):
            xx = (x + 1 + k) % X

            @pl.when(ends_here(i, xx))
            def _():
                pltpu.make_async_copy(HO.at[i, xx], HI.at[head], h_recv.at[head]).start()

            @pl.when(jnp.logical_not(ends_here(i, xx)))
            def _():
                home(i, xx).start()

    for part in range(3):
        weight_copy(0, part).wait()
    wait_act(mate)
    project(x, 0)
    send(0, x, 0)
    for part in range(3):
        weight_copy(1, part).wait()
    project(x, 1)
    send(0, x, 1)
    for i in range(L):
        send(1, x, i)
    forward(z, x)
    lam_out().start()
    ow_mate().start()
    MX[...] = jnp.full(MX.shape, very_low, jnp.float32)
    DN[...] = jnp.zeros(DN.shape, jnp.float32)
    ACC[...] = jnp.zeros(ACC.shape, jnp.float32)
    forward(early, x)
    relay(z, x)
    wait_act(across)
    act_pass().start()
    forward(later, x)
    wait_act(diagonal)
    def send_rest():
        for kind in range(2):
            for i in range(L):
                send(kind, 1 - x, i)

    project(1 - x, 0)
    project(1 - x, 1)

    @pl.when(jnp.logical_not(held))
    def _():
        send_rest()

    forward(z, 1 - x)
    relay(early, x)
    relay(later, x)
    forward(behind, x)
    top = z == Z - 1
    sooner = jnp.where(top, third, near)
    after = jnp.where(top, near, third)
    forward(sooner, 1 - x)

    relay(z, 1 - x)
    forward(after, 1 - x)
    relay(behind, x)

    @pl.when(held)
    def _():
        send_rest()

    relay(sooner, 1 - x)
    lam_out().wait_recv()
    wait_q(z)
    wait_q(near)

    @pl.when(top)
    def _():
        wait_q(third)

    wait_plane(z)
    wait_plane(sooner)

    def body_step(k, carry):
        upper = half == 1

        @pl.when(k == 0)
        def _():
            for n in range(2):
                ow_across(n).wait_recv()
                ow_pass(n).start()
            ow_side(1, side).start()

        @pl.when(k == 2)
        def _():
            ow_across(2).wait_recv()
            ow_side(3, side).start()
            ow_pass(2).start()

        @pl.when(k == 3)
        def _():
            forward(last, 1 - x)
            relay(after, 1 - x)

            @pl.when(jnp.logical_not(top))
            def _():
                wait_q(third)

            wait_plane(after)

        @pl.when(k == 4)
        def _():
            ow_side(0, side).start()
            ow_side(2, side).start()

        n = k % 3
        local = (k < 3) != top
        i_near = half * H + jnp.where(n == 0, 0, 1)
        i_third = jnp.where(upper, jnp.where(n == 0, 0, n + 1), H)
        i = jnp.where(local, i_near, i_third)
        j = jnp.where(local, half * H + n // 2, jnp.where(upper, 0, n))
        chunk(i, j)

        @pl.when(jnp.where(upper, jnp.logical_not(local) & (n == 0), jnp.where(local, n != 1, n == 2)))
        def _():
            finish(i)

        return carry

    lax.fori_loop(0, 6, body_step, 0)

    def last_step(k, carry):
        @pl.when(k == 0)
        def _():
            wait_q(last)

        @pl.when(k == 2 - half)
        def _():
            relay(last, 1 - x)

        @pl.when(k == 3 - 2 * half)
        def _():
            wait_plane(last)

        i = jnp.where(
            k == 1, jnp.where(top, last, near),
            jnp.where(k == 2, jnp.where(top, z, last), jnp.where(top, near, z)),
        )
        i = jnp.where((half == 0) | (k == 0), last, i)
        chunk(i, jnp.where(half == 0, k, jnp.where(k == 0, 0, last)))

        @pl.when(jnp.where(half == 0, k == 3, k > 0))
        def _():
            finish(i)

        return carry

    lax.fori_loop(0, 4, last_step, 0)
    ow_across(3).wait_recv()
    ow_pass(3).start()
    for k in range(2):
        ow_side(k, 1 - side).wait_recv()
        ow_pass(5 + k).start()
    ow_across(4).wait_recv()
    ow_pass(4).start()
    act_across().wait_send()
    act_mate().wait_send()
    act_pass().wait_send()
    ow_mate().wait_send()
    lam_out().wait_send()
    for l in range(L):
        for xx in range(X):
            for d in range(2):
                @pl.when(jnp.logical_not(stays(l, d)))
                def _():
                    for kind in range(2):
                        piece(kind, l, xx, d).wait_send()

    def settle(zs, carry):
        for xx in range(X):
            to_beside(zs, xx).wait_send()
            to_mate(zs, xx).wait_send()
            to_mate_again(zs, xx).wait_send()

        return carry

    lax.fori_loop(0, Z, settle, 0)
    own_ow().wait()
    ow_mate().wait_recv()
    TOT[...] = jnp.zeros(TOT.shape, jnp.float32)

    def add_head(i, code):
        @pl.when(i == 2)
        def _():
            for k in range(4):
                ow_pass(k).wait_recv()

        @pl.when(i == 4 - 2 * low)
        def _():
            for k in range(2, 4):
                ow_side(k, 1 - side).wait_recv()
            ow_pass(7).start()

        @pl.when(i == 6 - 3 * low)
        def _():
            for k in range(4, 8):
                ow_pass(k).wait_recv()

        plane, off = code % 8 // 2, code % 2
        plane = plane // 2 * 2 + (plane + off * side) % 2
        h = (x + off) % 2 * 2 * L + plane
        remote(HO.at[0, 0], HI.at[h], h_send.at[0, 0], h_recv.at[h], s, mate).wait_recv()
        TOT[...] += jnp.dot(HI[h], W[h], preferred_element_type=jnp.float32)
        return code // 8

    orders = [
        functools.reduce(lambda total, e: total * 8 + e, reversed(order), 0)
        for order in (
            (0, 2, 1, 6, 4, 5, 3, 7), (0, 2, 1, 3, 6, 4, 5, 7),
            (0, 2, 1, 4, 6, 5, 3, 7), (6, 0, 1, 3, 2, 5, 7, 4),
        )
    ]
    code = jnp.where(
        half == 0, jnp.where(low == 0, orders[0], orders[1]),
        jnp.where(low == 0, orders[2], orders[3]),
    )
    lax.fori_loop(0, T * L, add_head, code)
    for k in range(5):
        ow_across(k).wait_send()
    for k in range(4):
        ow_side(k, side).wait_send()
    for k in range(8):
        ow_pass(k).wait_send()
    out[...] = TOT[...].astype(jnp.bfloat16)


    def drain(zs, carry):
        for xx in range(X):
            @pl.when(jnp.logical_not(ends_here(zs, xx)))
            def _():
                home(zs, xx).wait_send()

        return carry

    lax.fori_loop(0, Z, drain, 0)


def fused(S, T, L, activations, query_weight, key_weight, value_weight, out_weight, lambdas, head_gain):
    R, D = activations.shape
    X, Y = 2, 2
    Z = S // Y
    bf, f32 = jnp.bfloat16, jnp.float32
    vmem = pl.BlockSpec(memory_space=pltpu.VMEM)
    hbm = pl.BlockSpec(memory_space=pl.ANY)
    smem = pl.BlockSpec(memory_space=pltpu.SMEM)
    dma = pltpu.SemaphoreType.DMA
    width = query_weight.shape[1]
    return pl.pallas_call(
        functools.partial(layer_kernel, S, T, L, R),
        out_shape=pltpu.VMEM((R, D), bf),
        in_specs=[hbm, hbm, hbm, hbm, hbm, smem, vmem],
        out_specs=vmem,
        scratch_shapes=[
            pltpu.VMEM((T, R, D), bf),
            pltpu.VMEM((L, D, 3 * width // L), bf),
            pltpu.VMEM((T * L, VALUE, D), bf),
            pltpu.VMEM((L, X, 2, R, 256), bf),
            pltpu.VMEM((L, X, 2, R, 512), bf),
            pltpu.VMEM((Z, X, R, 256), bf),
            pltpu.VMEM((S * T * R, 512), bf),
            pltpu.VMEM((Z, X, R, VALUE), bf),
            pltpu.VMEM((T * L, R, VALUE), bf),
            pltpu.VMEM((L, 8, 128), f32),
            pltpu.VMEM((L, 8, 128), f32),
            pltpu.VMEM((Z, 2, X * R, VALUE), f32),
            pltpu.VMEM((Z, 2, X * R, 128), f32),
            pltpu.VMEM((Z, 2, X * R, 128), f32),
            pltpu.VMEM((R, D), f32),
            dma((L, 3)), dma((2,)),
            dma((3,)), dma((T,)),
            dma((1,)), dma((1,)),
            dma((5,)), dma((5,)), dma((4,)), dma((4,)), dma((9,)), dma((9,)),
            dma((2, L, X, 2)), dma((2, Z, X)),
            dma((3, Z, X)), dma((3, Z, X)),
            dma((Z, X)), dma((T * L,)),
        ],
        compiler_params=pltpu.CompilerParams(
            has_side_effects=True, collective_id=0, vmem_limit_bytes=60 * 1024 * 1024
        ),
    )(
        activations, query_weight, key_weight, value_weight,
        out_weight.reshape(L, VALUE, D), lambdas, head_gain.reshape(1, VALUE),
    )


def empty_state(count, local_heads):
    return (
        jnp.full((local_heads, 2, count), very_low, jnp.float32),
        jnp.zeros((local_heads, 2, count), jnp.float32),
        jnp.zeros((local_heads, 2, count, VALUE), jnp.float32),
    )


def absorb(state, query_set, query_pos, key_block, value_block, key_first):
    running, denoms, accums = state
    local_heads = running.shape[0]
    span = key_block.shape[0]
    key_grid = key_block.reshape(span, local_heads, 2, HEAD)
    scores = jnp.einsum(
        "qhme,khme->hmqk", query_set, key_grid, preferred_element_type=jnp.float32
    ) * HEAD ** (-0.5)
    key_pos = key_first + jnp.arange(span, dtype=jnp.int32)
    allowed = key_pos[None, :] <= query_pos[:, None]
    masked = jnp.where(allowed, scores, very_low)
    updated = jnp.maximum(running, jnp.max(masked, axis=-1))
    exp_weights = jnp.where(allowed, jnp.exp(masked - updated[..., None]), 0.0)
    factor = jnp.exp(running - updated)
    denoms = denoms * factor + jnp.sum(exp_weights, axis=-1)
    value_grid = value_block.reshape(span, local_heads, VALUE)
    product = jnp.einsum(
        "hmqk,khv->hmqv",
        exp_weights.astype(jnp.bfloat16),
        value_grid,
        preferred_element_type=jnp.float32,
    )
    accums = accums * factor[..., None] + product
    return (updated, denoms, accums)


def make_folder(query_sets, carry, pieces):
    key_piece, value_piece = pieces
    length = key_piece.shape[0]
    span = math.gcd(length, 512)

    def one_span(span_index, states):
        offset = span_index * span
        key_block = lax.dynamic_slice_in_dim(key_piece, offset, span, 0)
        value_block = lax.dynamic_slice_in_dim(value_piece, offset, span, 0)
        fresh = []
        for state, query_entry in zip(states, query_sets):
            query_set, query_pos = query_entry

            def take(current):
                return absorb(current, query_set, query_pos, key_block, value_block, offset)

            def leave(current):
                return current

            fresh.append(lax.cond(offset <= query_pos[-1], take, leave, state))
        return tuple(fresh)

    return lax.fori_loop(0, length // span, one_span, carry)


def shards(activations, query_weight, key_weight, value_weight, out_weight, lambdas, head_gain):
    local_heads = lambdas.shape[0]
    query_width = query_weight.shape[1]
    joined_weight = jnp.concatenate([query_weight, key_weight, value_weight], axis=1)
    projected = jnp.dot(
        lax.all_gather(activations, "tp", axis=0, tiled=True),
        joined_weight,
        preferred_element_type=jnp.float32,
    ).astype(jnp.bfloat16)
    row_count = projected.shape[0]
    queries = projected[:, :query_width].reshape(row_count, local_heads, 2, HEAD)
    key_rows = projected[:, query_width : 2 * query_width]
    value_rows = projected[:, 2 * query_width :]
    position = lax.axis_index("sp") * row_count + jnp.arange(row_count, dtype=jnp.int32)
    query_sets = [(queries, position)]
    start_states = tuple((empty_state(entry[0].shape[0], local_heads) for entry in query_sets))
    finals = make_folder(
        query_sets,
        start_states,
        (
            lax.all_gather(key_rows, "sp", axis=0, tiled=True),
            lax.all_gather(value_rows, "sp", axis=0, tiled=True),
        ),
    )
    outputs = []
    for state in finals:
        running, denoms, accums = state
        combined = (
            accums[:, 0] / denoms[:, 0, :, None]
            - lambdas[:, None, None] * accums[:, 1] / denoms[:, 1, :, None]
        )
        inverse_rms = lax.rsqrt(jnp.mean(combined * combined, axis=-1, keepdims=True) + norm_floor)
        normed = (combined * inverse_rms * head_gain).astype(jnp.bfloat16)
        outputs.append(
            jnp.transpose(normed, (1, 0, 2)).reshape(normed.shape[1], local_heads * VALUE)
        )
    heads_out = outputs[0]
    return lax.psum_scatter(
        jnp.dot(heads_out, out_weight, preferred_element_type=jnp.float32).astype(jnp.bfloat16),
        "tp",
        scatter_dimension=0,
        tiled=True,
    )


def solution(mesh):
    in_specs = (
        P(("sp", "tp"), None),
        P(None, "tp"),
        P(None, "tp"),
        P(None, "tp"),
        P("tp", None),
        P("tp"),
        P(),
    )
    out_specs = P(("sp", "tp"), None)
    S, T = mesh.shape["sp"], mesh.shape["tp"]

    def layer(*args):
        L = args[5].shape[0] // T
        rows = args[0].shape[0] // (S * T)
        fits = T == 4 and L == 2 and S == L * T and rows % 16 == 0 and rows * 8 % 128 == 0
        local = functools.partial(fused, S, T, L) if fits else shards
        return jax.shard_map(
            local, mesh=mesh, in_specs=in_specs, out_specs=out_specs, check_vma=False
        )(*args)

    return layer
```

```python
import functools
import math

import jax
import jax.numpy as jnp
from jax import lax
from jax.experimental import pallas as pl
from jax.experimental.pallas import tpu as pltpu
from jax.sharding import PartitionSpec as P

HEAD = 128
VALUE = 256


norm_floor = 0.02
very_low = -1e30
MESH = pl.DeviceIdType.MESH


def layer_kernel(
    S, T, L, R,
    act, qw, kw, vw, ow, lam_ref, gain_ref,
    out,
    lam_in, gain, A, WP, W, PQ, PK, QC, KV, HO, HI, LS, LB, ACC, MX, DN, TOT,
    w_sem, own_sem, a_send, a_recv, lam_send, lam_recv,
    ox_send, ox_recv, oy_send, oy_recv, m_send, m_recv,
    p_send, p_recv, q_recv, f_send, f_recv, g_recv, h_send, h_recv,
):
    X, Y = 2, 2
    Z = S // Y
    H = Z // 2
    s = lax.axis_index("sp")
    t = lax.axis_index("tp")
    x = t // 2
    c = t % 2
    y = s % Y
    z = s // Y
    half = z // H
    low = z % H
    mate = x * 2 + (1 - c)
    across = (1 - x) * 2 + c
    diagonal = (1 - x) * 2 + (1 - c)
    beside = z * Y + (1 - y)
    pair = (half * H + 1 - low) * Y + y
    side = (low + y) % 2
    near = half * H + 1 - low
    third = (1 - half) * H
    last = third + 1
    edge = (z == 0) | (z == Z - 1)
    ahead = (1 - half) * (Z - 1)
    behind = (1 - half) * H + half * (H - 1)
    early = jnp.where(edge, ahead, near)
    later = jnp.where(edge, near, ahead)
    held = (z == Z - 1) & (c != half)
    head = x * 2 * L + z
    span = T * R
    scale = HEAD ** (-0.5) * math.log2(math.e)

    def remote(src, dst, ss, rs, sp, tp):
        return pltpu.make_async_remote_copy(
            src_ref=src, dst_ref=dst, send_sem=ss, recv_sem=rs,
            device_id=(sp, tp), device_id_type=MESH,
        )

    first_head = jnp.where(c == half, 1 - low, c)

    def head_at(i):
        return first_head if i == 0 else 1 - first_head

    def weight_copy(i, part):
        l = head_at(i)
        return pltpu.make_async_copy(
            (qw, kw, vw)[part].at[:, pl.ds(pl.multiple_of(l * 256, 256), 256)],
            WP.at[l, :, part * 256:(part + 1) * 256], w_sem.at[i],
        )

    def own_act():
        return pltpu.make_async_copy(act, A.at[t], own_sem.at[0])

    def small(k):
        pair = ((lam_ref, lam_in), (gain_ref, gain))[k]
        return pltpu.make_async_copy(*pair, own_sem.at[2 + k])

    def own_ow():
        return pltpu.make_async_copy(ow, W.at[pl.ds(t * L, L)], own_sem.at[1])

    def act_across():
        return remote(A.at[t], A.at[t], a_send.at[0], a_recv.at[t], s, across)

    def act_mate():
        return remote(A.at[t], A.at[t], a_send.at[0], a_recv.at[t], s, mate)

    def act_pass():
        return remote(A.at[across], A.at[across], a_send.at[0], a_recv.at[across], s, mate)

    def wait_act(i):
        remote(A.at[i], A.at[i], a_send.at[0], a_recv.at[i], s, mate).wait_recv()

    cut = VALUE // 4
    order = (0, 2, 3, 1)

    def slab(owner, l, k):
        return W.at[owner * L + l, pl.ds(k * cut, cut)]

    def ow_across(k):
        l, q = (side, order[k]) if k < 4 else (1 - side, order[3])
        return remote(
            ow.at[l, pl.ds(q * cut, cut)], slab(t, l, q), ox_send.at[0], ox_recv.at[k], s, across
        )

    def ow_side(k, l):
        if k < 2:
            part = slab(across, l, order[k])
        else:
            part = W.at[across * L + l, pl.ds(order[2] * cut + (k - 2) * (cut // 2), cut // 2)]
        target = (beside, pair)[k % 2]
        return remote(part, part, oy_send.at[0], oy_recv.at[min(k, 2)], target, t)

    def ow_pass(k):
        l, q = (side, order[k]) if k < 4 else (1 - side, (1, 0, 2, 3)[k - 4])
        part = slab(across, l, q)
        return remote(part, part, m_send.at[0], m_recv.at[k // 4], s, mate)

    def ow_mate():
        return remote(ow, W.at[pl.ds(t * L, L)], m_send.at[0], m_recv.at[2], s, mate)

    def lam_out():
        return remote(LS, LB, lam_send.at[0], lam_recv.at[0], s, mate)

    barrier = pltpu.get_barrier_semaphore()
    own_act().start()
    small(0).start()
    small(1).start()
    greeted = [(beside, t)]
    for i in range(Z):
        row = ((z + i) % Z) * Y + y
        greeted += [(row, mate), (row, across)] + ([(row, t)] if i > 0 else [])
    for sp, tp in greeted:
        pl.semaphore_signal(barrier, inc=1, device_id=(sp, tp), device_id_type=MESH)
    for part in range(3):
        weight_copy(0, part).start()
    own_act().wait()
    for part in range(3):
        weight_copy(1, part).start()
    own_ow().start()
    pl.semaphore_wait(barrier, len(greeted))

    act_across().start()
    act_mate().start()
    small(0).wait()
    small(1).wait()
    for l in range(L):
        LS[l] = jnp.full((8, 128), lam_in[l], jnp.float32)
    for k in range(5):
        ow_across(k).start()

    def piece_sp(l):
        return (c * L + l) * Y + y

    def kv_rows(row, zs, xx, core):
        return pl.ds(((zs * Y + row) * T + xx * 2 + core) * R, R)

    def ends(kind, l, xx, d):
        if kind == 0:
            return PK.at[l, xx, d], KV.at[kv_rows(y, z, xx, d)]
        return PQ.at[l, xx, d], QC.at[z, xx]

    def arrival(kind, zs, xx):
        return p_recv.at[zs, xx] if kind == 0 else q_recv.at[zs]

    def piece(kind, l, xx, d):
        return remote(
            *ends(kind, l, xx, d), p_send.at[kind], arrival(kind, z, xx),
            piece_sp(l), x * 2 + d,
        )

    def stays(l, d):
        return (piece_sp(l) == s) & (c == d)

    def send(kind, xx, i):
        l = head_at(i)
        for d in range(2):
            @pl.when(stays(l, d))
            def _():
                pltpu.make_async_copy(*ends(kind, l, xx, d), arrival(kind, z, xx)).start()

            @pl.when(jnp.logical_not(stays(l, d)))
            def _():
                piece(kind, l, xx, d).start()

    def project(xx, i):
        l = head_at(i)
        rows = A[pl.ds(xx * 2, 2)].reshape(2 * R, A.shape[2])
        got = jnp.dot(rows, WP[l], preferred_element_type=jnp.float32)
        PQ[l, xx] = (got[:, :256] * scale).astype(jnp.bfloat16).reshape(2, R, 256)
        PK[l, xx] = got[:, 256:].astype(jnp.bfloat16).reshape(2, R, 512)

    def to_beside(zs, xx):
        part = KV.at[kv_rows(y, zs, xx, c)]
        return remote(part, part, f_send.at[0], f_recv.at[zs, xx], beside, t)

    def to_mate(zs, xx):
        part = KV.at[kv_rows(y, zs, xx, c)]
        return remote(part, part, f_send.at[0], g_recv.at[zs], s, mate)

    def to_mate_again(zs, xx):
        part = KV.at[kv_rows(1 - y, zs, xx, c)]
        return remote(part, part, f_send.at[0], g_recv.at[zs], s, mate)

    def forward(zs, xx):
        part = KV.at[kv_rows(y, zs, xx, c)]
        remote(part, part, p_send.at[0], p_recv.at[zs, xx], s, mate).wait_recv()
        to_beside(zs, xx).start()
        to_mate(zs, xx).start()

    def wait_q(zs):
        part = QC.at[zs]
        remote(part, part, p_send.at[1], q_recv.at[zs], s, mate).wait_recv()

    def relay(zs, xx):
        to_beside(zs, xx).wait_recv()
        to_mate_again(zs, xx).start()

    def wait_plane(zs):
        part = KV.at[pl.ds(0, 2 * X * R)]
        remote(part, part, f_send.at[0], g_recv.at[zs], s, mate).wait_recv()

    q_rows = X * R
    k_rows = Y * span

    def chunk(i, j):
        row = lax.broadcasted_iota(jnp.int32, (q_rows, 128), 0)
        lane = lax.broadcasted_iota(jnp.int32, (q_rows, 128), 1)
        ahead_by = row + jnp.where(row >= R, R, 0) - lane + (y * span + c * R + (i - j) * k_rows)
        cols = range(0, k_rows, 128)
        weights, factors = [], []
        for m in range(2):
            q = QC[i, :, :, m * 128:(m + 1) * 128].reshape(q_rows, 128)
            keys = KV[pl.ds(j * k_rows, k_rows), m * 128:(m + 1) * 128]
            sc = lax.dot_general(
                q, keys, (((1,), (1,)), ((), ())), preferred_element_type=jnp.float32
            )
            parts = [jnp.where(ahead_by >= b, sc[:, b:b + 128], very_low) for b in cols]
            top_part = functools.reduce(jnp.maximum, parts)
            old = MX[i, m]
            new = jnp.maximum(old, jnp.max(top_part, axis=1, keepdims=True))
            parts = [jnp.exp2(part - new) for part in parts]
            factor = jnp.exp2(old - new)
            DN[i, m] = DN[i, m] * factor + functools.reduce(jnp.add, parts)
            MX[i, m] = new
            weights.append(jnp.concatenate([part.astype(jnp.bfloat16) for part in parts], axis=1))
            factors.append(factor)
        values = KV[pl.ds(j * k_rows, k_rows), 256:512]
        got = jnp.dot(
            jnp.concatenate(weights, axis=0), values, preferred_element_type=jnp.float32
        )
        for m in range(2):
            for b in range(0, VALUE, 128):
                fresh = got[m * q_rows:(m + 1) * q_rows, b:b + 128]
                ACC[i, m, :, b:b + 128] = ACC[i, m, :, b:b + 128] * factors[m] + fresh

    def home(zs, xx):
        return remote(
            HO.at[zs, xx], HI.at[head], h_send.at[0], h_recv.at[head],
            zs * Y + y, xx * 2 + c,
        )

    def ends_here(zs, xx):
        return (zs == z) & (xx == x)

    def finish(i):
        mine = jnp.where(z // L == c, LS[z % L], LB[z % L])[:1, :1]
        dens = [jnp.sum(DN[i, m], axis=1, keepdims=True) for m in range(2)]
        comb = ACC[i, 0] * (1.0 / dens[0]) - ACC[i, 1] * (mine / dens[1])
        inv = lax.rsqrt(jnp.mean(comb * comb, axis=1, keepdims=True) + norm_floor)
        HO[i] = (comb * inv * gain[...]).astype(jnp.bfloat16).reshape(X, R, VALUE)
        for k in range(X):
            xx = (x + 1 + k) % X

            @pl.when(ends_here(i, xx))
            def _():
                pltpu.make_async_copy(HO.at[i, xx], HI.at[head], h_recv.at[head]).start()

            @pl.when(jnp.logical_not(ends_here(i, xx)))
            def _():
                home(i, xx).start()

    def wait_weights(i):
        pltpu.make_async_copy(WP.at[i], WP.at[i], w_sem.at[i]).wait()

    wait_weights(0)
    wait_act(mate)
    project(x, 0)
    send(0, x, 0)
    wait_weights(1)
    project(x, 1)
    send(0, x, 1)
    for i in range(L):
        send(1, x, i)
    forward(z, x)
    lam_out().start()
    ow_mate().start()
    MX[...] = jnp.full(MX.shape, very_low, jnp.float32)
    DN[...] = jnp.zeros(DN.shape, jnp.float32)
    ACC[...] = jnp.zeros(ACC.shape, jnp.float32)
    forward(early, x)
    relay(z, x)
    wait_act(across)
    act_pass().start()
    forward(later, x)
    wait_act(diagonal)
    def send_rest():
        for kind in range(2):
            for i in range(L):
                send(kind, 1 - x, i)

    project(1 - x, 0)
    project(1 - x, 1)

    @pl.when(jnp.logical_not(held))
    def _():
        send_rest()

    forward(z, 1 - x)
    relay(early, x)
    relay(later, x)
    forward(behind, x)
    top = z == Z - 1
    sooner = jnp.where(top, third, near)
    after = jnp.where(top, near, third)
    forward(sooner, 1 - x)

    relay(z, 1 - x)
    forward(after, 1 - x)
    relay(behind, x)

    @pl.when(held)
    def _():
        send_rest()

    relay(sooner, 1 - x)
    lam_out().wait_recv()
    wait_q(z)
    wait_q(near)

    @pl.when(top)
    def _():
        wait_q(third)

    wait_plane(z)
    wait_plane(sooner)

    def body_step(k, carry):
        upper = half == 1

        @pl.when(k == 0)
        def _():
            for n in range(2):
                ow_across(n).wait_recv()
                ow_pass(n).start()
            ow_side(1, side).start()

        @pl.when(k == 2)
        def _():
            ow_across(2).wait_recv()
            ow_side(3, side).start()
            ow_pass(2).start()

        @pl.when(k == 3)
        def _():
            forward(last, 1 - x)
            relay(after, 1 - x)

            @pl.when(jnp.logical_not(top))
            def _():
                wait_q(third)

            wait_plane(after)

        @pl.when(k == 4)
        def _():
            ow_side(0, side).start()
            ow_side(2, side).start()

        n = k % 3
        local = (k < 3) != top
        i_near = half * H + jnp.where(n == 0, 0, 1)
        i_third = jnp.where(upper, jnp.where(n == 0, 0, n + 1), H)
        i = jnp.where(local, i_near, i_third)
        j = jnp.where(local, half * H + n // 2, jnp.where(upper, 0, n))
        chunk(i, j)

        @pl.when(jnp.where(upper, jnp.logical_not(local) & (n == 0), jnp.where(local, n != 1, n == 2)))
        def _():
            finish(i)

        return carry

    lax.fori_loop(0, 6, body_step, 0)

    def last_step(k, carry):
        @pl.when(k == 0)
        def _():
            wait_q(last)

        @pl.when(k == 2 - half)
        def _():
            relay(last, 1 - x)

        @pl.when(k == 3 - 2 * half)
        def _():
            wait_plane(last)

        i = jnp.where(
            k == 1, jnp.where(top, last, near),
            jnp.where(k == 2, jnp.where(top, near, last), z),
        )
        i = jnp.where((half == 0) | (k == 0), last, i)
        chunk(i, jnp.where(half == 0, k, jnp.where(k == 0, 0, last)))

        @pl.when(jnp.where(half == 0, k == 3, k > 0))
        def _():
            finish(i)

        return carry

    lax.fori_loop(0, 4, last_step, 0)
    ow_across(3).wait_recv()
    ow_pass(3).start()
    for k in range(2):
        ow_side(k, 1 - side).wait_recv()
        ow_pass(5 + k).start()
    ow_across(4).wait_recv()
    ow_pass(4).start()
    def sent(part, sem):
        remote(part, part, sem, lam_recv.at[0], s, mate).wait_send()

    sent(A.at[pl.ds(0, 3)], a_send.at[0])
    lam_out().wait_send()
    sent(KV.at[pl.ds(0, 3 * Z * X * R)], f_send.at[0])
    keeps = c == half

    def sent_pieces(count):
        sent(KV.at[pl.ds(0, count * X * R)], p_send.at[0])
        sent(QC.at[pl.ds(0, count)], p_send.at[1])

    @pl.when(keeps)
    def _():
        sent_pieces(2 * L - 1)

    @pl.when(jnp.logical_not(keeps))
    def _():
        sent_pieces(2 * L)

    own_ow().wait()
    ow_mate().wait_recv()
    TOT[...] = jnp.zeros(TOT.shape, jnp.float32)

    def wait_passed(n):
        part = W.at[0]
        remote(part, part, m_send.at[0], m_recv.at[n], s, mate).wait_recv()

    def add_head(i, code):
        @pl.when(i == 2)
        def _():
            wait_passed(0)

        @pl.when(i == 4 - 2 * low)
        def _():
            part = slab(across, 0, 0)
            remote(part, part, oy_send.at[0], oy_recv.at[2], s, mate).wait_recv()
            ow_pass(7).start()

        @pl.when(i == 6 - 3 * low)
        def _():
            wait_passed(1)

        plane, off = code % 8 // 2, code % 2
        plane = plane // 2 * 2 + (plane + off * side) % 2
        h = (x + off) % 2 * 2 * L + plane
        remote(HO.at[0, 0], HI.at[h], h_send.at[0], h_recv.at[h], s, mate).wait_recv()
        TOT[...] += jnp.dot(HI[h], W[h], preferred_element_type=jnp.float32)
        return code // 8

    orders = [
        functools.reduce(lambda total, e: total * 8 + e, reversed(order), 0)
        for order in (
            (0, 2, 1, 6, 4, 5, 3, 7), (0, 2, 1, 3, 6, 4, 5, 7),
            (0, 2, 1, 4, 6, 5, 3, 7), (6, 0, 1, 3, 2, 5, 7, 4),
        )
    ]
    code = jnp.where(
        half == 0, jnp.where(low == 0, orders[0], orders[1]),
        jnp.where(low == 0, orders[2], orders[3]),
    )
    lax.fori_loop(0, T * L, add_head, code)
    sent(W.at[pl.ds(0, 5), pl.ds(0, cut)], ox_send.at[0])
    sent(W.at[0, pl.ds(0, 3 * cut)], oy_send.at[0])
    sent(W.at[pl.ds(0, 2 * L)], m_send.at[0])
    out[...] = TOT[...].astype(jnp.bfloat16)


    sent(HI.at[pl.ds(0, Z * X - 1)], h_send.at[0])


def fused(S, T, L, activations, query_weight, key_weight, value_weight, out_weight, lambdas, head_gain):
    R, D = activations.shape
    X, Y = 2, 2
    Z = S // Y
    bf, f32 = jnp.bfloat16, jnp.float32
    vmem = pl.BlockSpec(memory_space=pltpu.VMEM)
    hbm = pl.BlockSpec(memory_space=pl.ANY)
    dma = pltpu.SemaphoreType.DMA
    width = query_weight.shape[1]
    return pl.pallas_call(
        functools.partial(layer_kernel, S, T, L, R),
        out_shape=pltpu.VMEM((R, D), bf),
        in_specs=[hbm] * 7,
        out_specs=vmem,
        scratch_shapes=[
            pltpu.SMEM((L,), f32),
            pltpu.VMEM((1, VALUE), f32),
            pltpu.VMEM((T, R, D), bf),
            pltpu.VMEM((L, D, 3 * width // L), bf),
            pltpu.VMEM((T * L, VALUE, D), bf),
            pltpu.VMEM((L, X, 2, R, 256), bf),
            pltpu.VMEM((L, X, 2, R, 512), bf),
            pltpu.VMEM((Z, X, R, 256), bf),
            pltpu.VMEM((S * T * R, 512), bf),
            pltpu.VMEM((Z, X, R, VALUE), bf),
            pltpu.VMEM((T * L, R, VALUE), bf),
            pltpu.VMEM((L, 8, 128), f32),
            pltpu.VMEM((L, 8, 128), f32),
            pltpu.VMEM((Z, 2, X * R, VALUE), f32),
            pltpu.VMEM((Z, 2, X * R, 128), f32),
            pltpu.VMEM((Z, 2, X * R, 128), f32),
            pltpu.VMEM((R, D), f32),
            dma((L,)), dma((4,)),
            dma((1,)), dma((T,)),
            dma((1,)), dma((1,)),
            dma((1,)), dma((5,)), dma((1,)), dma((3,)), dma((1,)), dma((3,)),
            dma((2,)), dma((Z, X)), dma((Z,)),
            dma((1,)), dma((Z, X)), dma((Z,)),
            dma((1,)), dma((T * L,)),
        ],
        compiler_params=pltpu.CompilerParams(
            has_side_effects=True, collective_id=0, vmem_limit_bytes=60 * 1024 * 1024
        ),
    )(
        activations, query_weight, key_weight, value_weight,
        out_weight.reshape(L, VALUE, D), lambdas, head_gain.reshape(1, VALUE),
    )


def empty_state(count, local_heads):
    return (
        jnp.full((local_heads, 2, count), very_low, jnp.float32),
        jnp.zeros((local_heads, 2, count), jnp.float32),
        jnp.zeros((local_heads, 2, count, VALUE), jnp.float32),
    )


def absorb(state, query_set, query_pos, key_block, value_block, key_first):
    running, denoms, accums = state
    local_heads = running.shape[0]
    span = key_block.shape[0]
    key_grid = key_block.reshape(span, local_heads, 2, HEAD)
    scores = jnp.einsum(
        "qhme,khme->hmqk", query_set, key_grid, preferred_element_type=jnp.float32
    ) * HEAD ** (-0.5)
    key_pos = key_first + jnp.arange(span, dtype=jnp.int32)
    allowed = key_pos[None, :] <= query_pos[:, None]
    masked = jnp.where(allowed, scores, very_low)
    updated = jnp.maximum(running, jnp.max(masked, axis=-1))
    exp_weights = jnp.where(allowed, jnp.exp(masked - updated[..., None]), 0.0)
    factor = jnp.exp(running - updated)
    denoms = denoms * factor + jnp.sum(exp_weights, axis=-1)
    value_grid = value_block.reshape(span, local_heads, VALUE)
    product = jnp.einsum(
        "hmqk,khv->hmqv",
        exp_weights.astype(jnp.bfloat16),
        value_grid,
        preferred_element_type=jnp.float32,
    )
    accums = accums * factor[..., None] + product
    return (updated, denoms, accums)


def make_folder(query_sets, carry, pieces):
    key_piece, value_piece = pieces
    length = key_piece.shape[0]
    span = math.gcd(length, 512)

    def one_span(span_index, states):
        offset = span_index * span
        key_block = lax.dynamic_slice_in_dim(key_piece, offset, span, 0)
        value_block = lax.dynamic_slice_in_dim(value_piece, offset, span, 0)
        fresh = []
        for state, query_entry in zip(states, query_sets):
            query_set, query_pos = query_entry

            def take(current):
                return absorb(current, query_set, query_pos, key_block, value_block, offset)

            def leave(current):
                return current

            fresh.append(lax.cond(offset <= query_pos[-1], take, leave, state))
        return tuple(fresh)

    return lax.fori_loop(0, length // span, one_span, carry)


def shards(activations, query_weight, key_weight, value_weight, out_weight, lambdas, head_gain):
    local_heads = lambdas.shape[0]
    query_width = query_weight.shape[1]
    joined_weight = jnp.concatenate([query_weight, key_weight, value_weight], axis=1)
    projected = jnp.dot(
        lax.all_gather(activations, "tp", axis=0, tiled=True),
        joined_weight,
        preferred_element_type=jnp.float32,
    ).astype(jnp.bfloat16)
    row_count = projected.shape[0]
    queries = projected[:, :query_width].reshape(row_count, local_heads, 2, HEAD)
    key_rows = projected[:, query_width : 2 * query_width]
    value_rows = projected[:, 2 * query_width :]
    position = lax.axis_index("sp") * row_count + jnp.arange(row_count, dtype=jnp.int32)
    query_sets = [(queries, position)]
    start_states = tuple((empty_state(entry[0].shape[0], local_heads) for entry in query_sets))
    finals = make_folder(
        query_sets,
        start_states,
        (
            lax.all_gather(key_rows, "sp", axis=0, tiled=True),
            lax.all_gather(value_rows, "sp", axis=0, tiled=True),
        ),
    )
    outputs = []
    for state in finals:
        running, denoms, accums = state
        combined = (
            accums[:, 0] / denoms[:, 0, :, None]
            - lambdas[:, None, None] * accums[:, 1] / denoms[:, 1, :, None]
        )
        inverse_rms = lax.rsqrt(jnp.mean(combined * combined, axis=-1, keepdims=True) + norm_floor)
        normed = (combined * inverse_rms * head_gain).astype(jnp.bfloat16)
        outputs.append(
            jnp.transpose(normed, (1, 0, 2)).reshape(normed.shape[1], local_heads * VALUE)
        )
    heads_out = outputs[0]
    return lax.psum_scatter(
        jnp.dot(heads_out, out_weight, preferred_element_type=jnp.float32).astype(jnp.bfloat16),
        "tp",
        scatter_dimension=0,
        tiled=True,
    )


def solution(mesh):
    in_specs = (
        P(("sp", "tp"), None),
        P(None, "tp"),
        P(None, "tp"),
        P(None, "tp"),
        P("tp", None),
        P("tp"),
        P(),
    )
    out_specs = P(("sp", "tp"), None)
    S, T = mesh.shape["sp"], mesh.shape["tp"]

    def layer(*args):
        L = args[5].shape[0] // T
        rows = args[0].shape[0] // (S * T)
        fits = T == 4 and L == 2 and S == L * T and rows % 16 == 0 and rows * 8 % 128 == 0
        local = functools.partial(fused, S, T, L) if fits else shards
        return jax.shard_map(
            local, mesh=mesh, in_specs=in_specs, out_specs=out_specs, check_vma=False
        )(*args)

    return layer
```

```python
import functools
import math

import jax
import jax.numpy as jnp
from jax import lax
from jax.experimental import pallas as pl
from jax.experimental.pallas import tpu as pltpu
from jax.sharding import PartitionSpec as P

HEAD = 128
VALUE = 256


norm_floor = 0.02
very_low = -1e30
MESH = pl.DeviceIdType.MESH


def layer_kernel(
    S, T, L, R,
    act, qw, kw, vw, ow, lam_ref, gain_ref,
    out,
    lam_in, gain, A, WP, W, PQ, PK, QC, KV, HO, HI, LS, LB, ACC, MX, DN, TOT,
    w_sem, own_sem, a_send, a_recv, lam_send, lam_recv,
    ox_send, ox_recv, oy_send, oy_recv, m_send, m_recv,
    p_send, p_recv, q_recv, f_send, f_recv, g_recv, h_send, h_recv,
):
    X, Y = 2, 2
    Z = S // Y
    H = Z // 2
    s = lax.axis_index("sp")
    t = lax.axis_index("tp")
    x = t // 2
    c = t % 2
    y = s % Y
    z = s // Y
    half = z // H
    low = z % H
    mate = x * 2 + (1 - c)
    across = (1 - x) * 2 + c
    diagonal = (1 - x) * 2 + (1 - c)
    beside = z * Y + (1 - y)
    pair = (half * H + 1 - low) * Y + y
    side = (low + y) % 2
    near = half * H + 1 - low
    third = (1 - half) * H
    last = third + 1
    edge = (z == 0) | (z == Z - 1)
    ahead = (1 - half) * (Z - 1)
    behind = (1 - half) * H + half * (H - 1)
    early = jnp.where(edge, ahead, near)
    later = jnp.where(edge, near, ahead)
    held = (z == Z - 1) & (c != half)
    head = x * 2 * L + z
    span = T * R
    scale = HEAD ** (-0.5) * math.log2(math.e)

    def remote(src, dst, ss, rs, sp, tp):
        return pltpu.make_async_remote_copy(
            src_ref=src, dst_ref=dst, send_sem=ss, recv_sem=rs,
            device_id=(sp, tp), device_id_type=MESH,
        )

    first_head = jnp.where(c == half, 1 - low, c)

    def head_at(i):
        return first_head if i == 0 else 1 - first_head

    def weight_copy(i, part):
        l = head_at(i)
        return pltpu.make_async_copy(
            (qw, kw, vw)[part].at[:, pl.ds(pl.multiple_of(l * 256, 256), 256)],
            WP.at[l, :, part * 256:(part + 1) * 256], w_sem.at[i],
        )

    def own_act():
        return pltpu.make_async_copy(act, A.at[t], own_sem.at[0])

    def small(k):
        pair = ((lam_ref, lam_in), (gain_ref, gain))[k]
        return pltpu.make_async_copy(*pair, own_sem.at[2 + k])

    def own_ow():
        return pltpu.make_async_copy(ow, W.at[pl.ds(t * L, L)], own_sem.at[1])

    def act_across():
        return remote(A.at[t], A.at[t], a_send.at[0], a_recv.at[t], s, across)

    def act_mate():
        return remote(A.at[t], A.at[t], a_send.at[0], a_recv.at[t], s, mate)

    def act_pass():
        return remote(A.at[across], A.at[across], a_send.at[0], a_recv.at[across], s, mate)

    def wait_act(i):
        remote(A.at[i], A.at[i], a_send.at[0], a_recv.at[i], s, mate).wait_recv()

    cut = VALUE // 4
    order = (0, 2, 3, 1)

    def slab(owner, l, k):
        return W.at[owner * L + l, pl.ds(k * cut, cut)]

    def ow_across(k):
        l, q = (side, order[k]) if k < 4 else (1 - side, order[3])
        return remote(
            ow.at[l, pl.ds(q * cut, cut)], slab(t, l, q), ox_send.at[0], ox_recv.at[k], s, across
        )

    def ow_side(k, l, aside=False):
        if k < 2:
            part = slab(across, l, order[k])
        else:
            part = W.at[across * L + l, pl.ds(order[2] * cut + (k - 2) * (cut // 2), cut // 2)]
        target = beside if aside else (beside, pair)[k % 2]
        return remote(part, part, oy_send.at[0], oy_recv.at[min(k, 2)], target, t)

    def ow_pass(k):
        l, q = (side, order[k]) if k < 4 else (1 - side, (1, 0, 2, 3)[k - 4])
        part = slab(across, l, q)
        return remote(part, part, m_send.at[0], m_recv.at[k // 4], s, mate)

    def ow_mate():
        return remote(ow, W.at[pl.ds(t * L, L)], m_send.at[0], m_recv.at[2], s, mate)

    def lam_out():
        return remote(LS, LB, lam_send.at[0], lam_recv.at[0], s, mate)

    barrier = pltpu.get_barrier_semaphore()
    own_act().start()
    small(0).start()
    small(1).start()
    greeted = [(beside, t)]
    for i in range(Z):
        row = ((z + i) % Z) * Y + y
        greeted += [(row, mate), (row, across)] + ([(row, t)] if i > 0 else [])
    for sp, tp in greeted:
        pl.semaphore_signal(barrier, inc=1, device_id=(sp, tp), device_id_type=MESH)
    for part in range(3):
        weight_copy(0, part).start()
    own_act().wait()
    for part in range(3):
        weight_copy(1, part).start()
    own_ow().start()
    pl.semaphore_wait(barrier, len(greeted))

    act_across().start()
    act_mate().start()
    small(0).wait()
    small(1).wait()
    for l in range(L):
        LS[l] = jnp.full((8, 128), lam_in[l], jnp.float32)
    for k in range(5):
        ow_across(k).start()

    def piece_sp(l):
        return (c * L + l) * Y + y

    def kv_rows(row, zs, xx, core):
        return pl.ds(((zs * Y + row) * T + xx * 2 + core) * R, R)

    def ends(kind, l, xx, d):
        if kind == 0:
            return PK.at[l, xx, d], KV.at[kv_rows(y, z, xx, d)]
        return PQ.at[l, xx, d], QC.at[z, xx]

    def arrival(kind, zs, xx):
        return p_recv.at[zs, xx] if kind == 0 else q_recv.at[zs]

    def piece(kind, l, xx, d):
        return remote(
            *ends(kind, l, xx, d), p_send.at[kind], arrival(kind, z, xx),
            piece_sp(l), x * 2 + d,
        )

    def stays(l, d):
        return (piece_sp(l) == s) & (c == d)

    def send(kind, xx, i):
        l = head_at(i)
        for d in range(2):
            @pl.when(stays(l, d))
            def _():
                pltpu.make_async_copy(*ends(kind, l, xx, d), arrival(kind, z, xx)).start()

            @pl.when(jnp.logical_not(stays(l, d)))
            def _():
                piece(kind, l, xx, d).start()

    def project(xx, i):
        l = head_at(i)
        rows = A[pl.ds(xx * 2, 2)].reshape(2 * R, A.shape[2])
        got = jnp.dot(rows, WP[l], preferred_element_type=jnp.float32)
        PQ[l, xx] = (got[:, :256] * scale).astype(jnp.bfloat16).reshape(2, R, 256)
        PK[l, xx] = got[:, 256:].astype(jnp.bfloat16).reshape(2, R, 512)

    def to_beside(zs, xx):
        part = KV.at[kv_rows(y, zs, xx, c)]
        return remote(part, part, f_send.at[0], f_recv.at[zs, xx], beside, t)

    def to_mate(zs, xx):
        part = KV.at[kv_rows(y, zs, xx, c)]
        return remote(part, part, f_send.at[0], g_recv.at[zs], s, mate)

    def to_mate_again(zs, xx):
        part = KV.at[kv_rows(1 - y, zs, xx, c)]
        return remote(part, part, f_send.at[0], g_recv.at[zs], s, mate)

    def forward(zs, xx):
        part = KV.at[kv_rows(y, zs, xx, c)]
        remote(part, part, p_send.at[0], p_recv.at[zs, xx], s, mate).wait_recv()
        to_beside(zs, xx).start()
        to_mate(zs, xx).start()

    def wait_q(zs):
        part = QC.at[zs]
        remote(part, part, p_send.at[1], q_recv.at[zs], s, mate).wait_recv()

    def relay(zs, xx):
        to_beside(zs, xx).wait_recv()
        to_mate_again(zs, xx).start()

    def wait_plane(zs):
        part = KV.at[pl.ds(0, 2 * X * R)]
        remote(part, part, f_send.at[0], g_recv.at[zs], s, mate).wait_recv()

    q_rows = X * R
    k_rows = Y * span

    def chunk(i, j):
        row = lax.broadcasted_iota(jnp.int32, (q_rows, 128), 0)
        lane = lax.broadcasted_iota(jnp.int32, (q_rows, 128), 1)
        ahead_by = row + jnp.where(row >= R, R, 0) - lane + (y * span + c * R + (i - j) * k_rows)
        cols = range(0, k_rows, 128)
        weights, factors = [], []
        for m in range(2):
            q = QC[i, :, :, m * 128:(m + 1) * 128].reshape(q_rows, 128)
            keys = KV[pl.ds(j * k_rows, k_rows), m * 128:(m + 1) * 128]
            sc = lax.dot_general(
                q, keys, (((1,), (1,)), ((), ())), preferred_element_type=jnp.float32
            )
            parts = [jnp.where(ahead_by >= b, sc[:, b:b + 128], very_low) for b in cols]
            top_part = functools.reduce(jnp.maximum, parts)
            old = MX[i, m]
            new = jnp.maximum(old, jnp.max(top_part, axis=1, keepdims=True))
            parts = [jnp.exp2(part - new) for part in parts]
            factor = jnp.exp2(old - new)
            DN[i, m] = DN[i, m] * factor + functools.reduce(jnp.add, parts)
            MX[i, m] = new
            weights.append(jnp.concatenate([part.astype(jnp.bfloat16) for part in parts], axis=1))
            factors.append(factor)
        values = KV[pl.ds(j * k_rows, k_rows), 256:512]
        got = jnp.dot(
            jnp.concatenate(weights, axis=0), values, preferred_element_type=jnp.float32
        )
        for m in range(2):
            for b in range(0, VALUE, 128):
                fresh = got[m * q_rows:(m + 1) * q_rows, b:b + 128]
                ACC[i, m, :, b:b + 128] = ACC[i, m, :, b:b + 128] * factors[m] + fresh

    def home(zs, xx):
        return remote(
            HO.at[zs, xx], HI.at[head], h_send.at[0], h_recv.at[head],
            zs * Y + y, xx * 2 + c,
        )

    def ends_here(zs, xx):
        return (zs == z) & (xx == x)

    def finish(i):
        mine = jnp.where(z // L == c, LS[z % L], LB[z % L])[:1, :1]
        dens = [jnp.sum(DN[i, m], axis=1, keepdims=True) for m in range(2)]
        comb = ACC[i, 0] * (1.0 / dens[0]) - ACC[i, 1] * (mine / dens[1])
        inv = lax.rsqrt(jnp.mean(comb * comb, axis=1, keepdims=True) + norm_floor)
        HO[i] = (comb * inv * gain[...]).astype(jnp.bfloat16).reshape(X, R, VALUE)
        for k in range(X):
            xx = (x + 1 + k) % X

            @pl.when(ends_here(i, xx))
            def _():
                pltpu.make_async_copy(HO.at[i, xx], HI.at[head], h_recv.at[head]).start()

            @pl.when(jnp.logical_not(ends_here(i, xx)))
            def _():
                home(i, xx).start()

    def wait_weights(i):
        pltpu.make_async_copy(WP.at[i], WP.at[i], w_sem.at[i]).wait()

    wait_weights(0)
    wait_act(mate)
    project(x, 0)
    send(0, x, 0)
    wait_weights(1)
    project(x, 1)
    send(0, x, 1)
    for i in range(L):
        send(1, x, i)
    forward(z, x)
    lam_out().start()
    ow_mate().start()
    MX[...] = jnp.full(MX.shape, very_low, jnp.float32)
    DN[...] = jnp.zeros(DN.shape, jnp.float32)
    ACC[...] = jnp.zeros(ACC.shape, jnp.float32)
    forward(early, x)
    relay(z, x)
    wait_act(across)
    act_pass().start()
    forward(later, x)
    wait_act(diagonal)
    def send_rest():
        for kind in range(2):
            for i in range(L):
                send(kind, 1 - x, i)

    project(1 - x, 0)

    @pl.when(jnp.logical_not(held))
    def _():
        send(0, 1 - x, 0)

    project(1 - x, 1)

    @pl.when(jnp.logical_not(held))
    def _():
        send(0, 1 - x, 1)
        for i in range(L):
            send(1, 1 - x, i)

    forward(z, 1 - x)
    relay(early, x)
    relay(later, x)
    forward(behind, x)
    top = z == Z - 1
    sooner = jnp.where(top, third, near)
    after = jnp.where(top, near, third)
    forward(sooner, 1 - x)

    relay(z, 1 - x)
    forward(after, 1 - x)
    relay(behind, x)

    @pl.when(held)
    def _():
        send_rest()

    relay(sooner, 1 - x)
    lam_out().wait_recv()
    wait_q(z)
    wait_q(near)

    @pl.when(top)
    def _():
        wait_q(third)

    wait_plane(z)
    wait_plane(sooner)

    def body_step(k, carry):
        upper = half == 1

        @pl.when(k == 0)
        def _():
            for n in range(2):
                ow_across(n).wait_recv()
                ow_pass(n).start()
            ow_side(1, side).start()

        @pl.when(k == 2)
        def _():
            ow_across(2).wait_recv()
            ow_pass(2).start()

            @pl.when(z != 1)
            def _():
                ow_side(3, side).start()

        @pl.when(k == 3 - 2 * top.astype(jnp.int32))
        def _():
            forward(last, 1 - x)

        @pl.when(k == 3)
        def _():
            relay(after, 1 - x)

            @pl.when(jnp.logical_not(top))
            def _():
                wait_q(third)

            wait_plane(after)

        @pl.when(k == jnp.where(z == 0, 3, 4))
        def _():
            ow_side(0, side).start()
            ow_side(2, side).start()

            @pl.when(z == 0)
            def _():
                ow_side(3, side, True).start()

        n = k % 3
        local = (k < 3) != top
        i_near = half * H + jnp.where(n == 0, 0, 1)
        i_third = jnp.where(upper, jnp.where(n == 0, 0, n + 1), H)
        i = jnp.where(local, i_near, i_third)
        j = jnp.where(local, half * H + n // 2, jnp.where(upper, 0, n))
        chunk(i, j)

        @pl.when(jnp.where(upper, jnp.logical_not(local) & (n == 0), jnp.where(local, n != 1, n == 2)))
        def _():
            finish(i)

        return carry

    lax.fori_loop(0, 6, body_step, 0)

    def last_step(k, carry):
        @pl.when(k == 0)
        def _():
            wait_q(last)

        @pl.when(k == 2 - half)
        def _():
            relay(last, 1 - x)

        @pl.when(k == 3 - 2 * half)
        def _():
            wait_plane(last)

        i = jnp.where(
            k == 1, jnp.where(top, last, near),
            jnp.where(k == 2, jnp.where(top, near, last), z),
        )
        i = jnp.where((half == 0) | (k == 0), last, i)
        chunk(i, jnp.where(half == 0, k, jnp.where(k == 0, 0, last)))

        @pl.when(jnp.where(half == 0, k == 3, k > 0))
        def _():
            finish(i)

        return carry

    lax.fori_loop(0, 4, last_step, 0)
    ow_across(3).wait_recv()
    ow_pass(3).start()
    for k in range(2):
        ow_side(k, 1 - side).wait_recv()
        ow_pass(5 + k).start()
    ow_across(4).wait_recv()
    ow_pass(4).start()
    def sent(part, sem):
        remote(part, part, sem, lam_recv.at[0], s, mate).wait_send()

    sent(A.at[pl.ds(0, 3)], a_send.at[0])
    lam_out().wait_send()
    sent(KV.at[pl.ds(0, 3 * Z * X * R)], f_send.at[0])
    keeps = c == half

    def sent_pieces(count):
        sent(KV.at[pl.ds(0, count * X * R)], p_send.at[0])
        sent(QC.at[pl.ds(0, count)], p_send.at[1])

    @pl.when(keeps)
    def _():
        sent_pieces(2 * L - 1)

    @pl.when(jnp.logical_not(keeps))
    def _():
        sent_pieces(2 * L)

    own_ow().wait()
    ow_mate().wait_recv()
    TOT[...] = jnp.zeros(TOT.shape, jnp.float32)

    def wait_passed(n):
        part = W.at[0]
        remote(part, part, m_send.at[0], m_recv.at[n], s, mate).wait_recv()

    def add_head(i, carry):
        entry = 0
        for n in range(T * L):
            entry = jnp.where(i == n, by_plane([order[n] for order in orders]), entry)

        @pl.when(i == 2)
        def _():
            wait_passed(0)

        @pl.when(i == pass_at)
        def _():
            part = slab(across, 0, 0)
            remote(part, part, oy_send.at[0], oy_recv.at[2], s, mate).wait_recv()
            ow_pass(7).start()

        @pl.when(i == late_at)
        def _():
            wait_passed(1)

        plane, off = entry // 4, entry // 2 % 2
        plane = plane // 2 * 2 + (plane + entry % 2 * side) % 2
        h = (x + off) % 2 * 2 * L + plane
        remote(HO.at[0, 0], HI.at[h], h_send.at[0], h_recv.at[h], s, mate).wait_recv()
        TOT[...] += jnp.dot(HI[h], W[h], preferred_element_type=jnp.float32)
        return carry

    def by_plane(values):
        return jnp.where(
            half == 0, jnp.where(low == 0, values[0], values[1]),
            jnp.where(low == 0, values[2], values[3]),
        )

    pass_at = by_plane((4, 2, 4, 1))
    late_at = by_plane((6, 3, 4, 3))
    orders = (
        (0, 4, 3, 12, 8, 11, 7, 15), (0, 4, 3, 7, 8, 10, 12, 14),
        (0, 4, 3, 8, 7, 10, 12, 14), (12, 0, 3, 7, 4, 11, 15, 8),
    )
    lax.fori_loop(0, T * L, add_head, 0)
    sent(W.at[pl.ds(0, 5), pl.ds(0, cut)], ox_send.at[0])

    for when, halves in ((z == 0, 7), (z == 1, 5), (z > 1, 6)):
        @pl.when(when)
        def _():
            sent(W.at[0, pl.ds(0, halves * cut // 2)], oy_send.at[0])

    sent(W.at[pl.ds(0, 2 * L)], m_send.at[0])
    out[...] = TOT[...].astype(jnp.bfloat16)


    sent(HI.at[pl.ds(0, Z * X - 1)], h_send.at[0])


def fused(S, T, L, activations, query_weight, key_weight, value_weight, out_weight, lambdas, head_gain):
    R, D = activations.shape
    X, Y = 2, 2
    Z = S // Y
    bf, f32 = jnp.bfloat16, jnp.float32
    vmem = pl.BlockSpec(memory_space=pltpu.VMEM)
    hbm = pl.BlockSpec(memory_space=pl.ANY)
    dma = pltpu.SemaphoreType.DMA
    width = query_weight.shape[1]
    return pl.pallas_call(
        functools.partial(layer_kernel, S, T, L, R),
        out_shape=pltpu.VMEM((R, D), bf),
        in_specs=[hbm] * 7,
        out_specs=vmem,
        scratch_shapes=[
            pltpu.SMEM((L,), f32),
            pltpu.VMEM((1, VALUE), f32),
            pltpu.VMEM((T, R, D), bf),
            pltpu.VMEM((L, D, 3 * width // L), bf),
            pltpu.VMEM((T * L, VALUE, D), bf),
            pltpu.VMEM((L, X, 2, R, 256), bf),
            pltpu.VMEM((L, X, 2, R, 512), bf),
            pltpu.VMEM((Z, X, R, 256), bf),
            pltpu.VMEM((S * T * R, 512), bf),
            pltpu.VMEM((Z, X, R, VALUE), bf),
            pltpu.VMEM((T * L, R, VALUE), bf),
            pltpu.VMEM((L, 8, 128), f32),
            pltpu.VMEM((L, 8, 128), f32),
            pltpu.VMEM((Z, 2, X * R, VALUE), f32),
            pltpu.VMEM((Z, 2, X * R, 128), f32),
            pltpu.VMEM((Z, 2, X * R, 128), f32),
            pltpu.VMEM((R, D), f32),
            dma((L,)), dma((4,)),
            dma((1,)), dma((T,)),
            dma((1,)), dma((1,)),
            dma((1,)), dma((5,)), dma((1,)), dma((3,)), dma((1,)), dma((3,)),
            dma((2,)), dma((Z, X)), dma((Z,)),
            dma((1,)), dma((Z, X)), dma((Z,)),
            dma((1,)), dma((T * L,)),
        ],
        compiler_params=pltpu.CompilerParams(
            has_side_effects=True, collective_id=0, vmem_limit_bytes=60 * 1024 * 1024
        ),
    )(
        activations, query_weight, key_weight, value_weight,
        out_weight.reshape(L, VALUE, D), lambdas, head_gain.reshape(1, VALUE),
    )


def empty_state(count, local_heads):
    return (
        jnp.full((local_heads, 2, count), very_low, jnp.float32),
        jnp.zeros((local_heads, 2, count), jnp.float32),
        jnp.zeros((local_heads, 2, count, VALUE), jnp.float32),
    )


def absorb(state, query_set, query_pos, key_block, value_block, key_first):
    running, denoms, accums = state
    local_heads = running.shape[0]
    span = key_block.shape[0]
    key_grid = key_block.reshape(span, local_heads, 2, HEAD)
    scores = jnp.einsum(
        "qhme,khme->hmqk", query_set, key_grid, preferred_element_type=jnp.float32
    ) * HEAD ** (-0.5)
    key_pos = key_first + jnp.arange(span, dtype=jnp.int32)
    allowed = key_pos[None, :] <= query_pos[:, None]
    masked = jnp.where(allowed, scores, very_low)
    updated = jnp.maximum(running, jnp.max(masked, axis=-1))
    exp_weights = jnp.where(allowed, jnp.exp(masked - updated[..., None]), 0.0)
    factor = jnp.exp(running - updated)
    denoms = denoms * factor + jnp.sum(exp_weights, axis=-1)
    value_grid = value_block.reshape(span, local_heads, VALUE)
    product = jnp.einsum(
        "hmqk,khv->hmqv",
        exp_weights.astype(jnp.bfloat16),
        value_grid,
        preferred_element_type=jnp.float32,
    )
    accums = accums * factor[..., None] + product
    return (updated, denoms, accums)


def make_folder(query_sets, carry, pieces):
    key_piece, value_piece = pieces
    length = key_piece.shape[0]
    span = math.gcd(length, 512)

    def one_span(span_index, states):
        offset = span_index * span
        key_block = lax.dynamic_slice_in_dim(key_piece, offset, span, 0)
        value_block = lax.dynamic_slice_in_dim(value_piece, offset, span, 0)
        fresh = []
        for state, query_entry in zip(states, query_sets):
            query_set, query_pos = query_entry

            def take(current):
                return absorb(current, query_set, query_pos, key_block, value_block, offset)

            def leave(current):
                return current

            fresh.append(lax.cond(offset <= query_pos[-1], take, leave, state))
        return tuple(fresh)

    return lax.fori_loop(0, length // span, one_span, carry)


def shards(activations, query_weight, key_weight, value_weight, out_weight, lambdas, head_gain):
    local_heads = lambdas.shape[0]
    query_width = query_weight.shape[1]
    joined_weight = jnp.concatenate([query_weight, key_weight, value_weight], axis=1)
    projected = jnp.dot(
        lax.all_gather(activations, "tp", axis=0, tiled=True),
        joined_weight,
        preferred_element_type=jnp.float32,
    ).astype(jnp.bfloat16)
    row_count = projected.shape[0]
    queries = projected[:, :query_width].reshape(row_count, local_heads, 2, HEAD)
    key_rows = projected[:, query_width : 2 * query_width]
    value_rows = projected[:, 2 * query_width :]
    position = lax.axis_index("sp") * row_count + jnp.arange(row_count, dtype=jnp.int32)
    query_sets = [(queries, position)]
    start_states = tuple((empty_state(entry[0].shape[0], local_heads) for entry in query_sets))
    finals = make_folder(
        query_sets,
        start_states,
        (
            lax.all_gather(key_rows, "sp", axis=0, tiled=True),
            lax.all_gather(value_rows, "sp", axis=0, tiled=True),
        ),
    )
    outputs = []
    for state in finals:
        running, denoms, accums = state
        combined = (
            accums[:, 0] / denoms[:, 0, :, None]
            - lambdas[:, None, None] * accums[:, 1] / denoms[:, 1, :, None]
        )
        inverse_rms = lax.rsqrt(jnp.mean(combined * combined, axis=-1, keepdims=True) + norm_floor)
        normed = (combined * inverse_rms * head_gain).astype(jnp.bfloat16)
        outputs.append(
            jnp.transpose(normed, (1, 0, 2)).reshape(normed.shape[1], local_heads * VALUE)
        )
    heads_out = outputs[0]
    return lax.psum_scatter(
        jnp.dot(heads_out, out_weight, preferred_element_type=jnp.float32).astype(jnp.bfloat16),
        "tp",
        scatter_dimension=0,
        tiled=True,
    )


def solution(mesh):
    in_specs = (
        P(("sp", "tp"), None),
        P(None, "tp"),
        P(None, "tp"),
        P(None, "tp"),
        P("tp", None),
        P("tp"),
        P(),
    )
    out_specs = P(("sp", "tp"), None)
    S, T = mesh.shape["sp"], mesh.shape["tp"]

    def layer(*args):
        L = args[5].shape[0] // T
        rows = args[0].shape[0] // (S * T)
        fits = T == 4 and L == 2 and S == L * T and rows % 16 == 0 and rows * 8 % 128 == 0
        local = functools.partial(fused, S, T, L) if fits else shards
        return jax.shard_map(
            local, mesh=mesh, in_specs=in_specs, out_specs=out_specs, check_vma=False
        )(*args)

    return layer
```

```python
import functools
import math

import jax
import jax.numpy as jnp
from jax import lax
from jax.experimental import pallas as pl
from jax.experimental.pallas import tpu as pltpu
from jax.sharding import PartitionSpec as P

HEAD = 128
VALUE = 256


norm_floor = 0.02
very_low = -1e30
MESH = pl.DeviceIdType.MESH


def layer_kernel(
    S, T, L, R,
    act, qw, kw, vw, ow, lam_ref, gain_ref,
    out,
    lam_in, gain, A, WP, W, PQ, PK, QC, KV, HO, HI, LS, LB, ACC, MX, DN, TOT,
    w_sem, own_sem, a_send, a_recv, lam_send, lam_recv,
    ox_send, ox_recv, oy_send, oy_recv, m_send, m_recv,
    p_send, p_recv, q_recv, f_send, f_recv, g_recv, h_send, h_recv,
):
    X, Y = 2, 2
    Z = S // Y
    H = Z // 2
    s = lax.axis_index("sp")
    t = lax.axis_index("tp")
    x = t // 2
    c = t % 2
    y = s % Y
    z = s // Y
    half = z // H
    low = z % H
    mate = x * 2 + (1 - c)
    across = (1 - x) * 2 + c
    diagonal = (1 - x) * 2 + (1 - c)
    beside = z * Y + (1 - y)
    pair = (half * H + 1 - low) * Y + y
    side = (low + y) % 2
    near = half * H + 1 - low
    third = (1 - half) * H
    last = third + 1
    edge = (z == 0) | (z == Z - 1)
    ahead = (1 - half) * (Z - 1)
    behind = (1 - half) * H + half * (H - 1)
    early = jnp.where(edge, ahead, near)
    later = jnp.where(edge, near, ahead)
    held = (z == Z - 1) & (c != half)
    head = x * 2 * L + z
    span = T * R
    scale = HEAD ** (-0.5) * math.log2(math.e)

    def remote(src, dst, ss, rs, sp, tp):
        return pltpu.make_async_remote_copy(
            src_ref=src, dst_ref=dst, send_sem=ss, recv_sem=rs,
            device_id=(sp, tp), device_id_type=MESH,
        )

    first_head = jnp.where(c == half, 1 - low, c)

    def head_at(i):
        return first_head if i == 0 else 1 - first_head

    def weight_copy(i, part):
        l = head_at(i)
        return pltpu.make_async_copy(
            (qw, kw, vw)[part].at[:, pl.ds(pl.multiple_of(l * 256, 256), 256)],
            WP.at[l, :, part * 256:(part + 1) * 256], w_sem.at[i],
        )

    def own_act():
        return pltpu.make_async_copy(act, A.at[t], own_sem.at[0])

    def small(k):
        pair = ((lam_ref, lam_in), (gain_ref, gain))[k]
        return pltpu.make_async_copy(*pair, own_sem.at[2 + k])

    def own_ow():
        return pltpu.make_async_copy(ow, W.at[pl.ds(t * L, L)], own_sem.at[1])

    def act_across():
        return remote(A.at[t], A.at[t], a_send.at[0], a_recv.at[t], s, across)

    def act_mate():
        return remote(A.at[t], A.at[t], a_send.at[0], a_recv.at[t], s, mate)

    def act_pass():
        return remote(A.at[across], A.at[across], a_send.at[0], a_recv.at[across], s, mate)

    def wait_act(i):
        remote(A.at[i], A.at[i], a_send.at[0], a_recv.at[i], s, mate).wait_recv()

    cut = VALUE // 4
    order = (0, 2, 3, 1)

    def slab(owner, l, k):
        return W.at[owner * L + l, pl.ds(k * cut, cut)]

    def ow_across(k):
        l, q = (side, order[k]) if k < 4 else (1 - side, order[3])
        return remote(
            ow.at[l, pl.ds(q * cut, cut)], slab(t, l, q), ox_send.at[0], ox_recv.at[k], s, across
        )

    def ow_side(k, l, aside=False):
        if k < 2:
            part = slab(across, l, order[k])
        else:
            part = W.at[across * L + l, pl.ds(order[2] * cut + (k - 2) * (cut // 2), cut // 2)]
        target = beside if aside else (beside, pair)[k % 2]
        return remote(part, part, oy_send.at[0], oy_recv.at[min(k, 2)], target, t)

    def ow_pass(k):
        l, q = (side, order[k]) if k < 4 else (1 - side, (1, 0, 2, 3)[k - 4])
        part = slab(across, l, q)
        return remote(part, part, m_send.at[0], m_recv.at[k // 4], s, mate)

    def ow_mate():
        return remote(ow, W.at[pl.ds(t * L, L)], m_send.at[0], m_recv.at[2], s, mate)

    def lam_out():
        return remote(LS, LB, lam_send.at[0], lam_recv.at[0], s, mate)

    barrier = pltpu.get_barrier_semaphore()
    own_act().start()
    small(0).start()
    small(1).start()
    greeted = [(beside, t)]
    for i in range(Z):
        row = ((z + i) % Z) * Y + y
        greeted += [(row, mate), (row, across)] + ([(row, t)] if i > 0 else [])
    for sp, tp in greeted:
        pl.semaphore_signal(barrier, inc=1, device_id=(sp, tp), device_id_type=MESH)
    for part in range(3):
        weight_copy(0, part).start()
    own_act().wait()
    for part in range(3):
        weight_copy(1, part).start()
    own_ow().start()
    pl.semaphore_wait(barrier, len(greeted))

    act_across().start()
    act_mate().start()
    small(0).wait()
    small(1).wait()
    for l in range(L):
        LS[l] = jnp.full((8, 128), lam_in[l], jnp.float32)
    for k in range(5):
        ow_across(k).start()

    def piece_sp(l):
        return (c * L + l) * Y + y

    def kv_rows(row, zs, xx, core):
        return pl.ds(((zs * Y + row) * T + xx * 2 + core) * R, R)

    def ends(kind, l, xx, d):
        if kind == 0:
            return PK.at[l, xx, d], KV.at[kv_rows(y, z, xx, d)]
        return PQ.at[l, xx, d], QC.at[z, xx]

    def arrival(kind, zs, xx):
        return p_recv.at[zs, xx] if kind == 0 else q_recv.at[zs]

    def piece(kind, l, xx, d):
        return remote(
            *ends(kind, l, xx, d), p_send.at[kind], arrival(kind, z, xx),
            piece_sp(l), x * 2 + d,
        )

    def stays(l, d):
        return (piece_sp(l) == s) & (c == d)

    def send(kind, xx, i):
        l = head_at(i)
        for d in range(2):
            @pl.when(stays(l, d))
            def _():
                pltpu.make_async_copy(*ends(kind, l, xx, d), arrival(kind, z, xx)).start()

            @pl.when(jnp.logical_not(stays(l, d)))
            def _():
                piece(kind, l, xx, d).start()

    def project(xx, i):
        l = head_at(i)
        rows = A[pl.ds(xx * 2, 2)].reshape(2 * R, A.shape[2])
        got = jnp.dot(rows, WP[l], preferred_element_type=jnp.float32)
        PQ[l, xx] = (got[:, :256] * scale).astype(jnp.bfloat16).reshape(2, R, 256)
        PK[l, xx] = got[:, 256:].astype(jnp.bfloat16).reshape(2, R, 512)

    def to_beside(zs, xx):
        part = KV.at[kv_rows(y, zs, xx, c)]
        return remote(part, part, f_send.at[0], f_recv.at[zs, xx], beside, t)

    def to_mate(zs, xx):
        part = KV.at[kv_rows(y, zs, xx, c)]
        return remote(part, part, f_send.at[0], g_recv.at[zs], s, mate)

    def to_mate_again(zs, xx):
        part = KV.at[kv_rows(1 - y, zs, xx, c)]
        return remote(part, part, f_send.at[0], g_recv.at[zs], s, mate)

    def forward(zs, xx):
        part = KV.at[kv_rows(y, zs, xx, c)]
        remote(part, part, p_send.at[0], p_recv.at[zs, xx], s, mate).wait_recv()
        to_beside(zs, xx).start()
        to_mate(zs, xx).start()

    def wait_q(zs):
        part = QC.at[zs]
        remote(part, part, p_send.at[1], q_recv.at[zs], s, mate).wait_recv()

    def relay(zs, xx):
        to_beside(zs, xx).wait_recv()
        to_mate_again(zs, xx).start()

    def wait_plane(zs):
        part = KV.at[pl.ds(0, 2 * X * R)]
        remote(part, part, f_send.at[0], g_recv.at[zs], s, mate).wait_recv()

    q_rows = X * R
    k_rows = Y * span

    def chunk(i, j):
        row = lax.broadcasted_iota(jnp.int32, (q_rows, 128), 0)
        lane = lax.broadcasted_iota(jnp.int32, (q_rows, 128), 1)
        ahead_by = row + jnp.where(row >= R, R, 0) - lane + (y * span + c * R + (i - j) * k_rows)
        cols = range(0, k_rows, 128)
        weights, factors = [], []
        for m in range(2):
            q = QC[i, :, :, m * 128:(m + 1) * 128].reshape(q_rows, 128)
            keys = KV[pl.ds(j * k_rows, k_rows), m * 128:(m + 1) * 128]
            sc = lax.dot_general(
                q, keys, (((1,), (1,)), ((), ())), preferred_element_type=jnp.float32
            )
            parts = [jnp.where(ahead_by >= b, sc[:, b:b + 128], very_low) for b in cols]
            top_part = functools.reduce(jnp.maximum, parts)
            old = MX[i, m]
            new = jnp.maximum(old, jnp.max(top_part, axis=1, keepdims=True))
            parts = [jnp.exp2(part - new) for part in parts]
            factor = jnp.exp2(old - new)
            DN[i, m] = DN[i, m] * factor + functools.reduce(jnp.add, parts)
            MX[i, m] = new
            weights.append(jnp.concatenate([part.astype(jnp.bfloat16) for part in parts], axis=1))
            factors.append(factor)
        values = KV[pl.ds(j * k_rows, k_rows), 256:512]
        got = jnp.dot(
            jnp.concatenate(weights, axis=0), values, preferred_element_type=jnp.float32
        )
        for m in range(2):
            for b in range(0, VALUE, 128):
                fresh = got[m * q_rows:(m + 1) * q_rows, b:b + 128]
                ACC[i, m, :, b:b + 128] = ACC[i, m, :, b:b + 128] * factors[m] + fresh

    def home(zs, xx):
        return remote(
            HO.at[zs, xx], HI.at[head], h_send.at[0], h_recv.at[head],
            zs * Y + y, xx * 2 + c,
        )

    def ends_here(zs, xx):
        return (zs == z) & (xx == x)

    def finish(i):
        mine = jnp.where(z // L == c, LS[z % L], LB[z % L])[:1, :1]
        dens = [jnp.sum(DN[i, m], axis=1, keepdims=True) for m in range(2)]
        comb = ACC[i, 0] * (1.0 / dens[0]) - ACC[i, 1] * (mine / dens[1])
        inv = lax.rsqrt(jnp.mean(comb * comb, axis=1, keepdims=True) + norm_floor)
        HO[i] = (comb * inv * gain[...]).astype(jnp.bfloat16).reshape(X, R, VALUE)
        for k in range(X):
            xx = (x + 1 + k) % X

            @pl.when(ends_here(i, xx))
            def _():
                pltpu.make_async_copy(HO.at[i, xx], HI.at[head], h_recv.at[head]).start()

            @pl.when(jnp.logical_not(ends_here(i, xx)))
            def _():
                home(i, xx).start()

    def wait_weights(i):
        pltpu.make_async_copy(WP.at[i], WP.at[i], w_sem.at[i]).wait()

    wait_weights(0)
    wait_act(mate)
    project(x, 0)
    send(0, x, 0)
    wait_weights(1)
    project(x, 1)
    send(0, x, 1)
    for i in range(L):
        send(1, x, i)
    forward(z, x)
    lam_out().start()
    ow_mate().start()
    MX[...] = jnp.full(MX.shape, very_low, jnp.float32)
    DN[...] = jnp.zeros(DN.shape, jnp.float32)
    ACC[...] = jnp.zeros(ACC.shape, jnp.float32)
    forward(early, x)
    relay(z, x)
    wait_act(across)
    act_pass().start()
    forward(later, x)
    wait_act(diagonal)
    def send_rest():
        for kind in range(2):
            for i in range(L):
                send(kind, 1 - x, i)

    project(1 - x, 0)

    @pl.when(jnp.logical_not(held))
    def _():
        send(0, 1 - x, 0)

    project(1 - x, 1)

    @pl.when(jnp.logical_not(held))
    def _():
        send(0, 1 - x, 1)
        for i in range(L):
            send(1, 1 - x, i)

    forward(z, 1 - x)
    relay(early, x)
    relay(later, x)
    forward(behind, x)
    top = z == Z - 1
    sooner = jnp.where(top, third, near)
    after = jnp.where(top, near, third)
    forward(sooner, 1 - x)

    relay(z, 1 - x)
    forward(after, 1 - x)
    relay(behind, x)

    @pl.when(held)
    def _():
        send_rest()

    relay(sooner, 1 - x)
    lam_out().wait_recv()
    wait_q(z)
    wait_q(near)

    @pl.when(top)
    def _():
        wait_q(third)

    wait_plane(z)
    wait_plane(sooner)

    def body_step(k, carry):
        upper = half == 1

        @pl.when(k == 0)
        def _():
            for n in range(2):
                ow_across(n).wait_recv()
                ow_pass(n).start()
            ow_side(1, side).start()

        @pl.when(k == 2)
        def _():
            ow_across(2).wait_recv()
            ow_pass(2).start()

            @pl.when(jnp.logical_not(top))
            def _():
                ow_side(2, side).start()

            @pl.when(z != 1)
            def _():
                ow_side(3, side).start()

        @pl.when(k == 3 - 2 * top.astype(jnp.int32))
        def _():
            forward(last, 1 - x)

        @pl.when(k == 3)
        def _():
            relay(after, 1 - x)

            @pl.when(jnp.logical_not(top))
            def _():
                wait_q(third)

            wait_plane(after)

        @pl.when(k == jnp.where(z == 0, 3, 4))
        def _():
            ow_side(0, side).start()

            @pl.when(top)
            def _():
                ow_side(2, side).start()

            @pl.when(z == 0)
            def _():
                ow_side(3, side, True).start()

        n = k % 3
        local = (k < 3) != top
        i_near = half * H + jnp.where(n == 0, 0, 1)
        i_third = jnp.where(upper, jnp.where(n == 0, 0, n + 1), H)
        i = jnp.where(local, i_near, i_third)
        j = jnp.where(local, half * H + n // 2, jnp.where(upper, 0, n))
        chunk(i, j)

        @pl.when(jnp.where(upper, jnp.logical_not(local) & (n == 0), jnp.where(local, n != 1, n == 2)))
        def _():
            finish(i)

        return carry

    lax.fori_loop(0, 6, body_step, 0)

    def last_step(k, carry):
        @pl.when(k == 0)
        def _():
            wait_q(last)

        @pl.when(k == 2 - half)
        def _():
            relay(last, 1 - x)

        @pl.when(k == 3 - 2 * half)
        def _():
            wait_plane(last)

        i = jnp.where(
            k == 1, jnp.where(top, last, near),
            jnp.where(k == 2, jnp.where(top, near, last), z),
        )
        i = jnp.where((half == 0) | (k == 0), last, i)
        chunk(i, jnp.where(half == 0, k, jnp.where(k == 0, 0, last)))

        @pl.when(jnp.where(half == 0, k == 3, k > 0))
        def _():
            finish(i)

        return carry

    lax.fori_loop(0, 4, last_step, 0)
    ow_across(3).wait_recv()
    ow_pass(3).start()
    for k in range(2):
        ow_side(k, 1 - side).wait_recv()
        ow_pass(5 + k).start()
    ow_across(4).wait_recv()
    ow_pass(4).start()
    def sent(part, sem):
        remote(part, part, sem, lam_recv.at[0], s, mate).wait_send()

    sent(A.at[pl.ds(0, 3)], a_send.at[0])
    lam_out().wait_send()
    sent(KV.at[pl.ds(0, 3 * Z * X * R)], f_send.at[0])
    keeps = c == half

    def sent_pieces(count):
        sent(KV.at[pl.ds(0, count * X * R)], p_send.at[0])
        sent(QC.at[pl.ds(0, count)], p_send.at[1])

    @pl.when(keeps)
    def _():
        sent_pieces(2 * L - 1)

    @pl.when(jnp.logical_not(keeps))
    def _():
        sent_pieces(2 * L)

    own_ow().wait()
    ow_mate().wait_recv()
    TOT[...] = jnp.zeros(TOT.shape, jnp.float32)

    def wait_passed(n):
        part = W.at[0]
        remote(part, part, m_send.at[0], m_recv.at[n], s, mate).wait_recv()

    def add_head(i, carry):
        entry = 0
        for n in range(T * L):
            entry = jnp.where(i == n, by_plane([order[n] for order in orders]), entry)

        @pl.when(i == 2)
        def _():
            wait_passed(0)

        @pl.when(i == pass_at)
        def _():
            part = slab(across, 0, 0)
            remote(part, part, oy_send.at[0], oy_recv.at[2], s, mate).wait_recv()
            ow_pass(7).start()

        @pl.when(i == late_at)
        def _():
            wait_passed(1)

        plane, off = entry // 4, entry // 2 % 2
        plane = plane // 2 * 2 + (plane + entry % 2 * side) % 2
        h = (x + off) % 2 * 2 * L + plane
        remote(HO.at[0, 0], HI.at[h], h_send.at[0], h_recv.at[h], s, mate).wait_recv()
        TOT[...] += jnp.dot(HI[h], W[h], preferred_element_type=jnp.float32)
        return carry

    def by_plane(values):
        return jnp.where(
            half == 0, jnp.where(low == 0, values[0], values[1]),
            jnp.where(low == 0, values[2], values[3]),
        )

    pass_at = by_plane((0, 1, 1, 1))
    late_at = by_plane((6, 3, 4, 2))
    orders = (
        (0, 4, 3, 12, 8, 11, 7, 15), (0, 4, 3, 7, 8, 10, 12, 14),
        (0, 4, 3, 8, 7, 10, 12, 14), (12, 0, 14, 2, 4, 6, 10, 8),
    )
    lax.fori_loop(0, T * L, add_head, 0)
    sent(W.at[pl.ds(0, 5), pl.ds(0, cut)], ox_send.at[0])

    for when, halves in ((z == 0, 7), (z == 1, 5), (z > 1, 6)):
        @pl.when(when)
        def _():
            sent(W.at[0, pl.ds(0, halves * cut // 2)], oy_send.at[0])

    sent(W.at[pl.ds(0, 2 * L)], m_send.at[0])
    out[...] = TOT[...].astype(jnp.bfloat16)


    sent(HI.at[pl.ds(0, Z * X - 1)], h_send.at[0])


def fused(S, T, L, activations, query_weight, key_weight, value_weight, out_weight, lambdas, head_gain):
    R, D = activations.shape
    X, Y = 2, 2
    Z = S // Y
    bf, f32 = jnp.bfloat16, jnp.float32
    vmem = pl.BlockSpec(memory_space=pltpu.VMEM)
    hbm = pl.BlockSpec(memory_space=pl.ANY)
    dma = pltpu.SemaphoreType.DMA
    width = query_weight.shape[1]
    return pl.pallas_call(
        functools.partial(layer_kernel, S, T, L, R),
        out_shape=pltpu.VMEM((R, D), bf),
        in_specs=[hbm] * 7,
        out_specs=vmem,
        scratch_shapes=[
            pltpu.SMEM((L,), f32),
            pltpu.VMEM((1, VALUE), f32),
            pltpu.VMEM((T, R, D), bf),
            pltpu.VMEM((L, D, 3 * width // L), bf),
            pltpu.VMEM((T * L, VALUE, D), bf),
            pltpu.VMEM((L, X, 2, R, 256), bf),
            pltpu.VMEM((L, X, 2, R, 512), bf),
            pltpu.VMEM((Z, X, R, 256), bf),
            pltpu.VMEM((S * T * R, 512), bf),
            pltpu.VMEM((Z, X, R, VALUE), bf),
            pltpu.VMEM((T * L, R, VALUE), bf),
            pltpu.VMEM((L, 8, 128), f32),
            pltpu.VMEM((L, 8, 128), f32),
            pltpu.VMEM((Z, 2, X * R, VALUE), f32),
            pltpu.VMEM((Z, 2, X * R, 128), f32),
            pltpu.VMEM((Z, 2, X * R, 128), f32),
            pltpu.VMEM((R, D), f32),
            dma((L,)), dma((4,)),
            dma((1,)), dma((T,)),
            dma((1,)), dma((1,)),
            dma((1,)), dma((5,)), dma((1,)), dma((3,)), dma((1,)), dma((3,)),
            dma((2,)), dma((Z, X)), dma((Z,)),
            dma((1,)), dma((Z, X)), dma((Z,)),
            dma((1,)), dma((T * L,)),
        ],
        compiler_params=pltpu.CompilerParams(
            has_side_effects=True, collective_id=0, vmem_limit_bytes=60 * 1024 * 1024
        ),
    )(
        activations, query_weight, key_weight, value_weight,
        out_weight.reshape(L, VALUE, D), lambdas, head_gain.reshape(1, VALUE),
    )


def empty_state(count, local_heads):
    return (
        jnp.full((local_heads, 2, count), very_low, jnp.float32),
        jnp.zeros((local_heads, 2, count), jnp.float32),
        jnp.zeros((local_heads, 2, count, VALUE), jnp.float32),
    )


def absorb(state, query_set, query_pos, key_block, value_block, key_first):
    running, denoms, accums = state
    local_heads = running.shape[0]
    span = key_block.shape[0]
    key_grid = key_block.reshape(span, local_heads, 2, HEAD)
    scores = jnp.einsum(
        "qhme,khme->hmqk", query_set, key_grid, preferred_element_type=jnp.float32
    ) * HEAD ** (-0.5)
    key_pos = key_first + jnp.arange(span, dtype=jnp.int32)
    allowed = key_pos[None, :] <= query_pos[:, None]
    masked = jnp.where(allowed, scores, very_low)
    updated = jnp.maximum(running, jnp.max(masked, axis=-1))
    exp_weights = jnp.where(allowed, jnp.exp(masked - updated[..., None]), 0.0)
    factor = jnp.exp(running - updated)
    denoms = denoms * factor + jnp.sum(exp_weights, axis=-1)
    value_grid = value_block.reshape(span, local_heads, VALUE)
    product = jnp.einsum(
        "hmqk,khv->hmqv",
        exp_weights.astype(jnp.bfloat16),
        value_grid,
        preferred_element_type=jnp.float32,
    )
    accums = accums * factor[..., None] + product
    return (updated, denoms, accums)


def make_folder(query_sets, carry, pieces):
    key_piece, value_piece = pieces
    length = key_piece.shape[0]
    span = math.gcd(length, 512)

    def one_span(span_index, states):
        offset = span_index * span
        key_block = lax.dynamic_slice_in_dim(key_piece, offset, span, 0)
        value_block = lax.dynamic_slice_in_dim(value_piece, offset, span, 0)
        fresh = []
        for state, query_entry in zip(states, query_sets):
            query_set, query_pos = query_entry

            def take(current):
                return absorb(current, query_set, query_pos, key_block, value_block, offset)

            def leave(current):
                return current

            fresh.append(lax.cond(offset <= query_pos[-1], take, leave, state))
        return tuple(fresh)

    return lax.fori_loop(0, length // span, one_span, carry)


def shards(activations, query_weight, key_weight, value_weight, out_weight, lambdas, head_gain):
    local_heads = lambdas.shape[0]
    query_width = query_weight.shape[1]
    joined_weight = jnp.concatenate([query_weight, key_weight, value_weight], axis=1)
    projected = jnp.dot(
        lax.all_gather(activations, "tp", axis=0, tiled=True),
        joined_weight,
        preferred_element_type=jnp.float32,
    ).astype(jnp.bfloat16)
    row_count = projected.shape[0]
    queries = projected[:, :query_width].reshape(row_count, local_heads, 2, HEAD)
    key_rows = projected[:, query_width : 2 * query_width]
    value_rows = projected[:, 2 * query_width :]
    position = lax.axis_index("sp") * row_count + jnp.arange(row_count, dtype=jnp.int32)
    query_sets = [(queries, position)]
    start_states = tuple((empty_state(entry[0].shape[0], local_heads) for entry in query_sets))
    finals = make_folder(
        query_sets,
        start_states,
        (
            lax.all_gather(key_rows, "sp", axis=0, tiled=True),
            lax.all_gather(value_rows, "sp", axis=0, tiled=True),
        ),
    )
    outputs = []
    for state in finals:
        running, denoms, accums = state
        combined = (
            accums[:, 0] / denoms[:, 0, :, None]
            - lambdas[:, None, None] * accums[:, 1] / denoms[:, 1, :, None]
        )
        inverse_rms = lax.rsqrt(jnp.mean(combined * combined, axis=-1, keepdims=True) + norm_floor)
        normed = (combined * inverse_rms * head_gain).astype(jnp.bfloat16)
        outputs.append(
            jnp.transpose(normed, (1, 0, 2)).reshape(normed.shape[1], local_heads * VALUE)
        )
    heads_out = outputs[0]
    return lax.psum_scatter(
        jnp.dot(heads_out, out_weight, preferred_element_type=jnp.float32).astype(jnp.bfloat16),
        "tp",
        scatter_dimension=0,
        tiled=True,
    )


def solution(mesh):
    in_specs = (
        P(("sp", "tp"), None),
        P(None, "tp"),
        P(None, "tp"),
        P(None, "tp"),
        P("tp", None),
        P("tp"),
        P(),
    )
    out_specs = P(("sp", "tp"), None)
    S, T = mesh.shape["sp"], mesh.shape["tp"]

    def layer(*args):
        L = args[5].shape[0] // T
        rows = args[0].shape[0] // (S * T)
        fits = T == 4 and L == 2 and S == L * T and rows % 16 == 0 and rows * 8 % 128 == 0
        local = functools.partial(fused, S, T, L) if fits else shards
        return jax.shard_map(
            local, mesh=mesh, in_specs=in_specs, out_specs=out_specs, check_vma=False
        )(*args)

    return layer
```

```python
import functools
import math

import jax
import jax.numpy as jnp
from jax import lax
from jax.experimental import pallas as pl
from jax.experimental.pallas import tpu as pltpu
from jax.sharding import PartitionSpec as P

HEAD = 128
VALUE = 256


norm_floor = 0.02
very_low = -1e30
MESH = pl.DeviceIdType.MESH


def layer_kernel(
    S, T, L, R,
    act, qw, kw, vw, ow, lam_ref, gain_ref,
    out,
    lam_in, gain, A, WP, W, PQ, PK, QC, KV, HO, HI, LS, LB, ACC, MX, DN, TOT,
    w_sem, own_sem, a_send, a_recv, lam_send, lam_recv,
    ox_send, ox_recv, oy_send, oy_recv, m_send, m_recv,
    p_send, p_recv, q_recv, f_send, f_recv, g_recv, h_send, h_recv,
):
    X, Y = 2, 2
    Z = S // Y
    H = Z // 2
    s = lax.axis_index("sp")
    t = lax.axis_index("tp")
    x = t // 2
    c = t % 2
    y = s % Y
    z = s // Y
    half = z // H
    low = z % H
    mate = x * 2 + (1 - c)
    across = (1 - x) * 2 + c
    diagonal = (1 - x) * 2 + (1 - c)
    beside = z * Y + (1 - y)
    pair = (half * H + 1 - low) * Y + y
    side = (low + y) % 2
    near = half * H + 1 - low
    third = (1 - half) * H
    last = third + 1
    edge = (z == 0) | (z == Z - 1)
    ahead = (1 - half) * (Z - 1)
    behind = (1 - half) * H + half * (H - 1)
    early = jnp.where(edge, ahead, near)
    later = jnp.where(edge, near, ahead)
    held = (z == Z - 1) & (c != half)
    head = x * 2 * L + z
    span = T * R
    scale = HEAD ** (-0.5) * math.log2(math.e)

    def remote(src, dst, ss, rs, sp, tp):
        return pltpu.make_async_remote_copy(
            src_ref=src, dst_ref=dst, send_sem=ss, recv_sem=rs,
            device_id=(sp, tp), device_id_type=MESH,
        )

    first_head = jnp.where(c == half, 1 - low, c)

    def head_at(i):
        return first_head if i == 0 else 1 - first_head

    def weight_copy(i, part):
        l = head_at(i)
        return pltpu.make_async_copy(
            (qw, kw, vw)[part].at[:, pl.ds(pl.multiple_of(l * 256, 256), 256)],
            WP.at[l, :, part * 256:(part + 1) * 256], w_sem.at[i],
        )

    def own_act():
        return pltpu.make_async_copy(act, A.at[t], own_sem.at[0])

    def small(k):
        pair = ((lam_ref, lam_in), (gain_ref, gain))[k]
        return pltpu.make_async_copy(*pair, own_sem.at[2 + k])

    def own_ow():
        return pltpu.make_async_copy(ow, W.at[pl.ds(t * L, L)], own_sem.at[1])

    def act_across():
        return remote(A.at[t], A.at[t], a_send.at[0], a_recv.at[t], s, across)

    def act_mate():
        return remote(A.at[t], A.at[t], a_send.at[0], a_recv.at[t], s, mate)

    def act_pass():
        return remote(A.at[across], A.at[across], a_send.at[0], a_recv.at[across], s, mate)

    def wait_act(i):
        remote(A.at[i], A.at[i], a_send.at[0], a_recv.at[i], s, mate).wait_recv()

    cut = VALUE // 4
    order = (0, 2, 3, 1)

    def slab(owner, l, k):
        return W.at[owner * L + l, pl.ds(k * cut, cut)]

    def ow_across(k):
        l, q = (side, order[k]) if k < 4 else (1 - side, order[3])
        return remote(
            ow.at[l, pl.ds(q * cut, cut)], slab(t, l, q), ox_send.at[0], ox_recv.at[k], s, across
        )

    def ow_side(k, l, aside=False):
        if k < 2:
            part = slab(across, l, order[k])
        else:
            part = W.at[across * L + l, pl.ds(order[2] * cut + (k - 2) * (cut // 2), cut // 2)]
        target = beside if aside else (beside, pair)[k % 2]
        return remote(part, part, oy_send.at[0], oy_recv.at[min(k, 2)], target, t)

    def ow_pass(k):
        l, q = (side, order[k]) if k < 4 else (1 - side, (1, 0, 2, 3)[k - 4])
        part = slab(across, l, q)
        return remote(part, part, m_send.at[0], m_recv.at[k // 4], s, mate)

    def ow_mate():
        return remote(ow, W.at[pl.ds(t * L, L)], m_send.at[0], m_recv.at[2], s, mate)

    def lam_out():
        return remote(LS, LB, lam_send.at[0], lam_recv.at[0], s, mate)

    barrier = pltpu.get_barrier_semaphore()
    own_act().start()
    small(0).start()
    small(1).start()
    greeted = [(beside, t)]
    for i in range(Z):
        row = ((z + i) % Z) * Y + y
        greeted += [(row, mate), (row, across)] + ([(row, t)] if i > 0 else [])
    for sp, tp in greeted:
        pl.semaphore_signal(barrier, inc=1, device_id=(sp, tp), device_id_type=MESH)
    for part in range(3):
        weight_copy(0, part).start()
    own_act().wait()
    for part in range(3):
        weight_copy(1, part).start()
    own_ow().start()
    pl.semaphore_wait(barrier, len(greeted))

    act_across().start()
    act_mate().start()
    small(0).wait()
    small(1).wait()
    for l in range(L):
        LS[l] = jnp.full((8, 128), lam_in[l], jnp.float32)
    for k in range(5):
        ow_across(k).start()

    def piece_sp(l):
        return (c * L + l) * Y + y

    def kv_rows(row, zs, xx, core):
        return pl.ds(((zs * Y + row) * T + xx * 2 + core) * R, R)

    def ends(kind, l, xx, d):
        if kind == 0:
            return PK.at[l, xx, d], KV.at[kv_rows(y, z, xx, d)]
        return PQ.at[l, xx, d], QC.at[z, xx]

    def arrival(kind, zs, xx):
        return p_recv.at[zs, xx] if kind == 0 else q_recv.at[zs]

    def piece(kind, l, xx, d):
        return remote(
            *ends(kind, l, xx, d), p_send.at[kind], arrival(kind, z, xx),
            piece_sp(l), x * 2 + d,
        )

    def stays(l, d):
        return (piece_sp(l) == s) & (c == d)

    def send(kind, xx, i):
        l = head_at(i)
        for d in range(2):
            @pl.when(stays(l, d))
            def _():
                pltpu.make_async_copy(*ends(kind, l, xx, d), arrival(kind, z, xx)).start()

            @pl.when(jnp.logical_not(stays(l, d)))
            def _():
                piece(kind, l, xx, d).start()

    def project(xx, i):
        l = head_at(i)
        rows = A[pl.ds(xx * 2, 2)].reshape(2 * R, A.shape[2])
        got = jnp.dot(rows, WP[l], preferred_element_type=jnp.float32)
        PQ[l, xx] = (got[:, :256] * scale).astype(jnp.bfloat16).reshape(2, R, 256)
        PK[l, xx] = got[:, 256:].astype(jnp.bfloat16).reshape(2, R, 512)

    def to_beside(zs, xx):
        part = KV.at[kv_rows(y, zs, xx, c)]
        return remote(part, part, f_send.at[0], f_recv.at[zs, xx], beside, t)

    def to_mate(zs, xx):
        part = KV.at[kv_rows(y, zs, xx, c)]
        return remote(part, part, f_send.at[0], g_recv.at[zs], s, mate)

    def to_mate_again(zs, xx):
        part = KV.at[kv_rows(1 - y, zs, xx, c)]
        return remote(part, part, f_send.at[0], g_recv.at[zs], s, mate)

    def forward(zs, xx):
        part = KV.at[kv_rows(y, zs, xx, c)]
        remote(part, part, p_send.at[0], p_recv.at[zs, xx], s, mate).wait_recv()
        to_beside(zs, xx).start()
        to_mate(zs, xx).start()

    def wait_q(zs):
        part = QC.at[zs]
        remote(part, part, p_send.at[1], q_recv.at[zs], s, mate).wait_recv()

    def relay(zs, xx):
        to_beside(zs, xx).wait_recv()
        to_mate_again(zs, xx).start()

    def wait_plane(zs):
        part = KV.at[pl.ds(0, 2 * X * R)]
        remote(part, part, f_send.at[0], g_recv.at[zs], s, mate).wait_recv()

    q_rows = X * R
    k_rows = Y * span

    def chunk(i, j):
        row = lax.broadcasted_iota(jnp.int32, (q_rows, 128), 0)
        lane = lax.broadcasted_iota(jnp.int32, (q_rows, 128), 1)
        ahead_by = row + jnp.where(row >= R, R, 0) - lane + (y * span + c * R + (i - j) * k_rows)
        cols = range(0, k_rows, 128)
        weights, factors = [], []
        for m in range(2):
            q = QC[i, :, :, m * 128:(m + 1) * 128].reshape(q_rows, 128)
            keys = KV[pl.ds(j * k_rows, k_rows), m * 128:(m + 1) * 128]
            sc = lax.dot_general(
                q, keys, (((1,), (1,)), ((), ())), preferred_element_type=jnp.float32
            )
            parts = [jnp.where(ahead_by >= b, sc[:, b:b + 128], very_low) for b in cols]
            top_part = functools.reduce(jnp.maximum, parts)
            old = MX[i, m]
            new = jnp.maximum(old, jnp.max(top_part, axis=1, keepdims=True))
            parts = [jnp.exp2(part - new) for part in parts]
            factor = jnp.exp2(old - new)
            DN[i, m] = DN[i, m] * factor + functools.reduce(jnp.add, parts)
            MX[i, m] = new
            weights.append(jnp.concatenate([part.astype(jnp.bfloat16) for part in parts], axis=1))
            factors.append(factor)
        values = KV[pl.ds(j * k_rows, k_rows), 256:512]
        got = jnp.dot(
            jnp.concatenate(weights, axis=0), values, preferred_element_type=jnp.float32
        )
        for m in range(2):
            for b in range(0, VALUE, 128):
                fresh = got[m * q_rows:(m + 1) * q_rows, b:b + 128]
                ACC[i, m, :, b:b + 128] = ACC[i, m, :, b:b + 128] * factors[m] + fresh

    def home(zs, xx):
        return remote(
            HO.at[zs, xx], HI.at[head], h_send.at[0], h_recv.at[head],
            zs * Y + y, xx * 2 + c,
        )

    def ends_here(zs, xx):
        return (zs == z) & (xx == x)

    def finish(i):
        mine = jnp.where(z // L == c, LS[z % L], LB[z % L])[:1, :1]
        dens = [jnp.sum(DN[i, m], axis=1, keepdims=True) for m in range(2)]
        comb = ACC[i, 0] * (1.0 / dens[0]) - ACC[i, 1] * (mine / dens[1])
        inv = lax.rsqrt(jnp.mean(comb * comb, axis=1, keepdims=True) + norm_floor)
        HO[i] = (comb * inv * gain[...]).astype(jnp.bfloat16).reshape(X, R, VALUE)
        for k in range(X):
            xx = (x + 1 + k) % X

            @pl.when(ends_here(i, xx))
            def _():
                pltpu.make_async_copy(HO.at[i, xx], HI.at[head], h_recv.at[head]).start()

            @pl.when(jnp.logical_not(ends_here(i, xx)))
            def _():
                home(i, xx).start()

    def wait_weights(i):
        pltpu.make_async_copy(WP.at[i], WP.at[i], w_sem.at[i]).wait()

    wait_weights(0)
    wait_act(mate)
    project(x, 0)
    send(0, x, 0)
    wait_weights(1)
    project(x, 1)
    send(0, x, 1)
    for i in range(L):
        send(1, x, i)
    forward(z, x)
    lam_out().start()
    ow_mate().start()
    MX[...] = jnp.full(MX.shape, very_low, jnp.float32)
    DN[...] = jnp.zeros(DN.shape, jnp.float32)
    ACC[...] = jnp.zeros(ACC.shape, jnp.float32)
    forward(early, x)
    relay(z, x)
    wait_act(across)
    act_pass().start()
    forward(later, x)
    wait_act(diagonal)
    def send_rest():
        for kind in range(2):
            for i in range(L):
                send(kind, 1 - x, i)

    project(1 - x, 0)

    @pl.when(jnp.logical_not(held))
    def _():
        send(0, 1 - x, 0)

    project(1 - x, 1)

    @pl.when(jnp.logical_not(held))
    def _():
        send(0, 1 - x, 1)
        for i in range(L):
            send(1, 1 - x, i)

    forward(z, 1 - x)
    relay(early, x)
    relay(later, x)
    forward(behind, x)
    top = z == Z - 1
    sooner = jnp.where(top, third, near)
    after = jnp.where(top, near, third)
    forward(sooner, 1 - x)

    relay(z, 1 - x)
    forward(after, 1 - x)
    @pl.when(held)
    def _():
        send_rest()

    relay(behind, x)

    relay(sooner, 1 - x)
    lam_out().wait_recv()
    wait_q(z)
    wait_q(near)

    @pl.when(top)
    def _():
        wait_q(third)

    wait_plane(z)
    wait_plane(sooner)

    def body_step(k, carry):
        upper = half == 1

        @pl.when(k == 0)
        def _():
            for n in range(2):
                ow_across(n).wait_recv()
                ow_pass(n).start()
            ow_side(1, side).start()

        @pl.when(k == 2)
        def _():
            ow_across(2).wait_recv()
            ow_pass(2).start()

            @pl.when(jnp.logical_not(top))
            def _():
                ow_side(2, side).start()

            @pl.when(z != 1)
            def _():
                ow_side(3, side).start()

        @pl.when(k == 3 - 2 * top.astype(jnp.int32))
        def _():
            forward(last, 1 - x)

        @pl.when(k == 3)
        def _():
            relay(after, 1 - x)

            @pl.when(jnp.logical_not(top))
            def _():
                wait_q(third)

            wait_plane(after)

        @pl.when(k == jnp.where(z == 0, 3, 4))
        def _():
            ow_side(0, side).start()

            @pl.when(top)
            def _():
                ow_side(2, side).start()

            @pl.when(z == 0)
            def _():
                ow_side(3, side, True).start()

        n = k % 3
        local = (k < 3) != top
        i_near = half * H + jnp.where(n == 0, 0, 1)
        i_third = jnp.where(upper, jnp.where(n == 0, 0, n + 1), H)
        i = jnp.where(local, i_near, i_third)
        j = jnp.where(local, half * H + n // 2, jnp.where(upper, 0, n))
        chunk(i, j)

        @pl.when(jnp.where(upper, jnp.logical_not(local) & (n == 0), jnp.where(local, n != 1, n == 2)))
        def _():
            finish(i)

        return carry

    lax.fori_loop(0, 6, body_step, 0)

    def last_step(k, carry):
        @pl.when(k == 0)
        def _():
            wait_q(last)

        @pl.when(k == 2 - half)
        def _():
            relay(last, 1 - x)

        @pl.when(k == 3 - 2 * half)
        def _():
            wait_plane(last)

        i = jnp.where(
            k == 1, jnp.where(top, last, near),
            jnp.where(k == 2, jnp.where(top, near, last), z),
        )
        i = jnp.where((half == 0) | (k == 0), last, i)
        chunk(i, jnp.where(half == 0, k, jnp.where(k == 0, 0, last)))

        @pl.when(jnp.where(half == 0, k == 3, k > 0))
        def _():
            finish(i)

        return carry

    lax.fori_loop(0, 4, last_step, 0)
    ow_across(3).wait_recv()
    ow_pass(3).start()
    for k in range(2):
        ow_side(k, 1 - side).wait_recv()
        ow_pass(5 + k).start()
    ow_across(4).wait_recv()
    ow_pass(4).start()
    def sent(part, sem):
        remote(part, part, sem, lam_recv.at[0], s, mate).wait_send()

    sent(A.at[pl.ds(0, 3)], a_send.at[0])
    lam_out().wait_send()
    sent(KV.at[pl.ds(0, 3 * Z * X * R)], f_send.at[0])
    keeps = c == half

    def sent_pieces(count):
        sent(KV.at[pl.ds(0, count * X * R)], p_send.at[0])
        sent(QC.at[pl.ds(0, count)], p_send.at[1])

    @pl.when(keeps)
    def _():
        sent_pieces(2 * L - 1)

    @pl.when(jnp.logical_not(keeps))
    def _():
        sent_pieces(2 * L)

    own_ow().wait()
    ow_mate().wait_recv()
    TOT[...] = jnp.zeros(TOT.shape, jnp.float32)

    def wait_passed(n):
        part = W.at[0]
        remote(part, part, m_send.at[0], m_recv.at[n], s, mate).wait_recv()

    def add_head(i, carry):
        entry = 0
        for n in range(T * L):
            entry = jnp.where(i == n, by_plane([order[n] for order in orders]), entry)

        @pl.when(i == 2)
        def _():
            wait_passed(0)

        @pl.when(i == pass_at)
        def _():
            part = slab(across, 0, 0)
            remote(part, part, oy_send.at[0], oy_recv.at[2], s, mate).wait_recv()
            ow_pass(7).start()

        @pl.when(i == late_at)
        def _():
            wait_passed(1)

        plane, off = entry // 4, entry // 2 % 2
        plane = plane // 2 * 2 + (plane + entry % 2 * side) % 2
        h = (x + off) % 2 * 2 * L + plane
        remote(HO.at[0, 0], HI.at[h], h_send.at[0], h_recv.at[h], s, mate).wait_recv()
        TOT[...] += jnp.dot(HI[h], W[h], preferred_element_type=jnp.float32)
        return carry

    def by_plane(values):
        return jnp.where(
            half == 0, jnp.where(low == 0, values[0], values[1]),
            jnp.where(low == 0, values[2], values[3]),
        )

    pass_at = by_plane((0, 1, 1, 1))
    late_at = by_plane((6, 3, 4, 2))
    orders = (
        (0, 4, 3, 12, 8, 11, 7, 15), (0, 4, 3, 7, 8, 10, 12, 14),
        (0, 4, 3, 8, 7, 10, 12, 14), (12, 0, 14, 2, 4, 6, 10, 8),
    )
    lax.fori_loop(0, T * L, add_head, 0)
    sent(W.at[pl.ds(0, 5), pl.ds(0, cut)], ox_send.at[0])

    for when, halves in ((z == 0, 7), (z == 1, 5), (z > 1, 6)):
        @pl.when(when)
        def _():
            sent(W.at[0, pl.ds(0, halves * cut // 2)], oy_send.at[0])

    sent(W.at[pl.ds(0, 2 * L)], m_send.at[0])
    out[...] = TOT[...].astype(jnp.bfloat16)


    sent(HI.at[pl.ds(0, Z * X - 1)], h_send.at[0])


def fused(S, T, L, activations, query_weight, key_weight, value_weight, out_weight, lambdas, head_gain):
    R, D = activations.shape
    X, Y = 2, 2
    Z = S // Y
    bf, f32 = jnp.bfloat16, jnp.float32
    vmem = pl.BlockSpec(memory_space=pltpu.VMEM)
    hbm = pl.BlockSpec(memory_space=pl.ANY)
    dma = pltpu.SemaphoreType.DMA
    width = query_weight.shape[1]
    return pl.pallas_call(
        functools.partial(layer_kernel, S, T, L, R),
        out_shape=pltpu.VMEM((R, D), bf),
        in_specs=[hbm] * 7,
        out_specs=vmem,
        scratch_shapes=[
            pltpu.SMEM((L,), f32),
            pltpu.VMEM((1, VALUE), f32),
            pltpu.VMEM((T, R, D), bf),
            pltpu.VMEM((L, D, 3 * width // L), bf),
            pltpu.VMEM((T * L, VALUE, D), bf),
            pltpu.VMEM((L, X, 2, R, 256), bf),
            pltpu.VMEM((L, X, 2, R, 512), bf),
            pltpu.VMEM((Z, X, R, 256), bf),
            pltpu.VMEM((S * T * R, 512), bf),
            pltpu.VMEM((Z, X, R, VALUE), bf),
            pltpu.VMEM((T * L, R, VALUE), bf),
            pltpu.VMEM((L, 8, 128), f32),
            pltpu.VMEM((L, 8, 128), f32),
            pltpu.VMEM((Z, 2, X * R, VALUE), f32),
            pltpu.VMEM((Z, 2, X * R, 128), f32),
            pltpu.VMEM((Z, 2, X * R, 128), f32),
            pltpu.VMEM((R, D), f32),
            dma((L,)), dma((4,)),
            dma((1,)), dma((T,)),
            dma((1,)), dma((1,)),
            dma((1,)), dma((5,)), dma((1,)), dma((3,)), dma((1,)), dma((3,)),
            dma((2,)), dma((Z, X)), dma((Z,)),
            dma((1,)), dma((Z, X)), dma((Z,)),
            dma((1,)), dma((T * L,)),
        ],
        compiler_params=pltpu.CompilerParams(
            has_side_effects=True, collective_id=0, vmem_limit_bytes=60 * 1024 * 1024
        ),
    )(
        activations, query_weight, key_weight, value_weight,
        out_weight.reshape(L, VALUE, D), lambdas, head_gain.reshape(1, VALUE),
    )


def empty_state(count, local_heads):
    return (
        jnp.full((local_heads, 2, count), very_low, jnp.float32),
        jnp.zeros((local_heads, 2, count), jnp.float32),
        jnp.zeros((local_heads, 2, count, VALUE), jnp.float32),
    )


def absorb(state, query_set, query_pos, key_block, value_block, key_first):
    running, denoms, accums = state
    local_heads = running.shape[0]
    span = key_block.shape[0]
    key_grid = key_block.reshape(span, local_heads, 2, HEAD)
    scores = jnp.einsum(
        "qhme,khme->hmqk", query_set, key_grid, preferred_element_type=jnp.float32
    ) * HEAD ** (-0.5)
    key_pos = key_first + jnp.arange(span, dtype=jnp.int32)
    allowed = key_pos[None, :] <= query_pos[:, None]
    masked = jnp.where(allowed, scores, very_low)
    updated = jnp.maximum(running, jnp.max(masked, axis=-1))
    exp_weights = jnp.where(allowed, jnp.exp(masked - updated[..., None]), 0.0)
    factor = jnp.exp(running - updated)
    denoms = denoms * factor + jnp.sum(exp_weights, axis=-1)
    value_grid = value_block.reshape(span, local_heads, VALUE)
    product = jnp.einsum(
        "hmqk,khv->hmqv",
        exp_weights.astype(jnp.bfloat16),
        value_grid,
        preferred_element_type=jnp.float32,
    )
    accums = accums * factor[..., None] + product
    return (updated, denoms, accums)


def make_folder(query_sets, carry, pieces):
    key_piece, value_piece = pieces
    length = key_piece.shape[0]
    span = math.gcd(length, 512)

    def one_span(span_index, states):
        offset = span_index * span
        key_block = lax.dynamic_slice_in_dim(key_piece, offset, span, 0)
        value_block = lax.dynamic_slice_in_dim(value_piece, offset, span, 0)
        fresh = []
        for state, query_entry in zip(states, query_sets):
            query_set, query_pos = query_entry

            def take(current):
                return absorb(current, query_set, query_pos, key_block, value_block, offset)

            def leave(current):
                return current

            fresh.append(lax.cond(offset <= query_pos[-1], take, leave, state))
        return tuple(fresh)

    return lax.fori_loop(0, length // span, one_span, carry)


def shards(activations, query_weight, key_weight, value_weight, out_weight, lambdas, head_gain):
    local_heads = lambdas.shape[0]
    query_width = query_weight.shape[1]
    joined_weight = jnp.concatenate([query_weight, key_weight, value_weight], axis=1)
    projected = jnp.dot(
        lax.all_gather(activations, "tp", axis=0, tiled=True),
        joined_weight,
        preferred_element_type=jnp.float32,
    ).astype(jnp.bfloat16)
    row_count = projected.shape[0]
    queries = projected[:, :query_width].reshape(row_count, local_heads, 2, HEAD)
    key_rows = projected[:, query_width : 2 * query_width]
    value_rows = projected[:, 2 * query_width :]
    position = lax.axis_index("sp") * row_count + jnp.arange(row_count, dtype=jnp.int32)
    query_sets = [(queries, position)]
    start_states = tuple((empty_state(entry[0].shape[0], local_heads) for entry in query_sets))
    finals = make_folder(
        query_sets,
        start_states,
        (
            lax.all_gather(key_rows, "sp", axis=0, tiled=True),
            lax.all_gather(value_rows, "sp", axis=0, tiled=True),
        ),
    )
    outputs = []
    for state in finals:
        running, denoms, accums = state
        combined = (
            accums[:, 0] / denoms[:, 0, :, None]
            - lambdas[:, None, None] * accums[:, 1] / denoms[:, 1, :, None]
        )
        inverse_rms = lax.rsqrt(jnp.mean(combined * combined, axis=-1, keepdims=True) + norm_floor)
        normed = (combined * inverse_rms * head_gain).astype(jnp.bfloat16)
        outputs.append(
            jnp.transpose(normed, (1, 0, 2)).reshape(normed.shape[1], local_heads * VALUE)
        )
    heads_out = outputs[0]
    return lax.psum_scatter(
        jnp.dot(heads_out, out_weight, preferred_element_type=jnp.float32).astype(jnp.bfloat16),
        "tp",
        scatter_dimension=0,
        tiled=True,
    )


def solution(mesh):
    in_specs = (
        P(("sp", "tp"), None),
        P(None, "tp"),
        P(None, "tp"),
        P(None, "tp"),
        P("tp", None),
        P("tp"),
        P(),
    )
    out_specs = P(("sp", "tp"), None)
    S, T = mesh.shape["sp"], mesh.shape["tp"]

    def layer(*args):
        L = args[5].shape[0] // T
        rows = args[0].shape[0] // (S * T)
        fits = T == 4 and L == 2 and S == L * T and rows % 16 == 0 and rows * 8 % 128 == 0
        local = functools.partial(fused, S, T, L) if fits else shards
        return jax.shard_map(
            local, mesh=mesh, in_specs=in_specs, out_specs=out_specs, check_vma=False
        )(*args)

    return layer
```
